32 devices in a mesh: sp: 8 (over z, x), tp: 4 (over y, core).
Axes of the slice: x: 2, y: 2, z: 4, core: 2. Of those that a mesh axis runs over, the one named last changes fastest.
Arguments:
- tokens: bfloat16 [4096, 2048], P('sp', 'tp'), may hold values from -6 to 6
- norm_gain: float32 [2048], replicated, may hold values from 0.1 to 1.9
- w_query: bfloat16 [2048, 1024], P('sp', 'tp'), may hold values from -1 to 1
- w_key: bfloat16 [2048, 256], P('sp', 'tp'), may hold values from -16 to 16
- w_value: bfloat16 [2048, 256], P('sp', 'tp'), may hold values from -1 to 1
- w_post_gate: bfloat16 [2048, 1024], P('sp', 'tp'), may hold values from -0.125 to 0.125
- w_pre_gate: bfloat16 [2048, 1024], P('sp', 'tp'), may hold values from -0.125 to 0.125
- w_conv_in: bfloat16 [2048, 1024], P('sp', 'tp'), may hold values from -0.125 to 0.125
- conv_taps: float32 [3, 1024], P(None, 'tp'), may hold values from -3 to 3
- sink_logit: float32 [16], P('tp'), may hold values from 2 to 6
- w_out_attn: bfloat16 [1024, 2048], P('tp', 'sp'), may hold values from -0.1875 to 0.1875
- w_out_conv: bfloat16 [1024, 2048], P('tp', 'sp'), may hold values from -0.1875 to 0.1875
Outputs:
- mixed: bfloat16 [4096, 2048], P(('sp', 'tp'))
- log_weight_sum: float32 [16, 4096], P('tp', 'sp')
The draws below stay inside these ranges and needn't reach their ends.
All inputs are finite; a program needn't handle non-finite values.
Results may differ from the reference program's by a relative error of at most 0.012.
The reference program's roundings to bfloat16 on the way count: a program that leaves them out, or rounds other values in their place, can miss the bound.
Values may be sent and summed in bfloat16 or wider, within the bound.
A program may use at most 64 MiB of HBM per device.

```python
import jax
import jax.numpy as jnp
from jax import lax

D = 2048
HEADS = 16
KV_HEADS = 4
HEAD_DIM = 64
CONV_CH = 1024
WINDOW = 128
GRID_W = 64
TOKENS = 4096


def query_key_pair(key):
    base = jax.random.fold_in(key, 11)
    query_seed, key_seed = jax.random.split(base, 2)
    fan_scale = D ** (-0.5)
    w_query = jnp.clip(jax.random.normal(query_seed, (D, HEADS * HEAD_DIM), jnp.float32), -6.0, 6.0) * fan_scale
    w_key = jnp.clip(jax.random.normal(key_seed, (D, KV_HEADS * HEAD_DIM), jnp.float32), -6.0, 6.0) * fan_scale
    return (w_query, w_key)


def draw_w_query(key, part):
    return query_key_pair(key)[0].astype(jnp.bfloat16)


def draw_w_key(key, part):
    return query_key_pair(key)[1].astype(jnp.bfloat16)


def steps_of(stream_key, dims, shards, smallest, high):
    factor_of, own = 1.0, jax.random.fold_in(stream_key, 6)
    for axis_at, blocks in shards:
        draws = jnp.exp(jax.random.uniform(jax.random.fold_in(own, axis_at), (blocks,), jnp.float32, smallest / len(shards), high / len(shards)))
        factor_of = factor_of * jnp.repeat(draws, dims[axis_at] // blocks).reshape([-1 if axis == axis_at else 1 for axis in range(len(dims))])
    return factor_of


def normal_values(key, dims, spread, limit, shards=(), kind=jnp.bfloat16):
    array = jax.random.normal(key, dims, jnp.float32) * spread
    if len(shards) > 0:
        array = steps_of(key, dims, shards, -0.22, 0.18) * array
    return jnp.clip(array, min=-limit, max=limit).astype(kind)


def setup_inputs(seed: int = 0) -> dict:
    streams_of = jax.random.split(jax.random.key(seed), 13)
    return {
        "tokens": normal_values(streams_of[0], (TOKENS, D), 1.0, 6.0, ((0, 8), (1, 4))),
        "norm_gain": jnp.clip(1.0 + 0.18 * jax.random.normal(streams_of[1], (D,), jnp.float32), 0.1, 1.9),
        "w_query": draw_w_query(jax.random.fold_in(streams_of[12], 71), 0),
        "w_key": draw_w_key(jax.random.fold_in(streams_of[12], 71), 0),
        "w_value": normal_values(streams_of[4], (D, KV_HEADS * HEAD_DIM), (D // 64) ** -0.5, 1.0, ((0, 8), (1, 4))),
        "w_post_gate": normal_values(streams_of[5], (D, CONV_CH), D ** -0.5, 0.125, ((0, 8), (1, 4))),
        "w_pre_gate": normal_values(streams_of[6], (D, CONV_CH), D ** -0.5, 0.125, ((0, 8), (1, 4))),
        "w_conv_in": normal_values(streams_of[7], (D, CONV_CH), D ** -0.5, 0.125, ((0, 8), (1, 4))),
        "conv_taps": normal_values(streams_of[8], (3, CONV_CH), 0.6, 3.0, ((1, 4),), jnp.float32),
        "sink_logit": jnp.clip(2.0 + 4.0 * jax.random.uniform(streams_of[9], (HEADS,), jnp.float32) ** steps_of(streams_of[9], (HEADS,), ((0, 4),), -0.2, 0.2), 2.0, 6.0),
        "w_out_attn": normal_values(streams_of[10], (HEADS * HEAD_DIM, D), (HEADS * HEAD_DIM) ** -0.5, 0.1875, ((0, 4), (1, 8))),
        "w_out_conv": normal_values(streams_of[11], (CONV_CH, D), CONV_CH ** -0.5, 0.1875, ((0, 4), (1, 8))),
    }


rope_base = 10000.0
norm_eps = 1e-06

def rotate_pair(values, angles):
    first_half, second_half = jnp.split(values, 2, axis=-1)
    cosine = jnp.cos(angles)[:, None, :]
    sine_part = jnp.sin(angles)[:, None, :]
    return jnp.concatenate([first_half * cosine - second_half * sine_part, first_half * sine_part + second_half * cosine], axis=-1)

def axial_rotate(values, positions):
    half_dim = values.shape[-1] // 2
    inv_freq = rope_base ** (-jnp.arange(0, half_dim, 2).astype(jnp.float32) / half_dim)
    row_angle = (positions // GRID_W).astype(jnp.float32)[:, None] * inv_freq
    col_angle = (positions % GRID_W).astype(jnp.float32)[:, None] * inv_freq
    row_part, col_part = jnp.split(values, 2, axis=-1)
    return jnp.concatenate([rotate_pair(row_part, row_angle), rotate_pair(col_part, col_angle)], axis=-1)

def reference(tokens, norm_gain, w_query, w_key, w_value, w_post_gate, w_pre_gate, w_conv_in, conv_taps, sink_logit, w_out_attn, w_out_conv):
    total_tokens = tokens.shape[0]
    whole = tokens.astype(jnp.float32)
    normed = (whole * lax.rsqrt(lax.optimization_barrier(jnp.mean(whole * whole, axis=1, keepdims=True)) + norm_eps) * norm_gain.astype(jnp.float32)).astype(jnp.bfloat16)

    def project(weight):
        return jnp.dot(normed, weight, preferred_element_type=jnp.float32)
    positions = jnp.arange(total_tokens, dtype=jnp.int32)
    queries = axial_rotate(project(w_query).reshape(total_tokens, HEADS, HEAD_DIM), positions).astype(jnp.bfloat16)
    keys_rot = axial_rotate(project(w_key).reshape(total_tokens, KV_HEADS, HEAD_DIM), positions).astype(jnp.bfloat16)
    values_all = project(w_value).astype(jnp.bfloat16).reshape(total_tokens, KV_HEADS, HEAD_DIM)
    mixed_input = lax.optimization_barrier((project(w_pre_gate) * project(w_conv_in)).astype(jnp.bfloat16)).astype(jnp.float32)
    padded = jnp.pad(mixed_input, ((1, 1), (0, 0)))
    tap_weights = conv_taps.astype(jnp.float32)
    convolved = tap_weights[0] * padded[:-2] + tap_weights[1] * padded[1:-1] + tap_weights[2] * padded[2:]
    conv_out = (project(w_post_gate) * convolved).astype(jnp.bfloat16)
    blocks = total_tokens // WINDOW
    group_size = HEADS // KV_HEADS
    pad_spec = ((WINDOW, WINDOW), (0, 0), (0, 0))
    keys_pad = jnp.pad(keys_rot, pad_spec)
    values_pad = jnp.pad(values_all, pad_spec)
    block_queries = queries.reshape(blocks, WINDOW, KV_HEADS, group_size, HEAD_DIM)
    sink_values = sink_logit.astype(jnp.float32).reshape(KV_HEADS, group_size)[:, :, None]

    def one_block(inputs):
        query_block, index = inputs
        key_block = lax.dynamic_slice_in_dim(keys_pad, index * WINDOW, 3 * WINDOW, 0)
        value_block = lax.dynamic_slice_in_dim(values_pad, index * WINDOW, 3 * WINDOW, 0)
        scores = jnp.einsum('qkgd,skd->kgqs', query_block.astype(jnp.float32), key_block.astype(jnp.float32)) * HEAD_DIM ** (-0.5)
        query_pos = index * WINDOW + jnp.arange(WINDOW, dtype=jnp.int32)
        key_pos = index * WINDOW - WINDOW + jnp.arange(3 * WINDOW, dtype=jnp.int32)
        allowed = (jnp.abs(key_pos[None, :] - query_pos[:, None]) <= WINDOW) & (key_pos >= 0)[None, :] & (key_pos < total_tokens)[None, :]
        scores = jnp.where(allowed[None, None], scores, -jnp.inf)
        row_max = jnp.maximum(lax.optimization_barrier(jnp.max(scores, axis=-1)), sink_values)
        exp_scores = jnp.exp(scores - row_max[..., None])
        denominator = lax.optimization_barrier(jnp.sum(exp_scores, axis=-1)) + jnp.exp(sink_values - row_max)
        weights = (exp_scores / denominator[..., None]).astype(jnp.bfloat16)
        attended = jnp.einsum('kgqs,skd->qkgd', weights.astype(jnp.float32), value_block.astype(jnp.float32)).astype(jnp.bfloat16)
        return (attended.reshape(WINDOW, HEADS * HEAD_DIM), row_max + jnp.log(denominator))
    attended, log_sum = lax.map(one_block, (block_queries, jnp.arange(blocks, dtype=jnp.int32)))
    attended = attended.reshape(total_tokens, HEADS * HEAD_DIM)
    log_weight_sum = jnp.transpose(log_sum, (1, 2, 0, 3)).reshape(HEADS, total_tokens)
    mixed = (jnp.dot(attended, w_out_attn, preferred_element_type=jnp.float32) + jnp.dot(conv_out, w_out_conv, preferred_element_type=jnp.float32)).astype(jnp.bfloat16)
    return (mixed, log_weight_sum)
```

```python
import functools
import math

import jax
import jax.numpy as jnp
from jax import lax
from jax.experimental import pallas as pl
from jax.experimental.pallas import tpu as pltpu
from jax.sharding import PartitionSpec as P

MESH = pl.DeviceIdType.MESH

HEAD_DIM = 64
WINDOW = 128
GRID_W = 64


rope_base = 10000.0
norm_eps = 1e-06


def padded(block, sides, width):
    for axis, dim in sides:
        count = lax.axis_size(axis)
        forward = [(i, i + 1) for i in range(count - 1)]
        backward = [(target, source) for source, target in forward]
        low = lax.ppermute(
            lax.slice_in_dim(block, block.shape[dim] - width, None, axis=dim), axis, forward
        )
        high = lax.ppermute(lax.slice_in_dim(block, 0, width, axis=dim), axis, backward)
        block = jnp.concatenate([low, block, high], axis=dim)
    return block


def rotate_pair(values, angles):
    first_half, second_half = jnp.split(values, 2, axis=-1)
    cosine = jnp.cos(angles)[:, None, :]
    sine_part = jnp.sin(angles)[:, None, :]
    return jnp.concatenate(
        [
            first_half * cosine - second_half * sine_part,
            first_half * sine_part + second_half * cosine,
        ],
        axis=-1,
    )


def axial_rotate(values, positions):
    half_dim = values.shape[-1] // 2
    inv_freq = rope_base ** (-jnp.arange(0, half_dim, 2).astype(jnp.float32) / half_dim)
    row_angle = (positions // GRID_W).astype(jnp.float32)[:, None] * inv_freq
    col_angle = (positions % GRID_W).astype(jnp.float32)[:, None] * inv_freq
    row_part, col_part = jnp.split(values, 2, axis=-1)
    return jnp.concatenate(
        [rotate_pair(row_part, row_angle), rotate_pair(col_part, col_angle)], axis=-1
    )


def block_windows(source, rows_local, blocks):
    pieces = [
        source[step * WINDOW : step * WINDOW + rows_local].reshape(
            (blocks, WINDOW) + source.shape[1:]
        )
        for step in range(3)
    ]
    return jnp.concatenate(pieces, axis=1)


def on_device(
    tokens,
    norm_gain,
    w_query,
    w_key,
    w_value,
    w_post_gate,
    w_pre_gate,
    w_conv_in,
    conv_taps,
    sink_logit,
    w_out_attn,
    w_out_conv,
):
    whole = lax.all_gather(tokens, "tp", axis=1, tiled=True)
    rows_local = whole.shape[0]
    whole_float = whole.astype(jnp.float32)
    mean_square = jnp.mean(whole_float * whole_float, axis=1, keepdims=True)
    normed = (whole_float * lax.rsqrt(mean_square + norm_eps) * norm_gain).astype(jnp.bfloat16)
    col_widths = [
        w_query.shape[1],
        w_key.shape[1],
        w_value.shape[1],
        w_post_gate.shape[1],
        w_pre_gate.shape[1],
        w_conv_in.shape[1],
    ]
    joined = jnp.concatenate(
        (
            lax.all_gather(w_query, "sp", axis=0, tiled=True),
            lax.all_gather(w_key, "sp", axis=0, tiled=True),
            lax.all_gather(w_value, "sp", axis=0, tiled=True),
            lax.all_gather(w_post_gate, "sp", axis=0, tiled=True),
            lax.all_gather(w_pre_gate, "sp", axis=0, tiled=True),
            lax.all_gather(w_conv_in, "sp", axis=0, tiled=True),
        ),
        axis=1,
    )
    projected = jnp.dot(normed, joined, preferred_element_type=jnp.float32)
    bounds = []
    running = 0
    for col_width in col_widths[:-1]:
        running += col_width
        bounds.append(running)
    query_raw, key_raw, value_raw, post_gate, pre_gate, conv_input = jnp.split(
        projected, bounds, axis=1
    )
    offset = lax.axis_index("sp") * rows_local
    positions = offset + jnp.arange(rows_local, dtype=jnp.int32)
    local_heads = w_query.shape[1] // HEAD_DIM
    local_groups = w_key.shape[1] // HEAD_DIM
    group_size = local_heads // local_groups
    queries = axial_rotate(query_raw.reshape(rows_local, local_heads, HEAD_DIM), positions).astype(
        jnp.bfloat16
    )
    keys_rot = axial_rotate(key_raw.reshape(rows_local, local_groups, HEAD_DIM), positions).astype(
        jnp.bfloat16
    )
    key_value = jnp.concatenate(
        [keys_rot.reshape(rows_local, local_groups * HEAD_DIM), value_raw.astype(jnp.bfloat16)],
        axis=1,
    )
    mixed_input = (pre_gate * conv_input).astype(jnp.bfloat16)
    kv_padded = padded(key_value, (("sp", 0),), WINDOW)
    conv_padded = padded(mixed_input, (("sp", 0),), 1)
    conv_float = conv_padded.astype(jnp.float32)
    convolved = (
        conv_taps[0] * conv_float[:-2]
        + conv_taps[1] * conv_float[1:-1]
        + conv_taps[2] * conv_float[2:]
    )
    conv_out = (post_gate * convolved).astype(jnp.bfloat16)
    total_tokens = rows_local * lax.axis_size("sp")
    blocks = rows_local // WINDOW
    padded_rows = rows_local + 2 * WINDOW
    block_queries = queries.reshape(blocks, WINDOW, local_groups, group_size, HEAD_DIM)
    block_keys = block_windows(
        kv_padded[:, : local_groups * HEAD_DIM].reshape(padded_rows, local_groups, HEAD_DIM),
        rows_local,
        blocks,
    )
    block_values = block_windows(
        kv_padded[:, local_groups * HEAD_DIM :].reshape(padded_rows, local_groups, HEAD_DIM),
        rows_local,
        blocks,
    )
    scores = jnp.einsum(
        "nqkgd,nskd->nkgqs", block_queries, block_keys, preferred_element_type=jnp.float32
    ) * HEAD_DIM ** (-0.5)
    query_pos = positions.reshape(blocks, WINDOW)
    key_pos = (
        offset
        - WINDOW
        + (jnp.arange(blocks, dtype=jnp.int32) * WINDOW)[:, None]
        + jnp.arange(3 * WINDOW, dtype=jnp.int32)[None, :]
    )
    distance = key_pos[:, None, :] - query_pos[:, :, None]
    allowed = (
        (jnp.abs(distance) <= WINDOW)
        & (key_pos >= 0)[:, None, :]
        & (key_pos < total_tokens)[:, None, :]
    )
    scores = jnp.where(allowed[:, None, None], scores, -jnp.inf)
    sink_values = sink_logit.reshape(local_groups, group_size)[None, :, :, None]
    row_max = jnp.maximum(jnp.max(scores, axis=-1), sink_values)
    exp_scores = jnp.exp(scores - row_max[..., None])
    denominator = jnp.sum(exp_scores, axis=-1) + jnp.exp(sink_values - row_max)
    weights = (exp_scores / denominator[..., None]).astype(jnp.bfloat16)
    attended = (
        jnp.einsum("nkgqs,nskd->nqkgd", weights, block_values, preferred_element_type=jnp.float32)
        .astype(jnp.bfloat16)
        .reshape(rows_local, local_heads * HEAD_DIM)
    )
    log_sum = row_max + jnp.log(denominator)
    log_weight_sum = jnp.transpose(log_sum, (1, 2, 0, 3)).reshape(local_heads, rows_local)
    out_attn, out_conv = (
        lax.all_gather(w_out_attn, "sp", axis=1, tiled=True),
        lax.all_gather(w_out_conv, "sp", axis=1, tiled=True),
    )
    mixed = lax.psum_scatter(
        (
            jnp.dot(attended, out_attn, preferred_element_type=jnp.float32)
            + jnp.dot(conv_out, out_conv, preferred_element_type=jnp.float32)
        ).astype(jnp.bfloat16),
        "tp",
        scatter_dimension=0,
        tiled=True,
    )
    return (mixed, log_weight_sum)


def fused_kernel(
    Z, X,
    tok_ref, gain_ref, wq_ref, wk_ref, wv_ref, wpost_ref, wpre_ref, wcin_ref, oa_ref, oc_ref, taps_ref, sink_ref,
    out_ref, lse_ref,
    cos_ref, sin_ref, tok, normed, win_a, win_b, wo, acc_a, acc_b, qbuf, kvp, cf, chalo_out, chalo_in, ac, ext, lse_buf,
    keep, send1, recv1, send2, recv2,
    tok_send, tok_recv, w_send, w_recv, sw_send, sw_recv, halo_sem, r1_send, r1_recv, r2_send, r2_recv, loc_sem,
):
    S = Z * X
    rows, width = tok_ref.shape
    depth = wq_ref.shape[0]
    ow, cols = oa_ref.shape
    qw = qbuf.shape[1]
    cw = cf.shape[1]
    kw = 2 * HEAD_DIM
    TP = tok.shape[0]
    chunk = rows // TP
    sp = lax.axis_index("sp")
    tp = lax.axis_index("tp")
    z, x = sp // X, sp % X
    c, y = tp % 2, tp // 2
    vs = z * X + c
    home, foreign = c == x, c != x
    role = jnp.where(home, 0, 1)
    sib = (sp, y * 2 + 1 - c)
    ynb = (sp, (1 - y) * 2 + c)
    yoth = (sp, (1 - y) * 2 + 1 - c)
    xnb = (z * X + 1 - x, tp)
    swp = (z * X + 1 - x, y * 2 + 1 - c)
    low, high = (sp - X, tp), (sp + X, tp)
    has_low, has_high = z > 0, z < Z - 1
    has_prev, has_next = vs > 0, vs < S - 1
    vn, vp = vs + 1, vs - 1 + S
    next_dev = ((vn // X) * X + x, y * 2 + vn % X)
    prev_dev = ((vp // X - Z) * X + x, y * 2 + vp % X)

    barrier = pltpu.get_barrier_semaphore()

    def greet(dev):
        pl.semaphore_signal(barrier, inc=1, device_id=dev, device_id_type=MESH)

    for dev in (sib, ynb, yoth, xnb, swp):
        greet(dev)
    peers = 5
    across_z = ((has_low, low), (has_high, high), (has_prev & (c == 0), prev_dev), (has_next & (c == 1), next_dev))
    for cond, dev in across_z:
        @pl.when(cond)
        def _(dev=dev):
            greet(dev)
        peers = peers + jnp.where(cond, 1, 0)

    pslot = jnp.where(home, sp, S)
    win_a[pslot, :, 0:qw] = wq_ref[...]
    kv_t = jnp.concatenate([wk_ref[...], wv_ref[...]], axis=0).astype(jnp.float32)
    win_a[pslot, :, qw:qw + kw] = jnp.transpose(kv_t).astype(jnp.bfloat16)
    for part, ref in enumerate((wpost_ref, wpre_ref, wcin_ref)):
        win_b[pslot, :, part * cw:(part + 1) * cw] = ref[...]
    heads = qw // HEAD_DIM
    ext[0] = jnp.zeros(ext.shape[1:], jnp.float32)
    ext[0, 0:3, :] = taps_ref[...]
    ext_lane = lax.broadcasted_iota(jnp.int32, (1, cw), 1)
    sink_row = jnp.zeros((1, cw), jnp.float32)
    for h in range(heads):
        sink_row = jnp.where(ext_lane == h, sink_ref[h], sink_row)
    ext[0, 3:4, :] = sink_row

    pl.semaphore_wait(barrier, peers)

    def remote(src, dst, ssem, rsem, dev):
        return pltpu.make_async_remote_copy(
            src_ref=src, dst_ref=dst, send_sem=ssem, recv_sem=rsem,
            device_id=dev, device_id_type=MESH,
        )

    bufs = (win_a, win_b, wo)
    targets = (low, high, sib)

    def wcopy(kind, slot, direction):
        block = bufs[kind].at[slot]
        return remote(block, block, w_send.at[kind, direction, slot], w_recv.at[kind, slot], targets[direction])

    def own_start(kind):
        for direction, cond in ((0, has_low), (1, has_high)):
            @pl.when(cond)
            def _(direction=direction):
                wcopy(kind, vs, direction).start()
        wcopy(kind, vs, 2).start()

    def swap(i, slot):
        src, dst = (
            (win_a.at[S], win_a.at[slot]),
            (win_b.at[S], win_b.at[slot]),
            (oa_ref, wo.at[slot, pl.ds(0, ow)]),
            (oc_ref, wo.at[slot, pl.ds(ow, cw)]),
            (ext.at[0], ext.at[1]),
            (lse_buf.at[0], lse_buf.at[1]),
        )[i]
        return remote(src, dst, sw_send.at[i], sw_recv.at[i], swp)

    tok_d = remote(tok_ref, tok.at[tp], tok_send.at[0], tok_recv.at[tp], sib)
    tok_y = remote(tok_ref, tok.at[tp], tok_send.at[1], tok_recv.at[tp], (sp, (1 - y) * 2 + x))
    tok_x = remote(tok_ref, tok.at[tp], tok_send.at[2], tok_recv.at[tp], (z * X + 1 - x, y * 2 + x))
    local = [
        pltpu.make_async_copy(tok_ref, tok.at[tp], loc_sem.at[0]),
        pltpu.make_async_copy(oa_ref, wo.at[vs, pl.ds(0, ow)], loc_sem.at[1]),
        pltpu.make_async_copy(oc_ref, wo.at[vs, pl.ds(ow, cw)], loc_sem.at[2]),
    ]

    @pl.when(home)
    def _():
        own_start(0)
        own_start(1)

    @pl.when(foreign)
    def _():
        swap(0, sp).start()

    tok_x.start()
    tok_y.start()

    @pl.when(foreign)
    def _():
        tok_d.start()
        for i in range(1, 5):
            swap(i, sp).start()

    @pl.when(home)
    def _():
        for copy in local:
            copy.start()

    MB = 128
    quarter = HEAD_DIM // 4

    def angles(i, carry):
        r = pl.ds(pl.multiple_of(i * MB, MB), MB)
        pos = vs * rows + i * MB + lax.broadcasted_iota(jnp.int32, (MB, kw), 0)
        lane = lax.broadcasted_iota(jnp.int32, (MB, kw), 1) % HEAD_DIM
        freq = jnp.exp((lane % quarter).astype(jnp.float32) * (-4.0 / HEAD_DIM * math.log(rope_base)))
        index = jnp.where(lane >= 2 * quarter, pos % GRID_W, pos // GRID_W)
        angle = index.astype(jnp.float32) * freq
        cos_ref[r, :] = jnp.cos(angle)
        sin_ref[r, :] = jnp.where(lane % (2 * quarter) < quarter, -1.0, 1.0) * jnp.sin(angle)
        return carry

    def comm(kind, dist):
        for up in (0, 1):
            zz = z + dist * (2 * up - 1)

            @pl.when((zz >= 0) & (zz < Z))
            def _(zz=zz, up=up):
                slot = zz * X + c
                wcopy(kind, slot, 2).wait_recv()

                @pl.when(has_low if up else has_high)
                def _():
                    wcopy(kind, slot, 0 if up else 1).start()
                wcopy(kind, slot, 2).start()

    def relay(cc):
        q = y * 2 + cc
        return remote(tok.at[q], tok.at[q], tok_send.at[3 + cc], tok_recv.at[q], ynb)

    def tok_wait(q):
        remote(tok.at[q], tok.at[q], tok_send.at[0], tok_recv.at[q], ynb).wait_recv()

    RB = 64

    def norm_rows(i, carry):
        r = pl.ds(pl.multiple_of(i * RB, RB), RB)
        total = jnp.zeros((RB, 1), jnp.float32)
        for t in range(TP):
            v = tok[t, r, :].astype(jnp.float32)
            total += jnp.sum(v * v, axis=1, keepdims=True)
        scale = lax.rsqrt(total / (TP * width) + norm_eps)
        for t in range(TP):
            v = tok[t, r, :].astype(jnp.float32)
            g = gain_ref[:, t * width:(t + 1) * width]
            normed[r, t * width:(t + 1) * width] = (v * scale * g).astype(jnp.bfloat16)
        return carry

    PB = 256
    pdepth = X * depth

    def project(kind, zz, first):
        win, acc = ((win_a, acc_a), (win_b, acc_b))[kind]
        n = acc.shape[1]
        wcopy(kind, zz * X + 1 - c, 2).wait_recv()

        def body(i, carry):
            r = pl.ds(pl.multiple_of(i * PB, PB), PB)
            k = pl.ds(pl.multiple_of(zz * pdepth, pdepth), pdepth)
            weight = win[pl.ds(zz * X, X)].reshape(pdepth, n)
            prod = jnp.dot(normed[r, k], weight, preferred_element_type=jnp.float32)
            if first:
                acc[r, :] = prod
            else:
                acc[r, :] += prod
            return carry
        lax.fori_loop(0, rows // PB, body, 0)

    def each_side(dist, fn):
        def step(side, carry):
            zz = z + dist * (2 * side - 1)

            @pl.when((zz >= 0) & (zz < Z))
            def _():
                fn(zz)
            return carry
        lax.fori_loop(0, 2, step, 0)

    def project_at(kind, dist):
        each_side(dist, lambda zz: project(kind, zz, False))

    lax.fori_loop(0, rows // MB, angles, 0)

    @pl.when(foreign)
    def _():
        swap(0, vs).wait_recv()
        own_start(0)

    comm(0, 1)

    @pl.when(foreign)
    def _():
        for cc in range(2):
            tok_wait(y * 2 + cc)
            relay(cc).start()
        swap(1, vs).wait_recv()
        own_start(1)

    comm(1, 1)
    if Z > 2:
        comm(0, 2)

    @pl.when(home)
    def _():
        for copy in local:
            copy.wait()
        tok_wait(y * 2 + 1 - c)
    for cc in range(2):
        tok_wait((1 - y) * 2 + cc)

    lax.fori_loop(0, rows // RB, norm_rows, 0)

    project(0, z, True)
    project(1, z, True)
    project_at(0, 1)
    if Z > 2:
        comm(1, 2)

    @pl.when(foreign)
    def _():
        for i in range(2, 5):
            swap(i, vs).wait_recv()
    own_start(2)
    project_at(1, 1)
    for dist in range(2, Z):
        if dist > 2:
            comm(0, dist)
        project_at(0, dist)

    def turned(v, cosv, sinv):
        lane = lax.broadcasted_iota(jnp.int32, v.shape, 1)
        partner = jnp.where(
            lane % (2 * quarter) < quarter,
            pltpu.roll(v, v.shape[1] - quarter, 1),
            pltpu.roll(v, quarter, 1),
        )
        return v * cosv + partner * sinv

    def k_rows(i, carry):
        r = pl.ds(pl.multiple_of(i * MB, MB), MB)
        v = acc_a[r, qw:qw + kw]
        lane = lax.broadcasted_iota(jnp.int32, v.shape, 1)
        kv = jnp.where(lane < HEAD_DIM, turned(v, cos_ref[r, :], sin_ref[r, :]), v)
        kvp[pl.ds(pl.multiple_of(WINDOW + i * MB, MB), MB), :] = kv.astype(jnp.bfloat16)
        return carry

    lax.fori_loop(0, rows // MB, k_rows, 0)

    def halo(i, src, dst, dev):
        return remote(src, dst, halo_sem.at[2 * i], halo_sem.at[2 * i + 1], dev)

    kv_next = halo(0, kvp.at[pl.ds(rows, WINDOW)], kvp.at[pl.ds(0, WINDOW)], next_dev)
    kv_prev = halo(1, kvp.at[pl.ds(WINDOW, WINDOW)], kvp.at[pl.ds(WINDOW + rows, WINDOW)], prev_dev)
    c_next = halo(2, chalo_out.at[1], chalo_in.at[0], next_dev)
    c_prev = halo(3, chalo_out.at[0], chalo_in.at[1], prev_dev)

    @pl.when(has_next)
    def _():
        kv_next.start()

    @pl.when(has_prev)
    def _():
        kv_prev.start()

    def q_rows(i, carry):
        r = pl.ds(pl.multiple_of(i * MB, MB), MB)
        for k in range(qw // kw):
            qbuf[r, k * kw:(k + 1) * kw] = turned(
                acc_a[r, k * kw:(k + 1) * kw], cos_ref[r, :], sin_ref[r, :]
            ).astype(jnp.bfloat16)
        return carry

    lax.fori_loop(0, rows // MB, q_rows, 0)

    zero_kv = jnp.zeros((WINDOW, kw), jnp.bfloat16)
    zero_c = jnp.zeros((8, cw), jnp.float32)

    @pl.when(has_prev)
    def _():
        kv_next.wait_recv()

    @pl.when(jnp.logical_not(has_prev))
    def _():
        kvp[0:WINDOW, :] = zero_kv

    @pl.when(has_next)
    def _():
        kv_prev.wait_recv()

    @pl.when(jnp.logical_not(has_next))
    def _():
        kvp[WINDOW + rows:, :] = zero_kv

    K3 = 3 * WINDOW
    total_tokens = rows * S

    def attend(b, carry):
        r = pl.ds(pl.multiple_of(b * WINDOW, WINDOW), WINDOW)
        kv = kvp[pl.ds(pl.multiple_of(b * WINDOW, WINDOW), K3), :].astype(jnp.float32)
        lane = lax.broadcasted_iota(jnp.int32, (K3, kw), 1)
        swapped = pltpu.roll(kv, HEAD_DIM, 1)
        kk = jnp.where(lane < HEAD_DIM, kv, swapped).astype(jnp.bfloat16)
        vv = jnp.where(lane < HEAD_DIM, swapped, kv).astype(jnp.bfloat16)
        k_half = [jnp.where(lane < HEAD_DIM, kk, 0), jnp.where(lane < HEAD_DIM, 0, kk)]
        v_half = [jnp.where(lane < HEAD_DIM, vv, 0), jnp.where(lane < HEAD_DIM, 0, vv)]
        qi = lax.broadcasted_iota(jnp.int32, (WINDOW, K3), 0)
        ki = lax.broadcasted_iota(jnp.int32, (WINDOW, K3), 1)
        first = vs * rows + b * WINDOW - WINDOW
        allowed = (ki >= qi) & (ki <= qi + 2 * WINDOW) & (ki + first >= 0) & (ki + first < total_tokens)
        lse_lane = lax.broadcasted_iota(jnp.int32, (WINDOW, WINDOW), 1)
        lse_all = jnp.zeros((WINDOW, WINDOW), jnp.float32)
        for pair in range(heads // 2):
            q = qbuf[r, pair * kw:(pair + 1) * kw]
            total = jnp.zeros((WINDOW, kw), jnp.float32)
            for side in range(2):
                h = pair * 2 + side
                s = lax.dot_general(
                    q, k_half[side], (((1,), (1,)), ((), ())), preferred_element_type=jnp.float32
                ) * HEAD_DIM ** (-0.5)
                s = jnp.where(allowed, s, -jnp.inf)
                sink = ext[role, 3:4, h:h + 1]
                top = jnp.maximum(jnp.max(s, axis=1, keepdims=True), sink)
                e = jnp.exp(s - top)
                den = jnp.sum(e, axis=1, keepdims=True) + jnp.exp(sink - top)
                w = (e * (1.0 / den)).astype(jnp.bfloat16)
                total += jnp.dot(w, v_half[side], preferred_element_type=jnp.float32)
                lse_all = jnp.where(lse_lane == h, top + jnp.log(den), lse_all)
            ac[r, pair * kw:(pair + 1) * kw] = total.astype(jnp.bfloat16)
        lse_buf[0, :, r] = jnp.transpose(lse_all)[0:heads, :]
        return carry

    blocks = rows // WINDOW
    lax.fori_loop(0, blocks, attend, 0)

    @pl.when(foreign)
    def _():
        swap(5, sp).start()

    for dist in range(2, Z):
        if dist > 2:
            comm(1, dist)
        project_at(1, dist)

    def c_rows(i, carry):
        r = pl.ds(pl.multiple_of(i * MB, MB), MB)
        mi = (acc_b[r, cw:2 * cw] * acc_b[r, 2 * cw:3 * cw]).astype(jnp.bfloat16)
        cf[pl.ds(pl.multiple_of(8 + i * MB, 8), MB), :] = mi.astype(jnp.float32)
        return carry

    lax.fori_loop(0, rows // MB, c_rows, 0)
    E = chalo_out.shape[1]
    chalo_out[0] = cf[8:8 + E, :].astype(jnp.bfloat16)
    chalo_out[1] = cf[8 + rows - E:8 + rows, :].astype(jnp.bfloat16)

    @pl.when(has_next)
    def _():
        c_next.start()

    @pl.when(has_prev)
    def _():
        c_prev.start()

    @pl.when(has_prev)
    def _():
        c_next.wait_recv()
        cf[0:8, :] = chalo_in[0, E - 8:E, :].astype(jnp.float32)

    @pl.when(jnp.logical_not(has_prev))
    def _():
        cf[0:8, :] = zero_c

    @pl.when(has_next)
    def _():
        c_prev.wait_recv()
        cf[8 + rows:16 + rows, :] = chalo_in[1, 0:8, :].astype(jnp.float32)

    @pl.when(jnp.logical_not(has_next))
    def _():
        cf[8 + rows:16 + rows, :] = zero_c

    taps = [ext[role, t:t + 1, :] for t in range(3)]
    for i in range(rows // MB):
        a = 8 + i * MB
        conv = (
            taps[0] * cf[a - 1:a - 1 + MB, :]
            + taps[1] * cf[a:a + MB, :]
            + taps[2] * cf[a + 1:a + 1 + MB, :]
        )
        ac[i * MB:(i + 1) * MB, qw:qw + cw] = (acc_b[i * MB:(i + 1) * MB, 0:cw] * conv).astype(jnp.bfloat16)

    mine_dev = (z * X + c, y * 2 + c)
    other_dev = (z * X + c, y * 2 + 1 - c)

    def r1(s, src, dst, dev):
        return remote(send1.at[s, src], recv1.at[s, dst], r1_send.at[s, src], r1_recv.at[s, dst], dev)

    def r2(s, src, dst, dev):
        return remote(send2.at[s, src], recv2.at[s, dst], r2_send.at[s, src], r2_recv.at[s, dst], dev)

    def out_dot(s, yo, m):
        co = c if m == 0 else 1 - c
        r = pl.ds(pl.multiple_of((2 * yo + co) * chunk, chunk), chunk)
        return jnp.dot(ac[r, :], wo[s], preferred_element_type=jnp.float32)

    def produce_x(s):
        for yo in range(2):
            for m in (1, 0):
                v = out_dot(s, yo, m)
                if m == 0:
                    keep[s, yo] = v
                send1[s, m, yo] = v.astype(jnp.bfloat16)
        r1(s, 1, role, other_dev).start()

        @pl.when(foreign)
        def _():
            r1(s, 0, 1, mine_dev).start()

    def produce_y(s):
        for m in range(2):
            send1[s, 0, m] = out_dot(s, 1 - y, m).astype(jnp.bfloat16)
        r1(s, 0, 0, ynb).start()
        for m in range(2):
            keep[s, m] = out_dot(s, y, m)

    def stage_x(s):
        r1(s, 0, 1, mine_dev).wait_recv()

        def pass_on(base):
            send2[s, 0] = (base(1 - y) + recv1[s, 1, 1 - y].astype(jnp.float32)).astype(jnp.bfloat16)
            r2(s, 0, 0, ynb).start()
            keep[s, y] = base(y) + recv1[s, 1, y].astype(jnp.float32)

        @pl.when(home)
        def _():
            pass_on(lambda yo: keep[s, yo])

        @pl.when(foreign)
        def _():
            r1(s, 1, 0, other_dev).wait_recv()
            pass_on(lambda yo: recv1[s, 0, yo].astype(jnp.float32))

    def stage_y(s):
        r1(s, 0, 0, ynb).wait_recv()
        send2[s, 1] = (keep[s, 1] + recv1[s, 0, 1].astype(jnp.float32)).astype(jnp.bfloat16)
        r2(s, 1, role, other_dev).start()
        mine = keep[s, 0] + recv1[s, 0, 0].astype(jnp.float32)

        @pl.when(home)
        def _():
            keep[s, 0] = mine

        @pl.when(foreign)
        def _():
            send2[s, 0] = mine.astype(jnp.bfloat16)
            r2(s, 0, 1, mine_dev).start()

    def place(s, v):
        out_ref[:, pl.ds(pl.multiple_of(s * cols, cols), cols)] = v.astype(jnp.bfloat16)

    def finish_x(s):
        r2(s, 0, 0, ynb).wait_recv()
        place(s, keep[s, y] + recv2[s, 0].astype(jnp.float32))

    def finish_y(s):
        r2(s, 0, 1, mine_dev).wait_recv()
        arrived = recv2[s, 1].astype(jnp.float32)

        @pl.when(home)
        def _():
            place(s, keep[s, 0] + arrived)

        @pl.when(foreign)
        def _():
            r2(s, 1, 0, other_dev).wait_recv()
            place(s, recv2[s, 0].astype(jnp.float32) + arrived)

    def produce(zz):
        wcopy(2, zz * X + 1 - c, 2).wait_recv()
        produce_x(zz * X)
        produce_y(zz * X + 1)

    def stage(zz):
        stage_x(zz * X)
        stage_y(zz * X + 1)

    def finish(zz):
        finish_x(zz * X)
        finish_y(zz * X + 1)

    produce(z)
    for dist in range(1, Z):
        comm(2, dist)
        each_side(dist, produce)
        if dist == 1:
            stage(z)
        else:
            each_side(dist - 1, stage)
    each_side(Z - 1, stage)
    finish(z)
    for dist in range(1, Z):
        each_side(dist, finish)

    @pl.when(home)
    def _():
        lse_ref[...] = lse_buf[0]

    @pl.when(foreign)
    def _():
        swap(5, vs).wait_recv()
        lse_ref[...] = lse_buf[1]
        tok_d.wait_send()
        for cc in range(2):
            relay(cc).wait_send()
        for i in range(6):
            swap(i, sp).wait_send()

    tok_x.wait_send()
    tok_y.wait_send()

    @pl.when(has_next)
    def _():
        kv_next.wait_send()
        c_next.wait_send()

    @pl.when(has_prev)
    def _():
        kv_prev.wait_send()
        c_prev.wait_send()

    def drain(zz, carry):
        slot = zz * X + c
        for kind in range(3):
            for direction, cond in ((0, (zz >= z) & has_low), (1, (zz <= z) & has_high)):
                @pl.when(cond)
                def _(kind=kind, direction=direction):
                    wcopy(kind, slot, direction).wait_send()
            wcopy(kind, slot, 2).wait_send()
        sx, sy = zz * X, zz * X + 1
        r1(sx, 1, role, other_dev).wait_send()
        r1(sy, 0, 0, ynb).wait_send()
        r2(sx, 0, 0, ynb).wait_send()
        r2(sy, 1, role, other_dev).wait_send()

        @pl.when(foreign)
        def _():
            r1(sx, 0, 1, mine_dev).wait_send()
            r2(sy, 0, 1, mine_dev).wait_send()
        return carry

    lax.fori_loop(0, Z, drain, 0)


def fused(
    tokens, norm_gain, w_query, w_key, w_value, w_post_gate, w_pre_gate, w_conv_in,
    conv_taps, sink_logit, w_out_attn, w_out_conv,
):
    S, TP = lax.axis_size("sp"), lax.axis_size("tp")
    X = 2
    Z = S // X
    rows, width = tokens.shape
    depth, qw = w_query.shape
    cw = w_post_gate.shape[1]
    ow, cols = w_out_attn.shape
    heads = qw // HEAD_DIM
    kw = 2 * HEAD_DIM
    chunk = rows // TP
    bf, f32 = jnp.bfloat16, jnp.float32
    dma = pltpu.SemaphoreType.DMA
    return pl.pallas_call(
        functools.partial(fused_kernel, Z, X),
        out_shape=(
            jax.ShapeDtypeStruct((chunk, S * cols), bf),
            jax.ShapeDtypeStruct((heads, rows), f32),
        ),
        in_specs=[pl.BlockSpec(memory_space=pltpu.VMEM)] * 11 + [pl.BlockSpec(memory_space=pltpu.SMEM)],
        out_specs=(pl.BlockSpec(memory_space=pltpu.VMEM),) * 2,
        scratch_shapes=[
            pltpu.VMEM((rows, kw), f32),
            pltpu.VMEM((rows, kw), f32),
            pltpu.VMEM((TP, rows, width), bf),
            pltpu.VMEM((rows, TP * width), bf),
            pltpu.VMEM((S + 1, depth, qw + kw), bf),
            pltpu.VMEM((S + 1, depth, 3 * cw), bf),
            pltpu.VMEM((S, ow + cw, cols), bf),
            pltpu.VMEM((rows, qw + kw), f32),
            pltpu.VMEM((rows, 3 * cw), f32),
            pltpu.VMEM((rows, qw), bf),
            pltpu.VMEM((rows + 2 * WINDOW, kw), bf),
            pltpu.VMEM((rows + 16, cw), f32),
            pltpu.VMEM((2, 16, cw), bf),
            pltpu.VMEM((2, 16, cw), bf),
            pltpu.VMEM((rows, qw + cw), bf),
            pltpu.VMEM((2, 8, cw), f32),
            pltpu.VMEM((2, heads, rows), f32),
            pltpu.VMEM((S, 2, chunk, cols), f32),
            pltpu.VMEM((S, 2, 2, chunk, cols), bf),
            pltpu.VMEM((S, 2, 2, chunk, cols), bf),
            pltpu.VMEM((S, 2, chunk, cols), bf),
            pltpu.VMEM((S, 2, chunk, cols), bf),
            dma((5,)), dma((TP,)),
            dma((3, 3, S)), dma((3, S)),
            dma((6,)), dma((6,)),
            dma((8,)),
            dma((S, 2)), dma((S, 2)), dma((S, 2)), dma((S, 2)),
            dma((3,)),
        ],
        compiler_params=pltpu.CompilerParams(
            collective_id=0, has_side_effects=True, vmem_limit_bytes=60 * 1024 * 1024
        ),
    )(
        tokens, norm_gain[None, :], w_query, w_key.T, w_value.T, w_post_gate, w_pre_gate, w_conv_in,
        w_out_attn, w_out_conv, conv_taps, sink_logit,
    )


def fits(
    tokens, norm_gain, w_query, w_key, w_value, w_post_gate, w_pre_gate, w_conv_in,
    conv_taps, sink_logit, w_out_attn, w_out_conv,
):
    S, TP = lax.axis_size("sp"), lax.axis_size("tp")
    return (
        TP == 4
        and S % 2 == 0
        and S >= 6
        and w_key.shape[1] == HEAD_DIM
        and w_query.shape[0] % 128 == 0
        and w_query.shape[1] % 128 == 0
        and w_post_gate.shape[1] % 128 == 0
        and w_out_attn.shape[1] % 128 == 0
        and tokens.shape[0] % (TP * WINDOW) == 0
        and tokens.shape[1] % 128 == 0
    )


def either(*args):
    return fused(*args) if fits(*args) else on_device(*args)


def solution(mesh):
    placed = (
        P("sp", "tp"),
        P(),
        P("sp", "tp"),
        P("sp", "tp"),
        P("sp", "tp"),
        P("sp", "tp"),
        P("sp", "tp"),
        P("sp", "tp"),
        P(None, "tp"),
        P("tp"),
        P("tp", "sp"),
        P("tp", "sp"),
    )
    return jax.shard_map(
        either,
        mesh=mesh,
        in_specs=placed,
        out_specs=(P(("sp", "tp"), None), P("tp", "sp")),
        check_vma=False,
    )
```

```python
import functools
import math

import jax
import jax.numpy as jnp
from jax import lax
from jax.experimental import pallas as pl
from jax.experimental.pallas import tpu as pltpu
from jax.sharding import PartitionSpec as P

MESH = pl.DeviceIdType.MESH

HEAD_DIM = 64
WINDOW = 128
GRID_W = 64
EDGE = 16


rope_base = 10000.0
norm_eps = 1e-06


def padded(block, sides, width):
    for axis, dim in sides:
        count = lax.axis_size(axis)
        forward = [(i, i + 1) for i in range(count - 1)]
        backward = [(target, source) for source, target in forward]
        low = lax.ppermute(
            lax.slice_in_dim(block, block.shape[dim] - width, None, axis=dim), axis, forward
        )
        high = lax.ppermute(lax.slice_in_dim(block, 0, width, axis=dim), axis, backward)
        block = jnp.concatenate([low, block, high], axis=dim)
    return block


def rotate_pair(values, angles):
    first_half, second_half = jnp.split(values, 2, axis=-1)
    cosine = jnp.cos(angles)[:, None, :]
    sine_part = jnp.sin(angles)[:, None, :]
    return jnp.concatenate(
        [
            first_half * cosine - second_half * sine_part,
            first_half * sine_part + second_half * cosine,
        ],
        axis=-1,
    )


def axial_rotate(values, positions):
    half_dim = values.shape[-1] // 2
    inv_freq = rope_base ** (-jnp.arange(0, half_dim, 2).astype(jnp.float32) / half_dim)
    row_angle = (positions // GRID_W).astype(jnp.float32)[:, None] * inv_freq
    col_angle = (positions % GRID_W).astype(jnp.float32)[:, None] * inv_freq
    row_part, col_part = jnp.split(values, 2, axis=-1)
    return jnp.concatenate(
        [rotate_pair(row_part, row_angle), rotate_pair(col_part, col_angle)], axis=-1
    )


def block_windows(source, rows_local, blocks):
    pieces = [
        source[step * WINDOW : step * WINDOW + rows_local].reshape(
            (blocks, WINDOW) + source.shape[1:]
        )
        for step in range(3)
    ]
    return jnp.concatenate(pieces, axis=1)


def on_device(
    tokens,
    norm_gain,
    w_query,
    w_key,
    w_value,
    w_post_gate,
    w_pre_gate,
    w_conv_in,
    conv_taps,
    sink_logit,
    w_out_attn,
    w_out_conv,
):
    whole = lax.all_gather(tokens, "tp", axis=1, tiled=True)
    rows_local = whole.shape[0]
    whole_float = whole.astype(jnp.float32)
    mean_square = jnp.mean(whole_float * whole_float, axis=1, keepdims=True)
    normed = (whole_float * lax.rsqrt(mean_square + norm_eps) * norm_gain).astype(jnp.bfloat16)
    col_widths = [
        w_query.shape[1],
        w_key.shape[1],
        w_value.shape[1],
        w_post_gate.shape[1],
        w_pre_gate.shape[1],
        w_conv_in.shape[1],
    ]
    joined = jnp.concatenate(
        (
            lax.all_gather(w_query, "sp", axis=0, tiled=True),
            lax.all_gather(w_key, "sp", axis=0, tiled=True),
            lax.all_gather(w_value, "sp", axis=0, tiled=True),
            lax.all_gather(w_post_gate, "sp", axis=0, tiled=True),
            lax.all_gather(w_pre_gate, "sp", axis=0, tiled=True),
            lax.all_gather(w_conv_in, "sp", axis=0, tiled=True),
        ),
        axis=1,
    )
    projected = jnp.dot(normed, joined, preferred_element_type=jnp.float32)
    bounds = []
    running = 0
    for col_width in col_widths[:-1]:
        running += col_width
        bounds.append(running)
    query_raw, key_raw, value_raw, post_gate, pre_gate, conv_input = jnp.split(
        projected, bounds, axis=1
    )
    offset = lax.axis_index("sp") * rows_local
    positions = offset + jnp.arange(rows_local, dtype=jnp.int32)
    local_heads = w_query.shape[1] // HEAD_DIM
    local_groups = w_key.shape[1] // HEAD_DIM
    group_size = local_heads // local_groups
    queries = axial_rotate(query_raw.reshape(rows_local, local_heads, HEAD_DIM), positions).astype(
        jnp.bfloat16
    )
    keys_rot = axial_rotate(key_raw.reshape(rows_local, local_groups, HEAD_DIM), positions).astype(
        jnp.bfloat16
    )
    key_value = jnp.concatenate(
        [keys_rot.reshape(rows_local, local_groups * HEAD_DIM), value_raw.astype(jnp.bfloat16)],
        axis=1,
    )
    mixed_input = (pre_gate * conv_input).astype(jnp.bfloat16)
    kv_padded = padded(key_value, (("sp", 0),), WINDOW)
    conv_padded = padded(mixed_input, (("sp", 0),), 1)
    conv_float = conv_padded.astype(jnp.float32)
    convolved = (
        conv_taps[0] * conv_float[:-2]
        + conv_taps[1] * conv_float[1:-1]
        + conv_taps[2] * conv_float[2:]
    )
    conv_out = (post_gate * convolved).astype(jnp.bfloat16)
    total_tokens = rows_local * lax.axis_size("sp")
    blocks = rows_local // WINDOW
    padded_rows = rows_local + 2 * WINDOW
    block_queries = queries.reshape(blocks, WINDOW, local_groups, group_size, HEAD_DIM)
    block_keys = block_windows(
        kv_padded[:, : local_groups * HEAD_DIM].reshape(padded_rows, local_groups, HEAD_DIM),
        rows_local,
        blocks,
    )
    block_values = block_windows(
        kv_padded[:, local_groups * HEAD_DIM :].reshape(padded_rows, local_groups, HEAD_DIM),
        rows_local,
        blocks,
    )
    scores = jnp.einsum(
        "nqkgd,nskd->nkgqs", block_queries, block_keys, preferred_element_type=jnp.float32
    ) * HEAD_DIM ** (-0.5)
    query_pos = positions.reshape(blocks, WINDOW)
    key_pos = (
        offset
        - WINDOW
        + (jnp.arange(blocks, dtype=jnp.int32) * WINDOW)[:, None]
        + jnp.arange(3 * WINDOW, dtype=jnp.int32)[None, :]
    )
    distance = key_pos[:, None, :] - query_pos[:, :, None]
    allowed = (
        (jnp.abs(distance) <= WINDOW)
        & (key_pos >= 0)[:, None, :]
        & (key_pos < total_tokens)[:, None, :]
    )
    scores = jnp.where(allowed[:, None, None], scores, -jnp.inf)
    sink_values = sink_logit.reshape(local_groups, group_size)[None, :, :, None]
    row_max = jnp.maximum(jnp.max(scores, axis=-1), sink_values)
    exp_scores = jnp.exp(scores - row_max[..., None])
    denominator = jnp.sum(exp_scores, axis=-1) + jnp.exp(sink_values - row_max)
    weights = (exp_scores / denominator[..., None]).astype(jnp.bfloat16)
    attended = (
        jnp.einsum("nkgqs,nskd->nqkgd", weights, block_values, preferred_element_type=jnp.float32)
        .astype(jnp.bfloat16)
        .reshape(rows_local, local_heads * HEAD_DIM)
    )
    log_sum = row_max + jnp.log(denominator)
    log_weight_sum = jnp.transpose(log_sum, (1, 2, 0, 3)).reshape(local_heads, rows_local)
    out_attn, out_conv = (
        lax.all_gather(w_out_attn, "sp", axis=1, tiled=True),
        lax.all_gather(w_out_conv, "sp", axis=1, tiled=True),
    )
    mixed = lax.psum_scatter(
        (
            jnp.dot(attended, out_attn, preferred_element_type=jnp.float32)
            + jnp.dot(conv_out, out_conv, preferred_element_type=jnp.float32)
        ).astype(jnp.bfloat16),
        "tp",
        scatter_dimension=0,
        tiled=True,
    )
    return (mixed, log_weight_sum)


def fused_kernel(
    Z, X,
    tok_ref, gain_ref, wq_ref, wk_ref, wv_ref, wpost_ref, wpre_ref, wcin_ref, oa_ref, oc_ref, taps_ref, sink_ref,
    out_ref, lse_ref,
    cos_ref, sin_ref, tok, normed, win_a, win_b, wo, acc_a, acc_b, qbuf, kvp, cf, ac, ext, lse_buf,
    keep, send1, recv1, send2, recv2,
    tok_send, tok_recv, w_send, w_recv, sw_send, sw_recv, halo_sem, r1_send, r1_recv, r2_send, r2_recv, loc_sem,
):
    S = Z * X
    rows, width = tok_ref.shape
    depth = wq_ref.shape[0]
    ow, cols = oa_ref.shape
    qw = qbuf.shape[1]
    cw = cf.shape[1]
    kw = 2 * HEAD_DIM
    TP = tok.shape[0]
    chunk = rows // TP
    sp = lax.axis_index("sp")
    tp = lax.axis_index("tp")
    z, x = sp // X, sp % X
    c, y = tp % 2, tp // 2
    vs = z * X + c
    home, foreign = c == x, c != x
    role = jnp.where(home, 0, 1)
    sib = (sp, y * 2 + 1 - c)
    ynb = (sp, (1 - y) * 2 + c)
    yoth = (sp, (1 - y) * 2 + 1 - c)
    xnb = (z * X + 1 - x, tp)
    swp = (z * X + 1 - x, y * 2 + 1 - c)
    low, high = (sp - X, tp), (sp + X, tp)
    has_low, has_high = z > 0, z < Z - 1
    has_prev, has_next = vs > 0, vs < S - 1
    vn, vp = vs + 1, vs - 1 + S
    next_dev = ((vn // X) * X + x, y * 2 + vn % X)
    prev_dev = ((vp // X - Z) * X + x, y * 2 + vp % X)

    barrier = pltpu.get_barrier_semaphore()

    def greet(dev):
        pl.semaphore_signal(barrier, inc=1, device_id=dev, device_id_type=MESH)

    for dev in (sib, ynb, yoth, xnb, swp):
        greet(dev)
    peers = 5
    across_z = ((has_low, low), (has_high, high), (has_prev & (c == 0), prev_dev), (has_next & (c == 1), next_dev))
    for cond, dev in across_z:
        @pl.when(cond)
        def _(dev=dev):
            greet(dev)
        peers = peers + jnp.where(cond, 1, 0)

    pslot = jnp.where(home, sp, S)
    win_a[pslot, :, 0:qw] = wq_ref[...]
    kv_t = jnp.concatenate([wk_ref[...], wv_ref[...]], axis=0).astype(jnp.float32)
    win_a[pslot, :, qw:qw + kw] = jnp.transpose(kv_t).astype(jnp.bfloat16)
    for part, ref in enumerate((wpost_ref, wpre_ref, wcin_ref)):
        win_b[pslot, :, part * cw:(part + 1) * cw] = ref[...]
    heads = qw // HEAD_DIM
    ext[0] = jnp.zeros(ext.shape[1:], jnp.float32)
    ext[0, 0:3, :] = taps_ref[...]
    for h in range(heads):
        ext[0, 3 + h:4 + h, :] = jnp.full((1, cw), sink_ref[h], jnp.float32)

    pl.semaphore_wait(barrier, peers)

    def remote(src, dst, ssem, rsem, dev):
        return pltpu.make_async_remote_copy(
            src_ref=src, dst_ref=dst, send_sem=ssem, recv_sem=rsem,
            device_id=dev, device_id_type=MESH,
        )

    bufs = (win_a, win_b, wo)
    targets = (low, high, sib)

    def wcopy(kind, slot, direction):
        block = bufs[kind].at[slot]
        return remote(block, block, w_send.at[kind, direction, slot], w_recv.at[kind, slot], targets[direction])

    def own_start(kind):
        for direction, cond in ((0, has_low), (1, has_high)):
            @pl.when(cond)
            def _(direction=direction):
                wcopy(kind, vs, direction).start()
        wcopy(kind, vs, 2).start()

    def swap(i, slot):
        src, dst = (
            (win_a.at[S], win_a.at[slot]),
            (win_b.at[S], win_b.at[slot]),
            (oa_ref, wo.at[slot, pl.ds(0, ow)]),
            (oc_ref, wo.at[slot, pl.ds(ow, cw)]),
            (ext.at[0], ext.at[1]),
            (lse_buf.at[0], lse_buf.at[1]),
        )[i]
        return remote(src, dst, sw_send.at[i], sw_recv.at[i], swp)

    TH = 2
    part_rows = rows // TH

    def tok_copy(src, q, i, part, dev):
        r = pl.ds(part * part_rows, part_rows)
        return remote(src.at[r], tok.at[q, r], tok_send.at[i, part], tok_recv.at[q, part], dev)

    tok_d = [tok_copy(tok_ref, tp, 0, part, sib) for part in range(TH)]
    tok_y = [tok_copy(tok_ref, tp, 1, part, (sp, (1 - y) * 2 + x)) for part in range(TH)]
    tok_x = [tok_copy(tok_ref, tp, 2, part, (z * X + 1 - x, y * 2 + x)) for part in range(TH)]
    local = [
        pltpu.make_async_copy(tok_ref, tok.at[tp], loc_sem.at[0]),
        pltpu.make_async_copy(oa_ref, wo.at[vs, pl.ds(0, ow)], loc_sem.at[1]),
        pltpu.make_async_copy(oc_ref, wo.at[vs, pl.ds(ow, cw)], loc_sem.at[2]),
    ]

    @pl.when(home)
    def _():
        own_start(0)
        own_start(1)

    @pl.when(foreign)
    def _():
        swap(0, sp).start()

    for part in range(TH):
        tok_x[part].start()
        tok_y[part].start()

    @pl.when(foreign)
    def _():
        for copy in tok_d:
            copy.start()
        for i in (1, 4, 2, 3):
            swap(i, sp).start()

    @pl.when(home)
    def _():
        for copy in local:
            copy.start()

    MB = 128
    quarter = HEAD_DIM // 4

    def angles(i, carry):
        r = pl.ds(pl.multiple_of(i * MB, MB), MB)
        pos = vs * rows + i * MB + lax.broadcasted_iota(jnp.int32, (MB, kw), 0)
        lane = lax.broadcasted_iota(jnp.int32, (MB, kw), 1) % HEAD_DIM
        freq = jnp.exp((lane % quarter).astype(jnp.float32) * (-4.0 / HEAD_DIM * math.log(rope_base)))
        index = jnp.where(lane >= 2 * quarter, pos % GRID_W, pos // GRID_W)
        angle = index.astype(jnp.float32) * freq
        cos_ref[r, :] = jnp.cos(angle)
        sin_ref[r, :] = jnp.where(lane % (2 * quarter) < quarter, -1.0, 1.0) * jnp.sin(angle)
        return carry

    def comm(kind, dist, only=None):
        for up in (0, 1):
            zz = z + dist * (2 * up - 1)
            valid = (zz >= 0) & (zz < Z)
            if only is not None:
                valid = valid & only

            @pl.when(valid)
            def _(zz=zz, up=up):
                slot = zz * X + c
                wcopy(kind, slot, 2).wait_recv()

                @pl.when(has_low if up else has_high)
                def _():
                    wcopy(kind, slot, 0 if up else 1).start()
                wcopy(kind, slot, 2).start()

    def relay(cc, part):
        q = y * 2 + cc
        return tok_copy(tok.at[q], q, 3 + cc, part, ynb)

    def tok_wait(q, part):
        tok_copy(tok.at[q], q, 0, part, ynb).wait_recv()

    RB = 64

    def norm_rows(i, carry):
        r = pl.ds(pl.multiple_of(i * RB, RB), RB)
        total = jnp.zeros((RB, 1), jnp.float32)
        for t in range(TP):
            v = tok[t, r, :].astype(jnp.float32)
            total += jnp.sum(v * v, axis=1, keepdims=True)
        scale = lax.rsqrt(total / (TP * width) + norm_eps)
        for t in range(TP):
            v = tok[t, r, :].astype(jnp.float32)
            g = gain_ref[:, t * width:(t + 1) * width]
            normed[r, t * width:(t + 1) * width] = (v * scale * g).astype(jnp.bfloat16)
        return carry

    pdepth = X * depth

    def project(kind, zz, first):
        win, acc = ((win_a, acc_a), (win_b, acc_b))[kind]
        n = acc.shape[1]
        wcopy(kind, zz * X + 1 - c, 2).wait_recv()

        pb = acc.shape[0] // 2

        def body(i, carry):
            r = pl.ds(pl.multiple_of(i * pb, 16), pb)
            k = pl.ds(pl.multiple_of(zz * pdepth, pdepth), pdepth)
            weight = win[pl.ds(zz * X, X)].reshape(pdepth, n)
            prod = jnp.dot(normed[r, k], weight, preferred_element_type=jnp.float32)
            if first:
                acc[r, :] = prod
            else:
                acc[r, :] += prod
            return carry
        lax.fori_loop(0, 2, body, 0)

    def each_side(dist, fn):
        def step(side, carry):
            zz = z + dist * (2 * side - 1)

            @pl.when((zz >= 0) & (zz < Z))
            def _():
                fn(zz)
            return carry
        lax.fori_loop(0, 2, step, 0)

    def project_at(kind, dist):
        each_side(dist, lambda zz: project(kind, zz, False))

    def halo(i, src, dst, dev):
        return remote(src, dst, halo_sem.at[2 * i], halo_sem.at[2 * i + 1], dev)

    kv_next = halo(0, kvp.at[pl.ds(rows, WINDOW)], kvp.at[pl.ds(0, WINDOW)], next_dev)
    kv_prev = halo(1, kvp.at[pl.ds(WINDOW, WINDOW)], kvp.at[pl.ds(WINDOW + rows, WINDOW)], prev_dev)
    n_next = halo(2, normed.at[pl.ds(rows - EDGE, EDGE)], normed.at[pl.ds(rows, EDGE)], next_dev)
    n_prev = halo(3, normed.at[pl.ds(0, EDGE)], normed.at[pl.ds(rows + EDGE, EDGE)], prev_dev)

    lax.fori_loop(0, rows // MB, angles, 0)

    @pl.when(foreign)
    def _():
        swap(0, vs).wait_recv()
        own_start(0)
        for cc in range(2):
            tok_wait(y * 2 + cc, 0)
            relay(cc, 0).start()

    comm(0, 1)

    @pl.when(foreign)
    def _():
        for cc in range(2):
            tok_wait(y * 2 + cc, 1)
            relay(cc, 1).start()

    comm(0, 2)

    @pl.when(foreign)
    def _():
        swap(1, vs).wait_recv()
        own_start(1)
        swap(4, vs).wait_recv()

    @pl.when(home)
    def _():
        comm(1, 1)
        for copy in local:
            copy.wait()
        for part in range(TH):
            tok_wait(y * 2 + 1 - c, part)
    for part in range(TH):
        for cc in range(2):
            tok_wait((1 - y) * 2 + cc, part)
        lax.fori_loop(part * (part_rows // RB), (part + 1) * (part_rows // RB), norm_rows, 0)

    @pl.when(has_next)
    def _():
        n_next.start()

    @pl.when(has_prev)
    def _():
        n_prev.start()

    for dist in range(3, Z):
        comm(0, dist)
    project(0, z, True)
    project_at(0, 1)

    @pl.when(foreign)
    def _():
        comm(1, 1)
    for dist in range(2, Z):
        project_at(0, dist)

    def turned(v, cosv, sinv):
        lane = lax.broadcasted_iota(jnp.int32, v.shape, 1)
        partner = jnp.where(
            lane % (2 * quarter) < quarter,
            pltpu.roll(v, v.shape[1] - quarter, 1),
            pltpu.roll(v, quarter, 1),
        )
        return v * cosv + partner * sinv

    def k_rows(i, carry):
        r = pl.ds(pl.multiple_of(i * MB, MB), MB)
        v = acc_a[r, qw:qw + kw]
        lane = lax.broadcasted_iota(jnp.int32, v.shape, 1)
        kv = jnp.where(lane < HEAD_DIM, turned(v, cos_ref[r, :], sin_ref[r, :]), v)
        kvp[pl.ds(pl.multiple_of(WINDOW + i * MB, MB), MB), :] = kv.astype(jnp.bfloat16)
        return carry

    lax.fori_loop(0, rows // MB, k_rows, 0)

    @pl.when(has_next)
    def _():
        kv_next.start()

    @pl.when(has_prev)
    def _():
        kv_prev.start()

    def q_rows(i, carry):
        r = pl.ds(pl.multiple_of(i * MB, MB), MB)
        for k in range(qw // kw):
            qbuf[r, k * kw:(k + 1) * kw] = turned(
                acc_a[r, k * kw:(k + 1) * kw], cos_ref[r, :], sin_ref[r, :]
            ).astype(jnp.bfloat16)
        return carry

    lax.fori_loop(0, rows // MB, q_rows, 0)

    K3 = 3 * WINDOW
    total_tokens = rows * S

    def attend(b, carry):
        r = pl.ds(pl.multiple_of(b * WINDOW, WINDOW), WINDOW)
        kv = kvp[pl.ds(pl.multiple_of(b * WINDOW, WINDOW), K3), :].astype(jnp.float32)
        lane = lax.broadcasted_iota(jnp.int32, (K3, kw), 1)
        swapped = pltpu.roll(kv, HEAD_DIM, 1)
        kk = jnp.where(lane < HEAD_DIM, kv, swapped).astype(jnp.bfloat16)
        vv = jnp.where(lane < HEAD_DIM, swapped, kv).astype(jnp.bfloat16)
        k_half = [jnp.where(lane < HEAD_DIM, kk, 0), jnp.where(lane < HEAD_DIM, 0, kk)]
        v_half = [jnp.where(lane < HEAD_DIM, vv, 0), jnp.where(lane < HEAD_DIM, 0, vv)]
        qi = lax.broadcasted_iota(jnp.int32, (WINDOW, K3), 0)
        ki = lax.broadcasted_iota(jnp.int32, (WINDOW, K3), 1)
        first = vs * rows + b * WINDOW - WINDOW
        allowed = (ki >= qi) & (ki <= qi + 2 * WINDOW) & (ki + first >= 0) & (ki + first < total_tokens)
        lse_lane = lax.broadcasted_iota(jnp.int32, (WINDOW, WINDOW), 1)
        lse_all = jnp.zeros((WINDOW, WINDOW), jnp.float32)
        for pair in range(heads // 2):
            q = qbuf[r, pair * kw:(pair + 1) * kw]
            total = jnp.zeros((WINDOW, kw), jnp.float32)
            for side in range(2):
                h = pair * 2 + side
                s = lax.dot_general(
                    q, k_half[side], (((1,), (1,)), ((), ())), preferred_element_type=jnp.float32
                ) * HEAD_DIM ** (-0.5)
                s = jnp.where(allowed, s, -jnp.inf)
                sink = ext[role, 3 + h:4 + h, 0:WINDOW]
                top = jnp.maximum(jnp.max(s, axis=1, keepdims=True), sink)
                e = jnp.exp(s - jnp.concatenate([top] * 3, axis=1))
                den = jnp.sum(e, axis=1, keepdims=True) + jnp.exp(sink - top)
                w = (e * jnp.concatenate([1.0 / den] * 3, axis=1)).astype(jnp.bfloat16)
                total += jnp.dot(w, v_half[side], preferred_element_type=jnp.float32)
                lse_all = jnp.where(lse_lane == h, top + jnp.log(den), lse_all)
            ac[r, pair * kw:(pair + 1) * kw] = total.astype(jnp.bfloat16)
        lse_buf[0, :, r] = jnp.transpose(lse_all)[0:heads, :]
        return carry

    blocks = rows // WINDOW
    zero_kv = jnp.zeros((WINDOW, kw), jnp.bfloat16)

    def prev_ready():
        @pl.when(has_prev)
        def _():
            kv_next.wait_recv()

        @pl.when(jnp.logical_not(has_prev))
        def _():
            kvp[0:WINDOW, :] = zero_kv

    def next_ready():
        @pl.when(has_next)
        def _():
            kv_prev.wait_recv()

        @pl.when(jnp.logical_not(has_next))
        def _():
            kvp[WINDOW + rows:, :] = zero_kv

    def edge_ready(at_start):
        @pl.when(at_start)
        def _():
            prev_ready()

        @pl.when(jnp.logical_not(at_start))
        def _():
            next_ready()

    def attend_from(i, carry):
        return attend((1 - c + i) % blocks, carry)

    def b_ready():
        @pl.when(has_prev)
        def _():
            n_next.wait_recv()

        @pl.when(has_next)
        def _():
            n_prev.wait_recv()

        @pl.when(jnp.logical_not(has_prev))
        def _():
            normed[rows:rows + EDGE, :] = jnp.zeros((EDGE, TP * width), jnp.bfloat16)

        @pl.when(jnp.logical_not(has_next))
        def _():
            normed[rows + EDGE:, :] = jnp.zeros((EDGE, TP * width), jnp.bfloat16)

    edge_ready(c == 1)
    lax.fori_loop(0, blocks // 2, attend_from, 0)
    b_ready()
    project(1, z, True)
    comm(1, 2)

    @pl.when(foreign)
    def _():
        for i in (2, 3):
            swap(i, vs).wait_recv()
        own_start(2)
    lax.fori_loop(blocks // 2, blocks - 1, attend_from, 0)
    edge_ready(c == 0)
    lax.fori_loop(blocks - 1, blocks, attend_from, 0)

    @pl.when(foreign)
    def _():
        swap(5, sp).start()

    project_at(1, 1)
    project_at(1, 2)

    @pl.when(home)
    def _():
        own_start(2)
    for dist in range(3, Z):
        comm(1, dist)
        project_at(1, dist)
    inner = has_low & has_high
    outer = jnp.logical_not(inner)
    comm(2, 1, inner)

    def gated(lo, n):
        return (acc_b[lo:lo + n, cw:2 * cw] * acc_b[lo:lo + n, 2 * cw:3 * cw]).astype(jnp.bfloat16)

    for i in range(rows // MB):
        cf[8 + i * MB:8 + (i + 1) * MB, :] = gated(i * MB, MB).astype(jnp.float32)
    edge = gated(rows, 2 * EDGE).astype(jnp.float32)
    cf[0:8, :] = edge[EDGE - 8:EDGE, :]
    cf[8 + rows:16 + rows, :] = edge[EDGE:EDGE + 8, :]

    taps = [ext[role, t:t + 1, :] for t in range(3)]
    for i in range(rows // MB):
        a = 8 + i * MB
        conv = (
            taps[0] * cf[a - 1:a - 1 + MB, :]
            + taps[1] * cf[a:a + MB, :]
            + taps[2] * cf[a + 1:a + 1 + MB, :]
        )
        ac[i * MB:(i + 1) * MB, qw:qw + cw] = (acc_b[i * MB:(i + 1) * MB, 0:cw] * conv).astype(jnp.bfloat16)

    mine_dev = (z * X + c, y * 2 + c)
    other_dev = (z * X + c, y * 2 + 1 - c)

    def r1(s, src, dst, dev):
        return remote(send1.at[s, src], recv1.at[s, dst], r1_send.at[s, src], r1_recv.at[s, dst], dev)

    def r2(s, src, dst, dev):
        return remote(send2.at[s, src], recv2.at[s, dst], r2_send.at[s, src], r2_recv.at[s, dst], dev)

    def out_dot(s, yo, m):
        co = c if m == 0 else 1 - c
        r = pl.ds(pl.multiple_of((2 * yo + co) * chunk, chunk), chunk)
        return jnp.dot(ac[r, :], wo[s], preferred_element_type=jnp.float32)

    def produce_x(s):
        for yo in range(2):
            for m in (1, 0):
                v = out_dot(s, yo, m)
                if m == 0:
                    keep[s, yo] = v
                send1[s, m, yo] = v.astype(jnp.bfloat16)
        r1(s, 1, role, other_dev).start()

        @pl.when(foreign)
        def _():
            r1(s, 0, 1, mine_dev).start()

    def produce_y(s):
        for m in range(2):
            send1[s, 0, m] = out_dot(s, 1 - y, m).astype(jnp.bfloat16)
        r1(s, 0, 0, ynb).start()
        for m in range(2):
            keep[s, m] = out_dot(s, y, m)

    def stage_x(s):
        r1(s, 0, 1, mine_dev).wait_recv()

        def pass_on(base):
            send2[s, 0] = (base(1 - y) + recv1[s, 1, 1 - y].astype(jnp.float32)).astype(jnp.bfloat16)
            r2(s, 0, 0, ynb).start()
            keep[s, y] = base(y) + recv1[s, 1, y].astype(jnp.float32)

        @pl.when(home)
        def _():
            pass_on(lambda yo: keep[s, yo])

        @pl.when(foreign)
        def _():
            r1(s, 1, 0, other_dev).wait_recv()
            pass_on(lambda yo: recv1[s, 0, yo].astype(jnp.float32))

    def stage_y(s):
        r1(s, 0, 0, ynb).wait_recv()
        send2[s, 1] = (keep[s, 1] + recv1[s, 0, 1].astype(jnp.float32)).astype(jnp.bfloat16)
        r2(s, 1, role, other_dev).start()
        mine = keep[s, 0] + recv1[s, 0, 0].astype(jnp.float32)

        @pl.when(home)
        def _():
            keep[s, 0] = mine

        @pl.when(foreign)
        def _():
            send2[s, 0] = mine.astype(jnp.bfloat16)
            r2(s, 0, 1, mine_dev).start()

    def place(s, v):
        out_ref[:, pl.ds(pl.multiple_of(s * cols, cols), cols)] = v.astype(jnp.bfloat16)

    def finish_x(s):
        r2(s, 0, 0, ynb).wait_recv()
        place(s, keep[s, y] + recv2[s, 0].astype(jnp.float32))

    def finish_y(s):
        r2(s, 0, 1, mine_dev).wait_recv()
        arrived = recv2[s, 1].astype(jnp.float32)

        @pl.when(home)
        def _():
            place(s, keep[s, 0] + arrived)

        @pl.when(foreign)
        def _():
            r2(s, 1, 0, other_dev).wait_recv()
            place(s, recv2[s, 0].astype(jnp.float32) + arrived)

    def produce(zz):
        wcopy(2, zz * X + 1 - c, 2).wait_recv()
        produce_x(zz * X)
        produce_y(zz * X + 1)

    def stage(zz):
        stage_x(zz * X)
        stage_y(zz * X + 1)

    def finish(zz):
        finish_x(zz * X)
        finish_y(zz * X + 1)

    produce(z)
    comm(2, 2, inner)
    for dist in range(1, Z):
        comm(2, dist, outer if dist < 3 else None)
        each_side(dist, produce)
        if dist == 1:
            stage(z)
        else:
            each_side(dist - 1, stage)
    each_side(Z - 1, stage)
    finish(z)
    for dist in range(1, Z):
        each_side(dist, finish)

    @pl.when(home)
    def _():
        lse_ref[...] = lse_buf[0]

    @pl.when(foreign)
    def _():
        swap(5, vs).wait_recv()
        lse_ref[...] = lse_buf[1]
        for part in range(TH):
            tok_d[part].wait_send()
            for cc in range(2):
                relay(cc, part).wait_send()
        for i in range(6):
            swap(i, sp).wait_send()

    for part in range(TH):
        tok_x[part].wait_send()
        tok_y[part].wait_send()

    @pl.when(has_next)
    def _():
        kv_next.wait_send()
        n_next.wait_send()

    @pl.when(has_prev)
    def _():
        kv_prev.wait_send()
        n_prev.wait_send()

    def drain(zz, carry):
        slot = zz * X + c
        for kind in range(3):
            for direction, cond in ((0, (zz >= z) & has_low), (1, (zz <= z) & has_high)):
                @pl.when(cond)
                def _(kind=kind, direction=direction):
                    wcopy(kind, slot, direction).wait_send()
            wcopy(kind, slot, 2).wait_send()
        sx, sy = zz * X, zz * X + 1
        r1(sx, 1, role, other_dev).wait_send()
        r1(sy, 0, 0, ynb).wait_send()
        r2(sx, 0, 0, ynb).wait_send()
        r2(sy, 1, role, other_dev).wait_send()

        @pl.when(foreign)
        def _():
            r1(sx, 0, 1, mine_dev).wait_send()
            r2(sy, 0, 1, mine_dev).wait_send()
        return carry

    lax.fori_loop(0, Z, drain, 0)


def fused(
    tokens, norm_gain, w_query, w_key, w_value, w_post_gate, w_pre_gate, w_conv_in,
    conv_taps, sink_logit, w_out_attn, w_out_conv,
):
    S, TP = lax.axis_size("sp"), lax.axis_size("tp")
    X = 2
    Z = S // X
    rows, width = tokens.shape
    depth, qw = w_query.shape
    cw = w_post_gate.shape[1]
    ow, cols = w_out_attn.shape
    heads = qw // HEAD_DIM
    kw = 2 * HEAD_DIM
    chunk = rows // TP
    bf, f32 = jnp.bfloat16, jnp.float32
    dma = pltpu.SemaphoreType.DMA
    return pl.pallas_call(
        functools.partial(fused_kernel, Z, X),
        out_shape=(
            jax.ShapeDtypeStruct((chunk, S * cols), bf),
            jax.ShapeDtypeStruct((heads, rows), f32),
        ),
        in_specs=[pl.BlockSpec(memory_space=pltpu.VMEM)] * 11 + [pl.BlockSpec(memory_space=pltpu.SMEM)],
        out_specs=(pl.BlockSpec(memory_space=pltpu.VMEM),) * 2,
        scratch_shapes=[
            pltpu.VMEM((rows, kw), f32),
            pltpu.VMEM((rows, kw), f32),
            pltpu.VMEM((TP, rows, width), bf),
            pltpu.VMEM((rows + 2 * EDGE, TP * width), bf),
            pltpu.VMEM((S + 1, depth, qw + kw), bf),
            pltpu.VMEM((S + 1, depth, 3 * cw), bf),
            pltpu.VMEM((S, ow + cw, cols), bf),
            pltpu.VMEM((rows, qw + kw), f32),
            pltpu.VMEM((rows + 2 * EDGE, 3 * cw), f32),
            pltpu.VMEM((rows, qw), bf),
            pltpu.VMEM((rows + 2 * WINDOW, kw), bf),
            pltpu.VMEM((rows + 16, cw), f32),
            pltpu.VMEM((rows, qw + cw), bf),
            pltpu.VMEM((2, -(-(3 + heads) // 8) * 8, cw), f32),
            pltpu.VMEM((2, heads, rows), f32),
            pltpu.VMEM((S, 2, chunk, cols), f32),
            pltpu.VMEM((S, 2, 2, chunk, cols), bf),
            pltpu.VMEM((S, 2, 2, chunk, cols), bf),
            pltpu.VMEM((S, 2, chunk, cols), bf),
            pltpu.VMEM((S, 2, chunk, cols), bf),
            dma((5, 2)), dma((TP, 2)),
            dma((3, 3, S)), dma((3, S)),
            dma((6,)), dma((6,)),
            dma((8,)),
            dma((S, 2)), dma((S, 2)), dma((S, 2)), dma((S, 2)),
            dma((3,)),
        ],
        compiler_params=pltpu.CompilerParams(
            collective_id=0, has_side_effects=True, vmem_limit_bytes=60 * 1024 * 1024
        ),
    )(
        tokens, norm_gain[None, :], w_query, w_key.T, w_value.T, w_post_gate, w_pre_gate, w_conv_in,
        w_out_attn, w_out_conv, conv_taps, sink_logit,
    )


def fits(
    tokens, norm_gain, w_query, w_key, w_value, w_post_gate, w_pre_gate, w_conv_in,
    conv_taps, sink_logit, w_out_attn, w_out_conv,
):
    S, TP = lax.axis_size("sp"), lax.axis_size("tp")
    return (
        TP == 4
        and S % 2 == 0
        and S >= 6
        and w_key.shape[1] == HEAD_DIM
        and w_query.shape[0] % 128 == 0
        and w_query.shape[1] % 128 == 0
        and w_post_gate.shape[1] % 128 == 0
        and w_out_attn.shape[1] % 128 == 0
        and tokens.shape[0] % (TP * WINDOW) == 0
        and tokens.shape[1] % 128 == 0
    )


def either(*args):
    return fused(*args) if fits(*args) else on_device(*args)


def solution(mesh):
    placed = (
        P("sp", "tp"),
        P(),
        P("sp", "tp"),
        P("sp", "tp"),
        P("sp", "tp"),
        P("sp", "tp"),
        P("sp", "tp"),
        P("sp", "tp"),
        P(None, "tp"),
        P("tp"),
        P("tp", "sp"),
        P("tp", "sp"),
    )
    return jax.shard_map(
        either,
        mesh=mesh,
        in_specs=placed,
        out_specs=(P(("sp", "tp"), None), P("tp", "sp")),
        check_vma=False,
    )
```

```python
import functools
import math

import jax
import jax.numpy as jnp
from jax import lax
from jax.experimental import pallas as pl
from jax.experimental.pallas import tpu as pltpu
from jax.sharding import PartitionSpec as P

MESH = pl.DeviceIdType.MESH

HEAD_DIM = 64
WINDOW = 128
GRID_W = 64
EDGE = 16


rope_base = 10000.0
norm_eps = 1e-06


def padded(block, sides, width):
    for axis, dim in sides:
        count = lax.axis_size(axis)
        forward = [(i, i + 1) for i in range(count - 1)]
        backward = [(target, source) for source, target in forward]
        low = lax.ppermute(
            lax.slice_in_dim(block, block.shape[dim] - width, None, axis=dim), axis, forward
        )
        high = lax.ppermute(lax.slice_in_dim(block, 0, width, axis=dim), axis, backward)
        block = jnp.concatenate([low, block, high], axis=dim)
    return block


def rotate_pair(values, angles):
    first_half, second_half = jnp.split(values, 2, axis=-1)
    cosine = jnp.cos(angles)[:, None, :]
    sine_part = jnp.sin(angles)[:, None, :]
    return jnp.concatenate(
        [
            first_half * cosine - second_half * sine_part,
            first_half * sine_part + second_half * cosine,
        ],
        axis=-1,
    )


def axial_rotate(values, positions):
    half_dim = values.shape[-1] // 2
    inv_freq = rope_base ** (-jnp.arange(0, half_dim, 2).astype(jnp.float32) / half_dim)
    row_angle = (positions // GRID_W).astype(jnp.float32)[:, None] * inv_freq
    col_angle = (positions % GRID_W).astype(jnp.float32)[:, None] * inv_freq
    row_part, col_part = jnp.split(values, 2, axis=-1)
    return jnp.concatenate(
        [rotate_pair(row_part, row_angle), rotate_pair(col_part, col_angle)], axis=-1
    )


def block_windows(source, rows_local, blocks):
    pieces = [
        source[step * WINDOW : step * WINDOW + rows_local].reshape(
            (blocks, WINDOW) + source.shape[1:]
        )
        for step in range(3)
    ]
    return jnp.concatenate(pieces, axis=1)


def on_device(
    tokens,
    norm_gain,
    w_query,
    w_key,
    w_value,
    w_post_gate,
    w_pre_gate,
    w_conv_in,
    conv_taps,
    sink_logit,
    w_out_attn,
    w_out_conv,
):
    whole = lax.all_gather(tokens, "tp", axis=1, tiled=True)
    rows_local = whole.shape[0]
    whole_float = whole.astype(jnp.float32)
    mean_square = jnp.mean(whole_float * whole_float, axis=1, keepdims=True)
    normed = (whole_float * lax.rsqrt(mean_square + norm_eps) * norm_gain).astype(jnp.bfloat16)
    col_widths = [
        w_query.shape[1],
        w_key.shape[1],
        w_value.shape[1],
        w_post_gate.shape[1],
        w_pre_gate.shape[1],
        w_conv_in.shape[1],
    ]
    joined = jnp.concatenate(
        (
            lax.all_gather(w_query, "sp", axis=0, tiled=True),
            lax.all_gather(w_key, "sp", axis=0, tiled=True),
            lax.all_gather(w_value, "sp", axis=0, tiled=True),
            lax.all_gather(w_post_gate, "sp", axis=0, tiled=True),
            lax.all_gather(w_pre_gate, "sp", axis=0, tiled=True),
            lax.all_gather(w_conv_in, "sp", axis=0, tiled=True),
        ),
        axis=1,
    )
    projected = jnp.dot(normed, joined, preferred_element_type=jnp.float32)
    bounds = []
    running = 0
    for col_width in col_widths[:-1]:
        running += col_width
        bounds.append(running)
    query_raw, key_raw, value_raw, post_gate, pre_gate, conv_input = jnp.split(
        projected, bounds, axis=1
    )
    offset = lax.axis_index("sp") * rows_local
    positions = offset + jnp.arange(rows_local, dtype=jnp.int32)
    local_heads = w_query.shape[1] // HEAD_DIM
    local_groups = w_key.shape[1] // HEAD_DIM
    group_size = local_heads // local_groups
    queries = axial_rotate(query_raw.reshape(rows_local, local_heads, HEAD_DIM), positions).astype(
        jnp.bfloat16
    )
    keys_rot = axial_rotate(key_raw.reshape(rows_local, local_groups, HEAD_DIM), positions).astype(
        jnp.bfloat16
    )
    key_value = jnp.concatenate(
        [keys_rot.reshape(rows_local, local_groups * HEAD_DIM), value_raw.astype(jnp.bfloat16)],
        axis=1,
    )
    mixed_input = (pre_gate * conv_input).astype(jnp.bfloat16)
    kv_padded = padded(key_value, (("sp", 0),), WINDOW)
    conv_padded = padded(mixed_input, (("sp", 0),), 1)
    conv_float = conv_padded.astype(jnp.float32)
    convolved = (
        conv_taps[0] * conv_float[:-2]
        + conv_taps[1] * conv_float[1:-1]
        + conv_taps[2] * conv_float[2:]
    )
    conv_out = (post_gate * convolved).astype(jnp.bfloat16)
    total_tokens = rows_local * lax.axis_size("sp")
    blocks = rows_local // WINDOW
    padded_rows = rows_local + 2 * WINDOW
    block_queries = queries.reshape(blocks, WINDOW, local_groups, group_size, HEAD_DIM)
    block_keys = block_windows(
        kv_padded[:, : local_groups * HEAD_DIM].reshape(padded_rows, local_groups, HEAD_DIM),
        rows_local,
        blocks,
    )
    block_values = block_windows(
        kv_padded[:, local_groups * HEAD_DIM :].reshape(padded_rows, local_groups, HEAD_DIM),
        rows_local,
        blocks,
    )
    scores = jnp.einsum(
        "nqkgd,nskd->nkgqs", block_queries, block_keys, preferred_element_type=jnp.float32
    ) * HEAD_DIM ** (-0.5)
    query_pos = positions.reshape(blocks, WINDOW)
    key_pos = (
        offset
        - WINDOW
        + (jnp.arange(blocks, dtype=jnp.int32) * WINDOW)[:, None]
        + jnp.arange(3 * WINDOW, dtype=jnp.int32)[None, :]
    )
    distance = key_pos[:, None, :] - query_pos[:, :, None]
    allowed = (
        (jnp.abs(distance) <= WINDOW)
        & (key_pos >= 0)[:, None, :]
        & (key_pos < total_tokens)[:, None, :]
    )
    scores = jnp.where(allowed[:, None, None], scores, -jnp.inf)
    sink_values = sink_logit.reshape(local_groups, group_size)[None, :, :, None]
    row_max = jnp.maximum(jnp.max(scores, axis=-1), sink_values)
    exp_scores = jnp.exp(scores - row_max[..., None])
    denominator = jnp.sum(exp_scores, axis=-1) + jnp.exp(sink_values - row_max)
    weights = (exp_scores / denominator[..., None]).astype(jnp.bfloat16)
    attended = (
        jnp.einsum("nkgqs,nskd->nqkgd", weights, block_values, preferred_element_type=jnp.float32)
        .astype(jnp.bfloat16)
        .reshape(rows_local, local_heads * HEAD_DIM)
    )
    log_sum = row_max + jnp.log(denominator)
    log_weight_sum = jnp.transpose(log_sum, (1, 2, 0, 3)).reshape(local_heads, rows_local)
    out_attn, out_conv = (
        lax.all_gather(w_out_attn, "sp", axis=1, tiled=True),
        lax.all_gather(w_out_conv, "sp", axis=1, tiled=True),
    )
    mixed = lax.psum_scatter(
        (
            jnp.dot(attended, out_attn, preferred_element_type=jnp.float32)
            + jnp.dot(conv_out, out_conv, preferred_element_type=jnp.float32)
        ).astype(jnp.bfloat16),
        "tp",
        scatter_dimension=0,
        tiled=True,
    )
    return (mixed, log_weight_sum)


def fused_kernel(
    Z, X,
    tok_ref, gain_ref, wq_ref, wk_ref, wv_ref, wpost_ref, wpre_ref, wcin_ref, oa_ref, oc_ref, taps_ref, sink_ref,
    out_ref, lse_ref,
    cos_ref, sin_ref, tok, normed, win_a, win_b, wo, acc_a, acc_b, qbuf, kvp, cf, ac, ext, lse_buf,
    keep, send1, recv1, send2, recv2,
    tok_send, tok_recv, wz_send, wd_send, w_recv, sw_send, sw_recv, halo_sem, r_send, r_recv, loc_sem,
):
    S = Z * X
    rows, width = tok_ref.shape
    depth = wq_ref.shape[0]
    ow, cols = oa_ref.shape
    qw = qbuf.shape[1]
    cw = cf.shape[1]
    kw = 2 * HEAD_DIM
    TP = tok.shape[0]
    chunk = rows // TP
    sp = lax.axis_index("sp")
    tp = lax.axis_index("tp")
    z, x = sp // X, sp % X
    c, y = tp % 2, tp // 2
    vs = z * X + c
    home, foreign = c == x, c != x
    role = jnp.where(home, 0, 1)
    sib = (sp, y * 2 + 1 - c)
    ynb = (sp, (1 - y) * 2 + c)
    yoth = (sp, (1 - y) * 2 + 1 - c)
    xnb = (z * X + 1 - x, tp)
    swp = (z * X + 1 - x, y * 2 + 1 - c)
    low, high = (sp - X, tp), (sp + X, tp)
    has_low, has_high = z > 0, z < Z - 1
    has_prev, has_next = vs > 0, vs < S - 1
    vn, vp = vs + 1, vs - 1 + S
    next_dev = ((vn // X) * X + x, y * 2 + vn % X)
    prev_dev = ((vp // X - Z) * X + x, y * 2 + vp % X)

    barrier = pltpu.get_barrier_semaphore()

    def greet(dev):
        pl.semaphore_signal(barrier, inc=1, device_id=dev, device_id_type=MESH)

    for dev in (sib, ynb, yoth, xnb, swp):
        greet(dev)
    peers = 5
    across_z = ((has_low, low), (has_high, high), (has_prev & (c == 0), prev_dev), (has_next & (c == 1), next_dev))
    for cond, dev in across_z:
        @pl.when(cond)
        def _(dev=dev):
            greet(dev)
        peers = peers + jnp.where(cond, 1, 0)

    pslot = jnp.where(home, sp, S)
    win_a[pslot, :, 0:qw] = wq_ref[...]
    kv_t = jnp.concatenate([wk_ref[...], wv_ref[...]], axis=0).astype(jnp.float32)
    win_a[pslot, :, qw:qw + kw] = jnp.transpose(kv_t).astype(jnp.bfloat16)
    for part, ref in enumerate((wpost_ref, wpre_ref, wcin_ref)):
        win_b[pslot, :, part * cw:(part + 1) * cw] = ref[...]
    heads = qw // HEAD_DIM
    ext[0] = jnp.zeros(ext.shape[1:], jnp.float32)
    ext[0, 0:3, :] = taps_ref[...]
    for h in range(heads):
        ext[0, 3 + h:4 + h, :] = jnp.full((1, cw), sink_ref[h], jnp.float32)

    pl.semaphore_wait(barrier, peers)

    def remote(src, dst, ssem, rsem, dev):
        return pltpu.make_async_remote_copy(
            src_ref=src, dst_ref=dst, send_sem=ssem, recv_sem=rsem,
            device_id=dev, device_id_type=MESH,
        )

    bufs = (win_a, win_b, wo)
    targets = (low, high, sib)

    def wcopy(kind, slot, direction):
        block = bufs[kind].at[slot]
        ssem = (wz_send, wz_send, wd_send)[direction].at[kind]
        return remote(block, block, ssem, w_recv.at[kind, slot], targets[direction])

    up_light = 2 * z + 1 < Z
    inner = has_low & has_high
    outer = jnp.logical_not(inner)

    def own_far(kind):
        for direction, cond in ((0, has_low & jnp.logical_not(up_light)), (1, has_high & up_light)):
            @pl.when(cond)
            def _(direction=direction):
                wcopy(kind, vs, direction).start()
        wcopy(kind, vs, 2).start()

    def own_near(kind):
        for direction, cond in ((0, has_low & up_light), (1, has_high & jnp.logical_not(up_light))):
            @pl.when(cond)
            def _(direction=direction):
                wcopy(kind, vs, direction).start()

    def own_start(kind):
        own_near(kind)
        own_far(kind)

    def swap(i, slot):
        src, dst = (
            (win_a.at[S], win_a.at[slot]),
            (win_b.at[S], win_b.at[slot]),
            (oa_ref, wo.at[slot, pl.ds(0, ow)]),
            (oc_ref, wo.at[slot, pl.ds(ow, cw)]),
            (ext.at[0], ext.at[1]),
            (lse_buf.at[0], lse_buf.at[1]),
        )[i]
        return remote(src, dst, sw_send.at[i], sw_recv.at[i], swp)

    TH = 2
    part_rows = rows // TH

    def tok_copy(src, q, i, part, dev):
        r = pl.ds(part * part_rows, part_rows)
        return remote(src.at[r], tok.at[q, r], tok_send.at[i], tok_recv.at[q, part], dev)

    tok_d = [tok_copy(tok_ref, tp, 1, part, sib) for part in range(TH)]
    tok_y = [tok_copy(tok_ref, tp, 0, part, (sp, (1 - y) * 2 + x)) for part in range(TH)]
    tok_x = [tok_copy(tok_ref, tp, 0, part, (z * X + 1 - x, y * 2 + x)) for part in range(TH)]
    local = [
        pltpu.make_async_copy(tok_ref, tok.at[tp], loc_sem.at[0]),
        pltpu.make_async_copy(oa_ref, wo.at[vs, pl.ds(0, ow)], loc_sem.at[1]),
        pltpu.make_async_copy(oc_ref, wo.at[vs, pl.ds(ow, cw)], loc_sem.at[2]),
    ]

    @pl.when(home)
    def _():
        own_start(0)
        own_start(1)

    @pl.when(foreign)
    def _():
        swap(0, sp).start()

    for part in range(TH):
        tok_x[part].start()
        tok_y[part].start()

    @pl.when(foreign)
    def _():
        for copy in tok_d:
            copy.start()
        for i in (1, 4, 2, 3):
            swap(i, sp).start()

    @pl.when(home)
    def _():
        for copy in local:
            copy.start()

    MB = 128
    quarter = HEAD_DIM // 4

    def angles(i, carry):
        r = pl.ds(pl.multiple_of(i * MB, MB), MB)
        pos = vs * rows + i * MB + lax.broadcasted_iota(jnp.int32, (MB, kw), 0)
        lane = lax.broadcasted_iota(jnp.int32, (MB, kw), 1) % HEAD_DIM
        freq = jnp.exp((lane % quarter).astype(jnp.float32) * (-4.0 / HEAD_DIM * math.log(rope_base)))
        index = jnp.where(lane >= 2 * quarter, pos % GRID_W, pos // GRID_W)
        angle = index.astype(jnp.float32) * freq
        cos_ref[r, :] = jnp.cos(angle)
        sin_ref[r, :] = jnp.where(lane % (2 * quarter) < quarter, -1.0, 1.0) * jnp.sin(angle)
        return carry

    def comm(kind, dist, only=None):
        for up in (0, 1):
            zz = z + dist * (2 * up - 1)
            valid = (zz >= 0) & (zz < Z)
            if only is not None:
                valid = valid & only

            @pl.when(valid)
            def _(zz=zz, up=up):
                slot = zz * X + c
                wcopy(kind, slot, 2).wait_recv()

                @pl.when(has_low if up else has_high)
                def _():
                    wcopy(kind, slot, 0 if up else 1).start()
                wcopy(kind, slot, 2).start()

    def relay(cc, part):
        q = y * 2 + cc
        return tok_copy(tok.at[q], q, 1, part, ynb)

    def tok_wait(q, part):
        tok_copy(tok.at[q], q, 0, part, ynb).wait_recv()

    RB = 64

    def norm_rows(i, carry):
        r = pl.ds(pl.multiple_of(i * RB, RB), RB)
        total = jnp.zeros((RB, 1), jnp.float32)
        for t in range(TP):
            v = tok[t, r, :].astype(jnp.float32)
            total += jnp.sum(v * v, axis=1, keepdims=True)
        scale = lax.rsqrt(total / (TP * width) + norm_eps)
        for t in range(TP):
            v = tok[t, r, :].astype(jnp.float32)
            g = gain_ref[:, t * width:(t + 1) * width]
            normed[r, t * width:(t + 1) * width] = (v * scale * g).astype(jnp.bfloat16)
        return carry

    pdepth = X * depth

    def project(kind, zz, first):
        win, acc = ((win_a, acc_a), (win_b, acc_b))[kind]
        n = acc.shape[1]
        wcopy(kind, zz * X + 1 - c, 2).wait_recv()

        pb = acc.shape[0] // 2

        def body(i, carry):
            r = pl.ds(pl.multiple_of(i * pb, 16), pb)
            k = pl.ds(pl.multiple_of(zz * pdepth, pdepth), pdepth)
            weight = win[pl.ds(zz * X, X)].reshape(pdepth, n)
            prod = jnp.dot(normed[r, k], weight, preferred_element_type=jnp.float32)
            if first:
                acc[r, :] = prod
            else:
                acc[r, :] += prod
            return carry
        lax.fori_loop(0, 2, body, 0)

    def each_side(dist, fn):
        def step(side, carry):
            zz = z + dist * (2 * side - 1)

            @pl.when((zz >= 0) & (zz < Z))
            def _():
                fn(zz)
            return carry
        lax.fori_loop(0, 2, step, 0)

    def project_at(kind, dist):
        each_side(dist, lambda zz: project(kind, zz, False))

    def halo(i, src, dst, dev):
        return remote(src, dst, halo_sem.at[2 * i], halo_sem.at[2 * i + 1], dev)

    kv_next = halo(0, kvp.at[pl.ds(rows, WINDOW)], kvp.at[pl.ds(0, WINDOW)], next_dev)
    kv_prev = halo(1, kvp.at[pl.ds(WINDOW, WINDOW)], kvp.at[pl.ds(WINDOW + rows, WINDOW)], prev_dev)
    n_next = halo(2, normed.at[pl.ds(rows - EDGE, EDGE)], normed.at[pl.ds(rows, EDGE)], next_dev)
    n_prev = halo(3, normed.at[pl.ds(0, EDGE)], normed.at[pl.ds(rows + EDGE, EDGE)], prev_dev)

    lax.fori_loop(0, rows // MB, angles, 0)

    @pl.when(foreign)
    def _():
        swap(0, vs).wait_recv()
        own_start(0)
        for cc in range(2):
            tok_wait(y * 2 + cc, 0)
            relay(cc, 0).start()

    comm(0, 1)

    @pl.when(foreign)
    def _():
        for cc in range(2):
            tok_wait(y * 2 + cc, 1)
            relay(cc, 1).start()

    @pl.when(home)
    def _():
        comm(1, 1)
    comm(0, 2)

    @pl.when(foreign)
    def _():
        swap(1, vs).wait_recv()
        own_start(1)
        swap(4, vs).wait_recv()

    @pl.when(home)
    def _():
        for copy in local:
            copy.wait()
        own_far(2)
        for part in range(TH):
            tok_wait(y * 2 + 1 - c, part)
    for part in range(TH):
        for cc in range(2):
            tok_wait((1 - y) * 2 + cc, part)
        lax.fori_loop(part * (part_rows // RB), (part + 1) * (part_rows // RB), norm_rows, 0)

    @pl.when(has_next)
    def _():
        n_next.start()

    @pl.when(has_prev)
    def _():
        n_prev.start()

    @pl.when(foreign)
    def _():
        comm(1, 1, inner)
        for i in (2, 3):
            swap(i, vs).wait_recv()
        own_far(2)

    for dist in range(3, Z):
        comm(0, dist)
    project(0, z, True)
    project_at(0, 1)

    @pl.when(home)
    def _():
        comm(1, 2)

    for dist in range(2, Z):
        project_at(0, dist)

    @pl.when(foreign)
    def _():
        comm(1, 1, outer)

    def turned(v, cosv, sinv):
        lane = lax.broadcasted_iota(jnp.int32, v.shape, 1)
        partner = jnp.where(
            lane % (2 * quarter) < quarter,
            pltpu.roll(v, v.shape[1] - quarter, 1),
            pltpu.roll(v, quarter, 1),
        )
        return v * cosv + partner * sinv

    def k_rows(i, carry):
        r = pl.ds(pl.multiple_of(i * MB, MB), MB)
        v = acc_a[r, qw:qw + kw]
        lane = lax.broadcasted_iota(jnp.int32, v.shape, 1)
        kv = jnp.where(lane < HEAD_DIM, turned(v, cos_ref[r, :], sin_ref[r, :]), v)
        kvp[pl.ds(pl.multiple_of(WINDOW + i * MB, MB), MB), :] = kv.astype(jnp.bfloat16)
        return carry

    lax.fori_loop(0, rows // MB, k_rows, 0)

    @pl.when(has_next)
    def _():
        kv_next.start()

    @pl.when(has_prev)
    def _():
        kv_prev.start()

    def q_rows(i, carry):
        r = pl.ds(pl.multiple_of(i * MB, MB), MB)
        for k in range(qw // kw):
            qbuf[r, k * kw:(k + 1) * kw] = turned(
                acc_a[r, k * kw:(k + 1) * kw], cos_ref[r, :], sin_ref[r, :]
            ).astype(jnp.bfloat16)
        return carry

    lax.fori_loop(0, rows // MB, q_rows, 0)

    K3 = 3 * WINDOW
    total_tokens = rows * S

    def attend(b, carry):
        r = pl.ds(pl.multiple_of(b * WINDOW, WINDOW), WINDOW)
        kv = kvp[pl.ds(pl.multiple_of(b * WINDOW, WINDOW), K3), :].astype(jnp.float32)
        lane = lax.broadcasted_iota(jnp.int32, (K3, kw), 1)
        swapped = pltpu.roll(kv, HEAD_DIM, 1)
        kk = jnp.where(lane < HEAD_DIM, kv, swapped).astype(jnp.bfloat16)
        vv = jnp.where(lane < HEAD_DIM, swapped, kv).astype(jnp.bfloat16)
        k_half = [jnp.where(lane < HEAD_DIM, kk, 0), jnp.where(lane < HEAD_DIM, 0, kk)]
        v_half = [jnp.where(lane < HEAD_DIM, vv, 0), jnp.where(lane < HEAD_DIM, 0, vv)]
        qi = lax.broadcasted_iota(jnp.int32, (WINDOW, K3), 0)
        ki = lax.broadcasted_iota(jnp.int32, (WINDOW, K3), 1)
        first = vs * rows + b * WINDOW - WINDOW
        allowed = (ki >= qi) & (ki <= qi + 2 * WINDOW) & (ki + first >= 0) & (ki + first < total_tokens)
        lse_lane = lax.broadcasted_iota(jnp.int32, (WINDOW, WINDOW), 1)
        lse_all = jnp.zeros((WINDOW, WINDOW), jnp.float32)
        for pair in range(heads // 2):
            q = qbuf[r, pair * kw:(pair + 1) * kw]
            total = jnp.zeros((WINDOW, kw), jnp.float32)
            for side in range(2):
                h = pair * 2 + side
                s = lax.dot_general(
                    q, k_half[side], (((1,), (1,)), ((), ())), preferred_element_type=jnp.float32
                ) * HEAD_DIM ** (-0.5)
                s = jnp.where(allowed, s, -jnp.inf)
                sink = ext[role, 3 + h:4 + h, 0:WINDOW]
                top = jnp.maximum(jnp.max(s, axis=1, keepdims=True), sink)
                e = jnp.exp(s - jnp.concatenate([top] * 3, axis=1))
                den = jnp.sum(e, axis=1, keepdims=True) + jnp.exp(sink - top)
                w = (e * jnp.concatenate([1.0 / den] * 3, axis=1)).astype(jnp.bfloat16)
                total += jnp.dot(w, v_half[side], preferred_element_type=jnp.float32)
                lse_all = jnp.where(lse_lane == h, top + jnp.log(den), lse_all)
            ac[r, pair * kw:(pair + 1) * kw] = total.astype(jnp.bfloat16)
        lse_buf[0, :, r] = jnp.transpose(lse_all)[0:heads, :]
        return carry

    blocks = rows // WINDOW
    zero_kv = jnp.zeros((WINDOW, kw), jnp.bfloat16)

    def prev_ready():
        @pl.when(has_prev)
        def _():
            kv_next.wait_recv()

        @pl.when(jnp.logical_not(has_prev))
        def _():
            kvp[0:WINDOW, :] = zero_kv

    def next_ready():
        @pl.when(has_next)
        def _():
            kv_prev.wait_recv()

        @pl.when(jnp.logical_not(has_next))
        def _():
            kvp[WINDOW + rows:, :] = zero_kv

    def edge_ready(at_start):
        @pl.when(at_start)
        def _():
            prev_ready()

        @pl.when(jnp.logical_not(at_start))
        def _():
            next_ready()

    def attend_from(i, carry):
        return attend((1 - c + i) % blocks, carry)

    def b_ready():
        @pl.when(has_prev)
        def _():
            n_next.wait_recv()

        @pl.when(has_next)
        def _():
            n_prev.wait_recv()

        @pl.when(jnp.logical_not(has_prev))
        def _():
            normed[rows:rows + EDGE, :] = jnp.zeros((EDGE, TP * width), jnp.bfloat16)

        @pl.when(jnp.logical_not(has_next))
        def _():
            normed[rows + EDGE:, :] = jnp.zeros((EDGE, TP * width), jnp.bfloat16)

    @pl.when(home)
    def _():
        for dist in range(3, Z):
            comm(1, dist)

    edge_ready(c == 1)
    lax.fori_loop(0, blocks // 2, attend_from, 0)
    b_ready()
    project(1, z, True)

    @pl.when(home)
    def _():
        own_near(2)

    @pl.when(foreign)
    def _():
        comm(1, 2)
        own_near(2)
    lax.fori_loop(blocks // 2, blocks - 1, attend_from, 0)
    edge_ready(c == 0)
    lax.fori_loop(blocks - 1, blocks, attend_from, 0)

    @pl.when(foreign)
    def _():
        swap(5, sp).start()

    project_at(1, 1)
    project_at(1, 2)

    @pl.when(foreign)
    def _():
        for dist in range(3, Z):
            comm(1, dist)
    for dist in range(3, Z):
        project_at(1, dist)
    comm(2, 1, inner)

    def gated(lo, n):
        return (acc_b[lo:lo + n, cw:2 * cw] * acc_b[lo:lo + n, 2 * cw:3 * cw]).astype(jnp.bfloat16)

    for i in range(rows // MB):
        cf[8 + i * MB:8 + (i + 1) * MB, :] = gated(i * MB, MB).astype(jnp.float32)
    edge = gated(rows, 2 * EDGE).astype(jnp.float32)
    cf[0:8, :] = edge[EDGE - 8:EDGE, :]
    cf[8 + rows:16 + rows, :] = edge[EDGE:EDGE + 8, :]

    taps = [ext[role, t:t + 1, :] for t in range(3)]
    for i in range(rows // MB):
        a = 8 + i * MB
        conv = (
            taps[0] * cf[a - 1:a - 1 + MB, :]
            + taps[1] * cf[a:a + MB, :]
            + taps[2] * cf[a + 1:a + 1 + MB, :]
        )
        ac[i * MB:(i + 1) * MB, qw:qw + cw] = (acc_b[i * MB:(i + 1) * MB, 0:cw] * conv).astype(jnp.bfloat16)

    mine_dev = (z * X + c, y * 2 + c)
    other_dev = (z * X + c, y * 2 + 1 - c)

    def r1(s, src, dst, dev, extra=0):
        return remote(send1.at[s, src], recv1.at[s, dst], r_send.at[extra], r_recv.at[s, dst], dev)

    def r2(s, src, dst, dev, sem, extra=0):
        return remote(send2.at[s, src], recv2.at[s, dst], r_send.at[2 + extra], r_recv.at[s, sem], dev)

    def out_dot(s, yo, m):
        co = c if m == 0 else 1 - c
        r = pl.ds(pl.multiple_of((2 * yo + co) * chunk, chunk), chunk)
        return jnp.dot(ac[r, :], wo[s], preferred_element_type=jnp.float32)

    def produce_x(s):
        for yo in range(2):
            for m in (1, 0):
                v = out_dot(s, yo, m)
                if m == 0:
                    keep[s, yo] = v
                send1[s, m, yo] = v.astype(jnp.bfloat16)
        r1(s, 1, role, other_dev).start()

        @pl.when(foreign)
        def _():
            r1(s, 0, 1, mine_dev, 1).start()

    def produce_y(s):
        for m in range(2):
            send1[s, 0, m] = out_dot(s, 1 - y, m).astype(jnp.bfloat16)
        r1(s, 0, 0, ynb).start()
        for m in range(2):
            keep[s, m] = out_dot(s, y, m)

    def stage_x(s):
        r1(s, 0, 1, mine_dev).wait_recv()

        def pass_on(base):
            send2[s, 0] = (base(1 - y) + recv1[s, 1, 1 - y].astype(jnp.float32)).astype(jnp.bfloat16)
            r2(s, 0, 0, ynb, 2).start()
            keep[s, y] = base(y) + recv1[s, 1, y].astype(jnp.float32)

        @pl.when(home)
        def _():
            pass_on(lambda yo: keep[s, yo])

        @pl.when(foreign)
        def _():
            r1(s, 1, 0, other_dev).wait_recv()
            pass_on(lambda yo: recv1[s, 0, yo].astype(jnp.float32))

    def stage_y(s):
        r1(s, 0, 0, ynb).wait_recv()
        send2[s, 1] = (keep[s, 1] + recv1[s, 0, 1].astype(jnp.float32)).astype(jnp.bfloat16)
        r2(s, 1, role, other_dev, 1 + role).start()
        mine = keep[s, 0] + recv1[s, 0, 0].astype(jnp.float32)

        @pl.when(home)
        def _():
            keep[s, 0] = mine

        @pl.when(foreign)
        def _():
            send2[s, 0] = mine.astype(jnp.bfloat16)
            r2(s, 0, 1, mine_dev, 2, 1).start()

    def place(s, v):
        out_ref[:, pl.ds(pl.multiple_of(s * cols, cols), cols)] = v.astype(jnp.bfloat16)

    def finish_x(s):
        r2(s, 0, 0, ynb, 2).wait_recv()
        place(s, keep[s, y] + recv2[s, 0].astype(jnp.float32))

    def finish_y(s):
        r2(s, 0, 1, mine_dev, 2).wait_recv()
        arrived = recv2[s, 1].astype(jnp.float32)

        @pl.when(home)
        def _():
            place(s, keep[s, 0] + arrived)

        @pl.when(foreign)
        def _():
            r2(s, 1, 0, other_dev, 1).wait_recv()
            place(s, recv2[s, 0].astype(jnp.float32) + arrived)

    def produce(zz):
        wcopy(2, zz * X + 1 - c, 2).wait_recv()
        produce_x(zz * X)
        produce_y(zz * X + 1)

    def stage(zz):
        stage_x(zz * X)
        stage_y(zz * X + 1)

    def finish(zz):
        finish_x(zz * X)
        finish_y(zz * X + 1)

    produce(z)
    for dist in range(1, Z):
        comm(2, dist, outer if dist < 3 else None)
        each_side(dist, produce)
        if dist == 1:
            comm(2, 2, inner)
        if dist == 1:
            stage(z)
        else:
            each_side(dist - 1, stage)
    each_side(Z - 1, stage)
    finish(z)
    for dist in range(1, Z):
        each_side(dist, finish)

    @pl.when(home)
    def _():
        lse_ref[...] = lse_buf[0]

    @pl.when(foreign)
    def _():
        swap(5, vs).wait_recv()
        lse_ref[...] = lse_buf[1]
        for i in range(6):
            swap(i, sp).wait_send()

    @pl.when(has_next)
    def _():
        kv_next.wait_send()
        n_next.wait_send()

    @pl.when(has_prev)
    def _():
        kv_prev.wait_send()
        n_prev.wait_send()

    def sent(block, sem):
        remote(block, block, sem, sem, sib).wait_send()

    sent(tok.at[pl.ds(0, 2)], tok_send.at[0])
    for kind in range(3):
        sent(bufs[kind].at[pl.ds(0, Z)], wd_send.at[kind])

        @pl.when(inner)
        def _(kind=kind):
            sent(bufs[kind].at[pl.ds(0, Z + 1)], wz_send.at[kind])

        @pl.when(outer)
        def _(kind=kind):
            sent(bufs[kind].at[pl.ds(0, 1)], wz_send.at[kind])
    sent(send1.at[pl.ds(0, Z)], r_send.at[0])
    sent(send2.at[pl.ds(0, Z)], r_send.at[2])

    @pl.when(foreign)
    def _():
        sent(tok.at[pl.ds(0, 3)], tok_send.at[1])
        sent(send1.at[pl.ds(0, Z), 0], r_send.at[1])
        sent(send2.at[pl.ds(0, Z), 0], r_send.at[3])


def fused(
    tokens, norm_gain, w_query, w_key, w_value, w_post_gate, w_pre_gate, w_conv_in,
    conv_taps, sink_logit, w_out_attn, w_out_conv,
):
    S, TP = lax.axis_size("sp"), lax.axis_size("tp")
    X = 2
    Z = S // X
    rows, width = tokens.shape
    depth, qw = w_query.shape
    cw = w_post_gate.shape[1]
    ow, cols = w_out_attn.shape
    heads = qw // HEAD_DIM
    kw = 2 * HEAD_DIM
    chunk = rows // TP
    bf, f32 = jnp.bfloat16, jnp.float32
    dma = pltpu.SemaphoreType.DMA
    return pl.pallas_call(
        functools.partial(fused_kernel, Z, X),
        out_shape=(
            pltpu.VMEM((chunk, S * cols), bf),
            pltpu.VMEM((heads, rows), f32),
        ),
        in_specs=[pl.BlockSpec(memory_space=pltpu.VMEM)] * 11 + [pl.BlockSpec(memory_space=pltpu.SMEM)],
        out_specs=(pl.BlockSpec(memory_space=pltpu.VMEM),) * 2,
        scratch_shapes=[
            pltpu.VMEM((rows, kw), f32),
            pltpu.VMEM((rows, kw), f32),
            pltpu.VMEM((TP, rows, width), bf),
            pltpu.VMEM((rows + 2 * EDGE, TP * width), bf),
            pltpu.VMEM((S + 1, depth, qw + kw), bf),
            pltpu.VMEM((S + 1, depth, 3 * cw), bf),
            pltpu.VMEM((S, ow + cw, cols), bf),
            pltpu.VMEM((rows, qw + kw), f32),
            pltpu.VMEM((rows + 2 * EDGE, 3 * cw), f32),
            pltpu.VMEM((rows, qw), bf),
            pltpu.VMEM((rows + 2 * WINDOW, kw), bf),
            pltpu.VMEM((rows + 16, cw), f32),
            pltpu.VMEM((rows, qw + cw), bf),
            pltpu.VMEM((2, -(-(3 + heads) // 8) * 8, cw), f32),
            pltpu.VMEM((2, heads, rows), f32),
            pltpu.VMEM((S, 2, chunk, cols), f32),
            pltpu.VMEM((S, 2, 2, chunk, cols), bf),
            pltpu.VMEM((S, 2, 2, chunk, cols), bf),
            pltpu.VMEM((S, 2, chunk, cols), bf),
            pltpu.VMEM((S, 2, chunk, cols), bf),
            dma((2,)), dma((TP, 2)),
            dma((3,)), dma((3,)), dma((3, S)),
            dma((6,)), dma((6,)),
            dma((8,)),
            dma((4,)), dma((S, 3)),
            dma((3,)),
        ],
        compiler_params=pltpu.CompilerParams(
            collective_id=0, has_side_effects=True, vmem_limit_bytes=60 * 1024 * 1024
        ),
    )(
        tokens, norm_gain[None, :], w_query, w_key.T, w_value.T, w_post_gate, w_pre_gate, w_conv_in,
        w_out_attn, w_out_conv, conv_taps, sink_logit,
    )


def fits(
    tokens, norm_gain, w_query, w_key, w_value, w_post_gate, w_pre_gate, w_conv_in,
    conv_taps, sink_logit, w_out_attn, w_out_conv,
):
    S, TP = lax.axis_size("sp"), lax.axis_size("tp")
    return (
        TP == 4
        and S % 2 == 0
        and S >= 6
        and w_key.shape[1] == HEAD_DIM
        and w_query.shape[0] % 128 == 0
        and w_query.shape[1] % 128 == 0
        and w_post_gate.shape[1] % 128 == 0
        and w_out_attn.shape[1] % 128 == 0
        and tokens.shape[0] % (TP * WINDOW) == 0
        and tokens.shape[1] % 128 == 0
    )


def either(*args):
    return fused(*args) if fits(*args) else on_device(*args)


def solution(mesh):
    placed = (
        P("sp", "tp"),
        P(),
        P("sp", "tp"),
        P("sp", "tp"),
        P("sp", "tp"),
        P("sp", "tp"),
        P("sp", "tp"),
        P("sp", "tp"),
        P(None, "tp"),
        P("tp"),
        P("tp", "sp"),
        P("tp", "sp"),
    )
    return jax.shard_map(
        either,
        mesh=mesh,
        in_specs=placed,
        out_specs=(P(("sp", "tp"), None), P("tp", "sp")),
        check_vma=False,
    )
```

```python
import functools
import math

import jax
import jax.numpy as jnp
from jax import lax
from jax.experimental import pallas as pl
from jax.experimental.pallas import tpu as pltpu
from jax.sharding import PartitionSpec as P

MESH = pl.DeviceIdType.MESH

HEAD_DIM = 64
WINDOW = 128
GRID_W = 64
EDGE = 16
NEAR = 8


rope_base = 10000.0
norm_eps = 1e-06


def padded(block, sides, width):
    for axis, dim in sides:
        count = lax.axis_size(axis)
        forward = [(i, i + 1) for i in range(count - 1)]
        backward = [(target, source) for source, target in forward]
        low = lax.ppermute(
            lax.slice_in_dim(block, block.shape[dim] - width, None, axis=dim), axis, forward
        )
        high = lax.ppermute(lax.slice_in_dim(block, 0, width, axis=dim), axis, backward)
        block = jnp.concatenate([low, block, high], axis=dim)
    return block


def rotate_pair(values, angles):
    first_half, second_half = jnp.split(values, 2, axis=-1)
    cosine = jnp.cos(angles)[:, None, :]
    sine_part = jnp.sin(angles)[:, None, :]
    return jnp.concatenate(
        [
            first_half * cosine - second_half * sine_part,
            first_half * sine_part + second_half * cosine,
        ],
        axis=-1,
    )


def axial_rotate(values, positions):
    half_dim = values.shape[-1] // 2
    inv_freq = rope_base ** (-jnp.arange(0, half_dim, 2).astype(jnp.float32) / half_dim)
    row_angle = (positions // GRID_W).astype(jnp.float32)[:, None] * inv_freq
    col_angle = (positions % GRID_W).astype(jnp.float32)[:, None] * inv_freq
    row_part, col_part = jnp.split(values, 2, axis=-1)
    return jnp.concatenate(
        [rotate_pair(row_part, row_angle), rotate_pair(col_part, col_angle)], axis=-1
    )


def block_windows(source, rows_local, blocks):
    pieces = [
        source[step * WINDOW : step * WINDOW + rows_local].reshape(
            (blocks, WINDOW) + source.shape[1:]
        )
        for step in range(3)
    ]
    return jnp.concatenate(pieces, axis=1)


def on_device(
    tokens,
    norm_gain,
    w_query,
    w_key,
    w_value,
    w_post_gate,
    w_pre_gate,
    w_conv_in,
    conv_taps,
    sink_logit,
    w_out_attn,
    w_out_conv,
):
    whole = lax.all_gather(tokens, "tp", axis=1, tiled=True)
    rows_local = whole.shape[0]
    whole_float = whole.astype(jnp.float32)
    mean_square = jnp.mean(whole_float * whole_float, axis=1, keepdims=True)
    normed = (whole_float * lax.rsqrt(mean_square + norm_eps) * norm_gain).astype(jnp.bfloat16)
    col_widths = [
        w_query.shape[1],
        w_key.shape[1],
        w_value.shape[1],
        w_post_gate.shape[1],
        w_pre_gate.shape[1],
        w_conv_in.shape[1],
    ]
    joined = jnp.concatenate(
        (
            lax.all_gather(w_query, "sp", axis=0, tiled=True),
            lax.all_gather(w_key, "sp", axis=0, tiled=True),
            lax.all_gather(w_value, "sp", axis=0, tiled=True),
            lax.all_gather(w_post_gate, "sp", axis=0, tiled=True),
            lax.all_gather(w_pre_gate, "sp", axis=0, tiled=True),
            lax.all_gather(w_conv_in, "sp", axis=0, tiled=True),
        ),
        axis=1,
    )
    projected = jnp.dot(normed, joined, preferred_element_type=jnp.float32)
    bounds = []
    running = 0
    for col_width in col_widths[:-1]:
        running += col_width
        bounds.append(running)
    query_raw, key_raw, value_raw, post_gate, pre_gate, conv_input = jnp.split(
        projected, bounds, axis=1
    )
    offset = lax.axis_index("sp") * rows_local
    positions = offset + jnp.arange(rows_local, dtype=jnp.int32)
    local_heads = w_query.shape[1] // HEAD_DIM
    local_groups = w_key.shape[1] // HEAD_DIM
    group_size = local_heads // local_groups
    queries = axial_rotate(query_raw.reshape(rows_local, local_heads, HEAD_DIM), positions).astype(
        jnp.bfloat16
    )
    keys_rot = axial_rotate(key_raw.reshape(rows_local, local_groups, HEAD_DIM), positions).astype(
        jnp.bfloat16
    )
    key_value = jnp.concatenate(
        [keys_rot.reshape(rows_local, local_groups * HEAD_DIM), value_raw.astype(jnp.bfloat16)],
        axis=1,
    )
    mixed_input = (pre_gate * conv_input).astype(jnp.bfloat16)
    kv_padded = padded(key_value, (("sp", 0),), WINDOW)
    conv_padded = padded(mixed_input, (("sp", 0),), 1)
    conv_float = conv_padded.astype(jnp.float32)
    convolved = (
        conv_taps[0] * conv_float[:-2]
        + conv_taps[1] * conv_float[1:-1]
        + conv_taps[2] * conv_float[2:]
    )
    conv_out = (post_gate * convolved).astype(jnp.bfloat16)
    total_tokens = rows_local * lax.axis_size("sp")
    blocks = rows_local // WINDOW
    padded_rows = rows_local + 2 * WINDOW
    block_queries = queries.reshape(blocks, WINDOW, local_groups, group_size, HEAD_DIM)
    block_keys = block_windows(
        kv_padded[:, : local_groups * HEAD_DIM].reshape(padded_rows, local_groups, HEAD_DIM),
        rows_local,
        blocks,
    )
    block_values = block_windows(
        kv_padded[:, local_groups * HEAD_DIM :].reshape(padded_rows, local_groups, HEAD_DIM),
        rows_local,
        blocks,
    )
    scores = jnp.einsum(
        "nqkgd,nskd->nkgqs", block_queries, block_keys, preferred_element_type=jnp.float32
    ) * HEAD_DIM ** (-0.5)
    query_pos = positions.reshape(blocks, WINDOW)
    key_pos = (
        offset
        - WINDOW
        + (jnp.arange(blocks, dtype=jnp.int32) * WINDOW)[:, None]
        + jnp.arange(3 * WINDOW, dtype=jnp.int32)[None, :]
    )
    distance = key_pos[:, None, :] - query_pos[:, :, None]
    allowed = (
        (jnp.abs(distance) <= WINDOW)
        & (key_pos >= 0)[:, None, :]
        & (key_pos < total_tokens)[:, None, :]
    )
    scores = jnp.where(allowed[:, None, None], scores, -jnp.inf)
    sink_values = sink_logit.reshape(local_groups, group_size)[None, :, :, None]
    row_max = jnp.maximum(jnp.max(scores, axis=-1), sink_values)
    exp_scores = jnp.exp(scores - row_max[..., None])
    denominator = jnp.sum(exp_scores, axis=-1) + jnp.exp(sink_values - row_max)
    weights = (exp_scores / denominator[..., None]).astype(jnp.bfloat16)
    attended = (
        jnp.einsum("nkgqs,nskd->nqkgd", weights, block_values, preferred_element_type=jnp.float32)
        .astype(jnp.bfloat16)
        .reshape(rows_local, local_heads * HEAD_DIM)
    )
    log_sum = row_max + jnp.log(denominator)
    log_weight_sum = jnp.transpose(log_sum, (1, 2, 0, 3)).reshape(local_heads, rows_local)
    out_attn, out_conv = (
        lax.all_gather(w_out_attn, "sp", axis=1, tiled=True),
        lax.all_gather(w_out_conv, "sp", axis=1, tiled=True),
    )
    mixed = lax.psum_scatter(
        (
            jnp.dot(attended, out_attn, preferred_element_type=jnp.float32)
            + jnp.dot(conv_out, out_conv, preferred_element_type=jnp.float32)
        ).astype(jnp.bfloat16),
        "tp",
        scatter_dimension=0,
        tiled=True,
    )
    return (mixed, log_weight_sum)


def fused_kernel(
    Z, X,
    tok_ref, gain_ref, wq_ref, wk_ref, wv_ref, wpost_ref, wpre_ref, wcin_ref, oa_ref, oc_ref, taps_ref, sink_ref,
    out_ref, lse_ref,
    cos_ref, sin_ref, tok, normed, win_a, win_b, wo, acc_a, acc_b, qbuf, kvp, cf, ac, acg, ext, lse_buf,
    keep, send1, recv1, send2, recv2, gout, gin,
    tok_send, tok_recv, wz_send, wd_send, w_recv, sw_send, sw_recv, halo_sem, r_send, r_recv, g_send, g_recv, loc_sem,
):
    S = Z * X
    rows, width = tok_ref.shape
    depth = wq_ref.shape[0]
    ow, cols = oa_ref.shape
    qw = qbuf.shape[1]
    cw = cf.shape[1]
    kw = 2 * HEAD_DIM
    TP = tok.shape[0]
    chunk = rows // TP
    sp = lax.axis_index("sp")
    tp = lax.axis_index("tp")
    z, x = sp // X, sp % X
    c, y = tp % 2, tp // 2
    vs = z * X + c
    home, foreign = c == x, c != x
    role = jnp.where(home, 0, 1)
    sib = (sp, y * 2 + 1 - c)
    ynb = (sp, (1 - y) * 2 + c)
    yoth = (sp, (1 - y) * 2 + 1 - c)
    xnb = (z * X + 1 - x, tp)
    swp = (z * X + 1 - x, y * 2 + 1 - c)
    low, high = (sp - X, tp), (sp + X, tp)
    has_low, has_high = z > 0, z < Z - 1
    has_prev, has_next = vs > 0, vs < S - 1
    vn, vp = vs + 1, vs - 1 + S
    next_dev = ((vn // X) * X + x, y * 2 + vn % X)
    prev_dev = ((vp // X - Z) * X + x, y * 2 + vp % X)

    barrier = pltpu.get_barrier_semaphore()

    def greet(dev):
        pl.semaphore_signal(barrier, inc=1, device_id=dev, device_id_type=MESH)

    for dev in (sib, ynb, yoth, xnb, swp):
        greet(dev)
    peers = 5
    across_z = ((has_low, low), (has_high, high), (has_prev & (c == 0), prev_dev), (has_next & (c == 1), next_dev))
    for cond, dev in across_z:
        @pl.when(cond)
        def _(dev=dev):
            greet(dev)
        peers = peers + jnp.where(cond, 1, 0)

    pslot = jnp.where(home, sp, S)
    win_a[pslot, :, 0:qw] = wq_ref[...]
    kv_t = jnp.concatenate([wk_ref[...], wv_ref[...]], axis=0).astype(jnp.float32)
    win_a[pslot, :, qw:qw + kw] = jnp.transpose(kv_t).astype(jnp.bfloat16)
    for part, ref in enumerate((wpost_ref, wpre_ref, wcin_ref)):
        win_b[pslot, :, part * cw:(part + 1) * cw] = ref[...]
    heads = qw // HEAD_DIM
    ext[0] = jnp.zeros(ext.shape[1:], jnp.float32)
    ext[0, 0:3, :] = taps_ref[...]
    for h in range(heads):
        ext[0, 3 + h:4 + h, :] = jnp.full((1, cw), sink_ref[h], jnp.float32)

    pl.semaphore_wait(barrier, peers)

    def remote(src, dst, ssem, rsem, dev):
        return pltpu.make_async_remote_copy(
            src_ref=src, dst_ref=dst, send_sem=ssem, recv_sem=rsem,
            device_id=dev, device_id_type=MESH,
        )

    bufs = (win_a, win_b, wo)
    targets = (low, high, sib)

    def wcopy(kind, slot, direction):
        block = bufs[kind].at[slot]
        ssem = (wz_send, wz_send, wd_send)[direction].at[kind]
        return remote(block, block, ssem, w_recv.at[kind, slot], targets[direction])

    up_light = 2 * z + 1 < Z
    inner = has_low & has_high
    outer = jnp.logical_not(inner)

    def sent(block, sem):
        remote(block, block, sem, sem, sib).wait_send()

    def own_far(kind):
        for direction, cond in ((0, has_low & jnp.logical_not(up_light)), (1, has_high & up_light)):
            @pl.when(cond)
            def _(direction=direction):
                wcopy(kind, vs, direction).start()
        wcopy(kind, vs, 2).start()

    def own_near(kind):
        for direction, cond in ((0, has_low & up_light), (1, has_high & jnp.logical_not(up_light))):
            @pl.when(cond)
            def _(direction=direction):
                wcopy(kind, vs, direction).start()

    def own_start(kind):
        own_near(kind)
        own_far(kind)

    def swap(i, slot):
        src, dst = (
            (win_a.at[S], win_a.at[slot]),
            (win_b.at[S], win_b.at[slot]),
            (oa_ref, wo.at[slot, pl.ds(0, ow)]),
            (oc_ref, wo.at[slot, pl.ds(ow, cw)]),
            (ext.at[0], ext.at[1]),
            (lse_buf.at[0], lse_buf.at[1]),
        )[i]
        return remote(src, dst, sw_send.at[i], sw_recv.at[i], swp)

    TH = 2
    part_rows = rows // TH

    def tok_copy(src, q, i, part, dev):
        r = pl.ds(part * part_rows, part_rows)
        return remote(src.at[r], tok.at[q, r], tok_send.at[i], tok_recv.at[q, part], dev)

    tok_d = [tok_copy(tok_ref, tp, 1, part, sib) for part in range(TH)]
    tok_y = [tok_copy(tok_ref, tp, 0, part, (sp, (1 - y) * 2 + x)) for part in range(TH)]
    tok_x = [tok_copy(tok_ref, tp, 0, part, (z * X + 1 - x, y * 2 + x)) for part in range(TH)]
    local = [
        pltpu.make_async_copy(tok_ref, tok.at[tp], loc_sem.at[0]),
        pltpu.make_async_copy(oa_ref, wo.at[vs, pl.ds(0, ow)], loc_sem.at[1]),
        pltpu.make_async_copy(oc_ref, wo.at[vs, pl.ds(ow, cw)], loc_sem.at[2]),
    ]

    @pl.when(home)
    def _():
        own_start(0)
        own_start(1)

    @pl.when(foreign)
    def _():
        swap(0, sp).start()

    for part in range(TH):
        tok_x[part].start()
        tok_y[part].start()

    @pl.when(foreign)
    def _():
        for copy in tok_d:
            copy.start()
        for i in (1, 4, 2, 3):
            swap(i, sp).start()

    @pl.when(home)
    def _():
        for copy in local:
            copy.start()

    MB = 128
    quarter = HEAD_DIM // 4

    def angles(i, carry):
        r = pl.ds(pl.multiple_of(i * MB, MB), MB)
        pos = vs * rows + i * MB + lax.broadcasted_iota(jnp.int32, (MB, kw), 0)
        lane = lax.broadcasted_iota(jnp.int32, (MB, kw), 1) % HEAD_DIM
        freq = jnp.exp((lane % quarter).astype(jnp.float32) * (-4.0 / HEAD_DIM * math.log(rope_base)))
        index = jnp.where(lane >= 2 * quarter, pos % GRID_W, pos // GRID_W)
        angle = index.astype(jnp.float32) * freq
        cos_ref[r, :] = jnp.cos(angle)
        sin_ref[r, :] = jnp.where(lane % (2 * quarter) < quarter, -1.0, 1.0) * jnp.sin(angle)
        return carry

    def comm(kind, dist, only=None, forward=True):
        for up in (0, 1):
            zz = z + dist * (2 * up - 1)
            valid = (zz >= 0) & (zz < Z)
            if only is not None:
                valid = valid & only

            @pl.when(valid)
            def _(zz=zz, up=up):
                slot = zz * X + c
                wcopy(kind, slot, 2).wait_recv()

                if forward:
                    @pl.when(has_low if up else has_high)
                    def _():
                        wcopy(kind, slot, 0 if up else 1).start()
                wcopy(kind, slot, 2).start()

    def relay(cc, part):
        q = y * 2 + cc
        return tok_copy(tok.at[q], q, 1, part, ynb)

    def tok_wait(q, part):
        tok_copy(tok.at[q], q, 0, part, ynb).wait_recv()

    RB = 64

    def norm_rows(i, carry):
        r = pl.ds(pl.multiple_of(i * RB, RB), RB)
        total = jnp.zeros((RB, 1), jnp.float32)
        for t in range(TP):
            v = tok[t, r, :].astype(jnp.float32)
            total += jnp.sum(v * v, axis=1, keepdims=True)
        scale = lax.rsqrt(total / (TP * width) + norm_eps)
        for t in range(TP):
            v = tok[t, r, :].astype(jnp.float32)
            g = gain_ref[:, t * width:(t + 1) * width]
            normed[r, t * width:(t + 1) * width] = (v * scale * g).astype(jnp.bfloat16)
        return carry

    pdepth = X * depth

    def project(kind, zz, first):
        win, acc = ((win_a, acc_a), (win_b, acc_b))[kind]
        n = acc.shape[1]
        wcopy(kind, zz * X + 1 - c, 2).wait_recv()

        pb = acc.shape[0] // 2

        def body(i, carry):
            r = pl.ds(pl.multiple_of(i * pb, 16), pb)
            k = pl.ds(pl.multiple_of(zz * pdepth, pdepth), pdepth)
            weight = win[pl.ds(zz * X, X)].reshape(pdepth, n)
            prod = jnp.dot(normed[r, k], weight, preferred_element_type=jnp.float32)
            if first:
                acc[r, :] = prod
            else:
                acc[r, :] += prod
            return carry
        lax.fori_loop(0, 2, body, 0)

    def each_side(dist, fn):
        def step(side, carry):
            zz = z + dist * (2 * side - 1)

            @pl.when((zz >= 0) & (zz < Z))
            def _():
                fn(zz)
            return carry
        lax.fori_loop(0, 2, step, 0)

    def project_at(kind, dist):
        each_side(dist, lambda zz: project(kind, zz, False))

    def halo(i, src, dst, dev):
        return remote(src, dst, halo_sem.at[2 * i], halo_sem.at[2 * i + 1], dev)

    kv_next = halo(0, kvp.at[pl.ds(rows, WINDOW)], kvp.at[pl.ds(0, WINDOW)], next_dev)
    kv_prev = halo(1, kvp.at[pl.ds(WINDOW, WINDOW)], kvp.at[pl.ds(WINDOW + rows, WINDOW)], prev_dev)
    n_next = halo(2, normed.at[pl.ds(rows - NEAR, NEAR)], normed.at[pl.ds(rows + EDGE - NEAR, NEAR)], next_dev)
    n_prev = halo(3, normed.at[pl.ds(0, NEAR)], normed.at[pl.ds(rows + EDGE, NEAR)], prev_dev)

    lax.fori_loop(0, rows // MB, angles, 0)

    @pl.when(foreign)
    def _():
        swap(0, vs).wait_recv()
        own_start(0)
        for cc in range(2):
            tok_wait(y * 2 + cc, 0)
            relay(cc, 0).start()

    comm(0, 1)

    @pl.when(foreign)
    def _():
        for cc in range(2):
            tok_wait(y * 2 + cc, 1)
            relay(cc, 1).start()

    @pl.when(home)
    def _():
        comm(1, 1)
    comm(0, 2)

    @pl.when(foreign)
    def _():
        swap(1, vs).wait_recv()
        own_start(1)
        swap(4, vs).wait_recv()

    @pl.when(home)
    def _():
        for copy in local:
            copy.wait()
        own_far(2)
        for part in range(TH):
            tok_wait(y * 2 + 1 - c, part)
    for part in range(TH):
        for cc in range(2):
            tok_wait((1 - y) * 2 + cc, part)
        lax.fori_loop(part * (part_rows // RB), (part + 1) * (part_rows // RB), norm_rows, 0)

    @pl.when(has_next)
    def _():
        n_next.start()

    @pl.when(has_prev)
    def _():
        n_prev.start()

    @pl.when(foreign)
    def _():
        comm(1, 1, inner)
        for i in (2, 3):
            swap(i, vs).wait_recv()
        own_far(2)

    for dist in range(3, Z):
        comm(0, dist)
    project(0, z, True)
    project_at(0, 1)

    @pl.when(home)
    def _():
        comm(1, 2)

    for dist in range(2, Z):
        project_at(0, dist)

    @pl.when(foreign)
    def _():
        comm(1, 1, outer)

    def turned(v, cosv, sinv):
        lane = lax.broadcasted_iota(jnp.int32, v.shape, 1)
        partner = jnp.where(
            lane % (2 * quarter) < quarter,
            pltpu.roll(v, v.shape[1] - quarter, 1),
            pltpu.roll(v, quarter, 1),
        )
        return v * cosv + partner * sinv

    def k_rows(i, carry):
        r = pl.ds(pl.multiple_of(i * MB, MB), MB)
        v = acc_a[r, qw:qw + kw]
        lane = lax.broadcasted_iota(jnp.int32, v.shape, 1)
        kv = jnp.where(lane < HEAD_DIM, turned(v, cos_ref[r, :], sin_ref[r, :]), v)
        kvp[pl.ds(pl.multiple_of(WINDOW + i * MB, MB), MB), :] = kv.astype(jnp.bfloat16)
        return carry

    lax.fori_loop(0, rows // MB, k_rows, 0)

    @pl.when(has_next)
    def _():
        kv_next.start()

    @pl.when(has_prev)
    def _():
        kv_prev.start()

    def q_rows(i, carry):
        r = pl.ds(pl.multiple_of(i * MB, MB), MB)
        for k in range(qw // kw):
            qbuf[r, k * kw:(k + 1) * kw] = turned(
                acc_a[r, k * kw:(k + 1) * kw], cos_ref[r, :], sin_ref[r, :]
            ).astype(jnp.bfloat16)
        return carry

    lax.fori_loop(0, rows // MB, q_rows, 0)

    K3 = 3 * WINDOW
    total_tokens = rows * S

    guest_dev = (sp + X * jnp.where(inner == up_light, -1, 1), tp)
    far = jnp.where(up_light, Z - 1, 0)

    def guest_copy(half, r):
        return remote(ac.at[half, r], acg.at[half, r], g_send.at[half], g_recv.at[half], guest_dev)

    def attend(b, carry):
        r = pl.ds(pl.multiple_of(b * WINDOW, WINDOW), WINDOW)
        kv = kvp[pl.ds(pl.multiple_of(b * WINDOW, WINDOW), K3), :].astype(jnp.float32)
        lane = lax.broadcasted_iota(jnp.int32, (K3, kw), 1)
        swapped = pltpu.roll(kv, HEAD_DIM, 1)
        kk = jnp.where(lane < HEAD_DIM, kv, swapped).astype(jnp.bfloat16)
        vv = jnp.where(lane < HEAD_DIM, swapped, kv).astype(jnp.bfloat16)
        k_half = [jnp.where(lane < HEAD_DIM, kk, 0), jnp.where(lane < HEAD_DIM, 0, kk)]
        v_half = [jnp.where(lane < HEAD_DIM, vv, 0), jnp.where(lane < HEAD_DIM, 0, vv)]
        qi = lax.broadcasted_iota(jnp.int32, (WINDOW, K3), 0)
        ki = lax.broadcasted_iota(jnp.int32, (WINDOW, K3), 1)
        first = vs * rows + b * WINDOW - WINDOW
        allowed = (ki >= qi) & (ki <= qi + 2 * WINDOW) & (ki + first >= 0) & (ki + first < total_tokens)
        lse_lane = lax.broadcasted_iota(jnp.int32, (WINDOW, WINDOW), 1)
        lse_all = jnp.zeros((WINDOW, WINDOW), jnp.float32)
        for pair in range(heads // 2):
            q = qbuf[r, pair * kw:(pair + 1) * kw]
            total = jnp.zeros((WINDOW, kw), jnp.float32)
            for side in range(2):
                h = pair * 2 + side
                s = lax.dot_general(
                    q, k_half[side], (((1,), (1,)), ((), ())), preferred_element_type=jnp.float32
                ) * HEAD_DIM ** (-0.5)
                s = jnp.where(allowed, s, -jnp.inf)
                sink = ext[role, 3 + h:4 + h, 0:WINDOW]
                top = jnp.maximum(jnp.max(s, axis=1, keepdims=True), sink)
                e = jnp.exp(s - jnp.concatenate([top] * 3, axis=1))
                den = jnp.sum(e, axis=1, keepdims=True) + jnp.exp(sink - top)
                w = (e * jnp.concatenate([1.0 / den] * 3, axis=1)).astype(jnp.bfloat16)
                total += jnp.dot(w, v_half[side], preferred_element_type=jnp.float32)
                lse_all = jnp.where(lse_lane == h, top + jnp.log(den), lse_all)
            ac[0, r, pair * kw:(pair + 1) * kw] = total.astype(jnp.bfloat16)

        @pl.when(outer)
        def _():
            guest_copy(0, r).start()
        lse_buf[0, :, r] = jnp.transpose(lse_all)[0:heads, :]
        return carry

    blocks = rows // WINDOW
    zero_kv = jnp.zeros((WINDOW, kw), jnp.bfloat16)

    def prev_ready():
        @pl.when(has_prev)
        def _():
            kv_next.wait_recv()

        @pl.when(jnp.logical_not(has_prev))
        def _():
            kvp[0:WINDOW, :] = zero_kv

    def next_ready():
        @pl.when(has_next)
        def _():
            kv_prev.wait_recv()

        @pl.when(jnp.logical_not(has_next))
        def _():
            kvp[WINDOW + rows:, :] = zero_kv

    def edge_ready(at_start):
        @pl.when(at_start)
        def _():
            prev_ready()

        @pl.when(jnp.logical_not(at_start))
        def _():
            next_ready()

    def attend_from(i, carry):
        return attend((1 - c + i) % blocks, carry)

    def b_ready():
        @pl.when(has_prev)
        def _():
            n_next.wait_recv()

        @pl.when(has_next)
        def _():
            n_prev.wait_recv()

        zero_n = jnp.zeros((NEAR, TP * width), jnp.bfloat16)
        normed[rows:rows + EDGE - NEAR, :] = zero_n
        normed[rows + EDGE + NEAR:, :] = zero_n

        @pl.when(jnp.logical_not(has_prev))
        def _():
            normed[rows + EDGE - NEAR:rows + EDGE, :] = zero_n

        @pl.when(jnp.logical_not(has_next))
        def _():
            normed[rows + EDGE:rows + EDGE + NEAR, :] = zero_n

    @pl.when(home)
    def _():
        for dist in range(3, Z):
            comm(1, dist)

    edge_ready(c == 1)
    lax.fori_loop(0, blocks // 2, attend_from, 0)
    b_ready()
    project(1, z, True)

    @pl.when(foreign)
    def _():
        comm(1, 2)
        own_near(2)
    lax.fori_loop(blocks // 2, blocks - 1, attend_from, 0)
    edge_ready(c == 0)
    lax.fori_loop(blocks - 1, blocks, attend_from, 0)

    @pl.when(foreign)
    def _():
        swap(5, sp).start()

    project_at(1, 1)
    project_at(1, 2)

    @pl.when(home)
    def _():
        own_near(2)

    @pl.when(foreign)
    def _():
        for dist in range(3, Z):
            comm(1, dist)
    for dist in range(3, Z):
        project_at(1, dist)
    comm(2, 1, inner)

    def gated(lo, n):
        return (acc_b[lo:lo + n, cw:2 * cw] * acc_b[lo:lo + n, 2 * cw:3 * cw]).astype(jnp.bfloat16)

    for i in range(rows // MB):
        cf[8 + i * MB:8 + (i + 1) * MB, :] = gated(i * MB, MB).astype(jnp.float32)
    edge = gated(rows, 2 * EDGE).astype(jnp.float32)
    cf[0:8, :] = edge[EDGE - 8:EDGE, :]
    cf[8 + rows:16 + rows, :] = edge[EDGE:EDGE + 8, :]

    taps = [ext[role, t:t + 1, :] for t in range(3)]
    for i in range(rows // MB):
        a = 8 + i * MB
        conv = (
            taps[0] * cf[a - 1:a - 1 + MB, :]
            + taps[1] * cf[a:a + MB, :]
            + taps[2] * cf[a + 1:a + 1 + MB, :]
        )
        ac[1, i * MB:(i + 1) * MB, :] = (acc_b[i * MB:(i + 1) * MB, 0:cw] * conv).astype(jnp.bfloat16)

        @pl.when(outer)
        def _(i=i):
            guest_copy(1, pl.ds(i * MB, MB)).start()

    mine_dev = (z * X + c, y * 2 + c)
    other_dev = (z * X + c, y * 2 + 1 - c)

    def r1(s, src, dst, dev, extra=0):
        return remote(send1.at[s, src], recv1.at[s, dst], r_send.at[extra], r_recv.at[s, dst], dev)

    def r2(s, src, dst, dev, sem, extra=0):
        return remote(send2.at[s, src], recv2.at[s, dst], r_send.at[2 + extra], r_recv.at[s, sem], dev)

    def out_dot(src, w, yo, m):
        co = c if m == 0 else 1 - c
        r = pl.ds(pl.multiple_of((2 * yo + co) * chunk, chunk), chunk)
        both = jnp.concatenate([src[0, r, :], src[1, r, :]], axis=1)
        return jnp.dot(both, wo[w], preferred_element_type=jnp.float32)

    def produce_x(s, w, src):
        for yo in range(2):
            for m in (1, 0):
                v = out_dot(src, w, yo, m)
                if m == 0:
                    keep[s, yo] = v
                send1[s, m, yo] = v.astype(jnp.bfloat16)
        r1(s, 1, role, other_dev).start()

        @pl.when(foreign)
        def _():
            r1(s, 0, 1, mine_dev, 1).start()

    def produce_y(s, w, src):
        for m in range(2):
            send1[s, 0, m] = out_dot(src, w, 1 - y, m).astype(jnp.bfloat16)
        r1(s, 0, 0, ynb).start()
        for m in range(2):
            keep[s, m] = out_dot(src, w, y, m)

    def stage_x(s):
        r1(s, 0, 1, mine_dev).wait_recv()

        def pass_on(base):
            send2[s, 0] = (base(1 - y) + recv1[s, 1, 1 - y].astype(jnp.float32)).astype(jnp.bfloat16)
            r2(s, 0, 0, ynb, 2).start()
            keep[s, y] = base(y) + recv1[s, 1, y].astype(jnp.float32)

        @pl.when(home)
        def _():
            pass_on(lambda yo: keep[s, yo])

        @pl.when(foreign)
        def _():
            r1(s, 1, 0, other_dev).wait_recv()
            pass_on(lambda yo: recv1[s, 0, yo].astype(jnp.float32))

    def stage_y(s):
        r1(s, 0, 0, ynb).wait_recv()
        send2[s, 1] = (keep[s, 1] + recv1[s, 0, 1].astype(jnp.float32)).astype(jnp.bfloat16)
        r2(s, 1, role, other_dev, 1 + role).start()
        mine = keep[s, 0] + recv1[s, 0, 0].astype(jnp.float32)

        @pl.when(home)
        def _():
            keep[s, 0] = mine

        @pl.when(foreign)
        def _():
            send2[s, 0] = mine.astype(jnp.bfloat16)
            r2(s, 0, 1, mine_dev, 2, 1).start()

    def place(s, v):
        out_ref[:, pl.ds(pl.multiple_of(s * cols, cols), cols)] = v.astype(jnp.bfloat16)

    def finish_x(s, place=place):
        r2(s, 0, 0, ynb, 2).wait_recv()
        place(s, keep[s, y] + recv2[s, 0].astype(jnp.float32))

    def finish_y(s, place=place):
        r2(s, 0, 1, mine_dev, 2).wait_recv()
        arrived = recv2[s, 1].astype(jnp.float32)

        @pl.when(home)
        def _():
            place(s, keep[s, 0] + arrived)

        @pl.when(foreign)
        def _():
            r2(s, 1, 0, other_dev, 1).wait_recv()
            place(s, recv2[s, 0].astype(jnp.float32) + arrived)

    def produce_from(b, zz, src):
        produce_x(b, zz * X, src)
        produce_y(b + 1, zz * X + 1, src)

    def produce(zz):
        wcopy(2, zz * X + 1 - c, 2).wait_recv()
        produce_from(zz * X, zz, ac)

    def stage(zz):
        stage_x(zz * X)
        stage_y(zz * X + 1)

    def finish(zz):
        finish_x(zz * X)
        finish_y(zz * X + 1)

    def hand_back(i):
        return remote(gout.at[i], gin.at[i], g_send.at[2 + i], g_recv.at[2 + i], guest_dev)

    def back(i):
        def put(s, v):
            gout[i] = v.astype(jnp.bfloat16)
            hand_back(i).start()
        return put

    produce(z)
    comm(2, 1, outer)
    each_side(1, produce)
    comm(2, 2, inner, False)
    stage(z)
    comm(2, 2, outer, False)

    @pl.when(outer)
    def _():
        each_side(2, produce)
        each_side(1, stage)

    @pl.when(inner)
    def _():
        for half in range(2):
            remote(acg.at[half], acg.at[half], g_send.at[half], g_recv.at[half], guest_dev).wait_recv()
        wcopy(2, far * X + 1 - c, 2).wait_recv()
        produce_from(S, far, acg)
        each_side(1, stage)
        stage(Z)
        produce_from(far * X, far, ac)
    @pl.when(inner)
    def _():
        finish_x(S, back(0))
        finish_y(S + 1, back(1))
    each_side(2, stage)
    finish(z)
    each_side(1, finish)
    each_side(2, finish)

    @pl.when(inner)
    def _():
        for i in range(2):
            hand_back(i).wait_send()

    @pl.when(outer)
    def _():
        for i in range(2):
            hand_back(i).wait_recv()
            place(far * X + i, gin[i])
        for half in range(2):
            sent(ac.at[half], g_send.at[half])

    @pl.when(home)
    def _():
        lse_ref[...] = lse_buf[0]

    @pl.when(foreign)
    def _():
        swap(5, vs).wait_recv()
        lse_ref[...] = lse_buf[1]
        for i in range(6):
            swap(i, sp).wait_send()

    @pl.when(has_next)
    def _():
        kv_next.wait_send()
        n_next.wait_send()

    @pl.when(has_prev)
    def _():
        kv_prev.wait_send()
        n_prev.wait_send()

    sent(tok.at[pl.ds(0, 2)], tok_send.at[0])
    for cond, pairs, along in ((inner, Z + 1, Z + 1), (outer, Z - 1, 1)):
        @pl.when(cond)
        def _(pairs=pairs, along=along):
            for kind in range(3):
                fewer = 1 if kind == 2 and along > 1 else 0
                sent(bufs[kind].at[pl.ds(0, along - fewer)], wz_send.at[kind])
                sent(bufs[kind].at[pl.ds(0, Z if kind < 2 else min(pairs, Z))], wd_send.at[kind])
            sent(send1.at[pl.ds(0, pairs)], r_send.at[0])
            sent(send2.at[pl.ds(0, pairs)], r_send.at[2])

            @pl.when(foreign)
            def _():
                sent(send1.at[pl.ds(0, pairs), 0], r_send.at[1])
                sent(send2.at[pl.ds(0, pairs), 0], r_send.at[3])

    @pl.when(foreign)
    def _():
        sent(tok.at[pl.ds(0, 3)], tok_send.at[1])


def fused(
    tokens, norm_gain, w_query, w_key, w_value, w_post_gate, w_pre_gate, w_conv_in,
    conv_taps, sink_logit, w_out_attn, w_out_conv,
):
    S, TP = lax.axis_size("sp"), lax.axis_size("tp")
    X = 2
    Z = S // X
    rows, width = tokens.shape
    depth, qw = w_query.shape
    cw = w_post_gate.shape[1]
    ow, cols = w_out_attn.shape
    heads = qw // HEAD_DIM
    kw = 2 * HEAD_DIM
    chunk = rows // TP
    bf, f32 = jnp.bfloat16, jnp.float32
    dma = pltpu.SemaphoreType.DMA
    return pl.pallas_call(
        functools.partial(fused_kernel, Z, X),
        out_shape=(
            pltpu.VMEM((chunk, S * cols), bf),
            pltpu.VMEM((heads, rows), f32),
        ),
        in_specs=[pl.BlockSpec(memory_space=pltpu.VMEM)] * 11 + [pl.BlockSpec(memory_space=pltpu.SMEM)],
        out_specs=(pl.BlockSpec(memory_space=pltpu.VMEM),) * 2,
        scratch_shapes=[
            pltpu.VMEM((rows, kw), f32),
            pltpu.VMEM((rows, kw), f32),
            pltpu.VMEM((TP, rows, width), bf),
            pltpu.VMEM((rows + 2 * EDGE, TP * width), bf),
            pltpu.VMEM((S + 1, depth, qw + kw), bf),
            pltpu.VMEM((S + 1, depth, 3 * cw), bf),
            pltpu.VMEM((S, ow + cw, cols), bf),
            pltpu.VMEM((rows, qw + kw), f32),
            pltpu.VMEM((rows + 2 * EDGE, 3 * cw), f32),
            pltpu.VMEM((rows, qw), bf),
            pltpu.VMEM((rows + 2 * WINDOW, kw), bf),
            pltpu.VMEM((rows + 16, cw), f32),
            pltpu.VMEM((2, rows, qw), bf),
            pltpu.VMEM((2, rows, qw), bf),
            pltpu.VMEM((2, -(-(3 + heads) // 8) * 8, cw), f32),
            pltpu.VMEM((2, heads, rows), f32),
            pltpu.VMEM((S + X, 2, chunk, cols), f32),
            pltpu.VMEM((S + X, 2, 2, chunk, cols), bf),
            pltpu.VMEM((S + X, 2, 2, chunk, cols), bf),
            pltpu.VMEM((S + X, 2, chunk, cols), bf),
            pltpu.VMEM((S + X, 2, chunk, cols), bf),
            pltpu.VMEM((X, chunk, cols), bf),
            pltpu.VMEM((X, chunk, cols), bf),
            dma((2,)), dma((TP, 2)),
            dma((3,)), dma((3,)), dma((3, S)),
            dma((6,)), dma((6,)),
            dma((8,)),
            dma((4,)), dma((S + X, 3)),
            dma((4,)), dma((4,)),
            dma((3,)),
        ],
        compiler_params=pltpu.CompilerParams(
            collective_id=0, has_side_effects=True, vmem_limit_bytes=60 * 1024 * 1024
        ),
    )(
        tokens, norm_gain[None, :], w_query, w_key.T, w_value.T, w_post_gate, w_pre_gate, w_conv_in,
        w_out_attn, w_out_conv, conv_taps, sink_logit,
    )


def fits(
    tokens, norm_gain, w_query, w_key, w_value, w_post_gate, w_pre_gate, w_conv_in,
    conv_taps, sink_logit, w_out_attn, w_out_conv,
):
    S, TP = lax.axis_size("sp"), lax.axis_size("tp")
    return (
        TP == 4
        and S % 2 == 0
        and S == 8
        and w_key.shape[1] == HEAD_DIM
        and w_query.shape[0] % 128 == 0
        and w_query.shape[1] % 128 == 0
        and w_post_gate.shape[1] == w_query.shape[1]
        and w_out_attn.shape[1] % 128 == 0
        and tokens.shape[0] % (TP * WINDOW) == 0
        and tokens.shape[1] % 128 == 0
    )


def either(*args):
    return fused(*args) if fits(*args) else on_device(*args)


def solution(mesh):
    placed = (
        P("sp", "tp"),
        P(),
        P("sp", "tp"),
        P("sp", "tp"),
        P("sp", "tp"),
        P("sp", "tp"),
        P("sp", "tp"),
        P("sp", "tp"),
        P(None, "tp"),
        P("tp"),
        P("tp", "sp"),
        P("tp", "sp"),
    )
    return jax.shard_map(
        either,
        mesh=mesh,
        in_specs=placed,
        out_specs=(P(("sp", "tp"), None), P("tp", "sp")),
        check_vma=False,
    )
```

```python
import functools
import math

import jax
import jax.numpy as jnp
from jax import lax
from jax.experimental import pallas as pl
from jax.experimental.pallas import tpu as pltpu
from jax.sharding import PartitionSpec as P

MESH = pl.DeviceIdType.MESH

HEAD_DIM = 64
WINDOW = 128
GRID_W = 64
EDGE = 16
NEAR = 8


rope_base = 10000.0
norm_eps = 1e-06


def padded(block, sides, width):
    for axis, dim in sides:
        count = lax.axis_size(axis)
        forward = [(i, i + 1) for i in range(count - 1)]
        backward = [(target, source) for source, target in forward]
        low = lax.ppermute(
            lax.slice_in_dim(block, block.shape[dim] - width, None, axis=dim), axis, forward
        )
        high = lax.ppermute(lax.slice_in_dim(block, 0, width, axis=dim), axis, backward)
        block = jnp.concatenate([low, block, high], axis=dim)
    return block


def rotate_pair(values, angles):
    first_half, second_half = jnp.split(values, 2, axis=-1)
    cosine = jnp.cos(angles)[:, None, :]
    sine_part = jnp.sin(angles)[:, None, :]
    return jnp.concatenate(
        [
            first_half * cosine - second_half * sine_part,
            first_half * sine_part + second_half * cosine,
        ],
        axis=-1,
    )


def axial_rotate(values, positions):
    half_dim = values.shape[-1] // 2
    inv_freq = rope_base ** (-jnp.arange(0, half_dim, 2).astype(jnp.float32) / half_dim)
    row_angle = (positions // GRID_W).astype(jnp.float32)[:, None] * inv_freq
    col_angle = (positions % GRID_W).astype(jnp.float32)[:, None] * inv_freq
    row_part, col_part = jnp.split(values, 2, axis=-1)
    return jnp.concatenate(
        [rotate_pair(row_part, row_angle), rotate_pair(col_part, col_angle)], axis=-1
    )


def block_windows(source, rows_local, blocks):
    pieces = [
        source[step * WINDOW : step * WINDOW + rows_local].reshape(
            (blocks, WINDOW) + source.shape[1:]
        )
        for step in range(3)
    ]
    return jnp.concatenate(pieces, axis=1)


def on_device(
    tokens,
    norm_gain,
    w_query,
    w_key,
    w_value,
    w_post_gate,
    w_pre_gate,
    w_conv_in,
    conv_taps,
    sink_logit,
    w_out_attn,
    w_out_conv,
):
    whole = lax.all_gather(tokens, "tp", axis=1, tiled=True)
    rows_local = whole.shape[0]
    whole_float = whole.astype(jnp.float32)
    mean_square = jnp.mean(whole_float * whole_float, axis=1, keepdims=True)
    normed = (whole_float * lax.rsqrt(mean_square + norm_eps) * norm_gain).astype(jnp.bfloat16)
    col_widths = [
        w_query.shape[1],
        w_key.shape[1],
        w_value.shape[1],
        w_post_gate.shape[1],
        w_pre_gate.shape[1],
        w_conv_in.shape[1],
    ]
    joined = jnp.concatenate(
        (
            lax.all_gather(w_query, "sp", axis=0, tiled=True),
            lax.all_gather(w_key, "sp", axis=0, tiled=True),
            lax.all_gather(w_value, "sp", axis=0, tiled=True),
            lax.all_gather(w_post_gate, "sp", axis=0, tiled=True),
            lax.all_gather(w_pre_gate, "sp", axis=0, tiled=True),
            lax.all_gather(w_conv_in, "sp", axis=0, tiled=True),
        ),
        axis=1,
    )
    projected = jnp.dot(normed, joined, preferred_element_type=jnp.float32)
    bounds = []
    running = 0
    for col_width in col_widths[:-1]:
        running += col_width
        bounds.append(running)
    query_raw, key_raw, value_raw, post_gate, pre_gate, conv_input = jnp.split(
        projected, bounds, axis=1
    )
    offset = lax.axis_index("sp") * rows_local
    positions = offset + jnp.arange(rows_local, dtype=jnp.int32)
    local_heads = w_query.shape[1] // HEAD_DIM
    local_groups = w_key.shape[1] // HEAD_DIM
    group_size = local_heads // local_groups
    queries = axial_rotate(query_raw.reshape(rows_local, local_heads, HEAD_DIM), positions).astype(
        jnp.bfloat16
    )
    keys_rot = axial_rotate(key_raw.reshape(rows_local, local_groups, HEAD_DIM), positions).astype(
        jnp.bfloat16
    )
    key_value = jnp.concatenate(
        [keys_rot.reshape(rows_local, local_groups * HEAD_DIM), value_raw.astype(jnp.bfloat16)],
        axis=1,
    )
    mixed_input = (pre_gate * conv_input).astype(jnp.bfloat16)
    kv_padded = padded(key_value, (("sp", 0),), WINDOW)
    conv_padded = padded(mixed_input, (("sp", 0),), 1)
    conv_float = conv_padded.astype(jnp.float32)
    convolved = (
        conv_taps[0] * conv_float[:-2]
        + conv_taps[1] * conv_float[1:-1]
        + conv_taps[2] * conv_float[2:]
    )
    conv_out = (post_gate * convolved).astype(jnp.bfloat16)
    total_tokens = rows_local * lax.axis_size("sp")
    blocks = rows_local // WINDOW
    padded_rows = rows_local + 2 * WINDOW
    block_queries = queries.reshape(blocks, WINDOW, local_groups, group_size, HEAD_DIM)
    block_keys = block_windows(
        kv_padded[:, : local_groups * HEAD_DIM].reshape(padded_rows, local_groups, HEAD_DIM),
        rows_local,
        blocks,
    )
    block_values = block_windows(
        kv_padded[:, local_groups * HEAD_DIM :].reshape(padded_rows, local_groups, HEAD_DIM),
        rows_local,
        blocks,
    )
    scores = jnp.einsum(
        "nqkgd,nskd->nkgqs", block_queries, block_keys, preferred_element_type=jnp.float32
    ) * HEAD_DIM ** (-0.5)
    query_pos = positions.reshape(blocks, WINDOW)
    key_pos = (
        offset
        - WINDOW
        + (jnp.arange(blocks, dtype=jnp.int32) * WINDOW)[:, None]
        + jnp.arange(3 * WINDOW, dtype=jnp.int32)[None, :]
    )
    distance = key_pos[:, None, :] - query_pos[:, :, None]
    allowed = (
        (jnp.abs(distance) <= WINDOW)
        & (key_pos >= 0)[:, None, :]
        & (key_pos < total_tokens)[:, None, :]
    )
    scores = jnp.where(allowed[:, None, None], scores, -jnp.inf)
    sink_values = sink_logit.reshape(local_groups, group_size)[None, :, :, None]
    row_max = jnp.maximum(jnp.max(scores, axis=-1), sink_values)
    exp_scores = jnp.exp(scores - row_max[..., None])
    denominator = jnp.sum(exp_scores, axis=-1) + jnp.exp(sink_values - row_max)
    weights = (exp_scores / denominator[..., None]).astype(jnp.bfloat16)
    attended = (
        jnp.einsum("nkgqs,nskd->nqkgd", weights, block_values, preferred_element_type=jnp.float32)
        .astype(jnp.bfloat16)
        .reshape(rows_local, local_heads * HEAD_DIM)
    )
    log_sum = row_max + jnp.log(denominator)
    log_weight_sum = jnp.transpose(log_sum, (1, 2, 0, 3)).reshape(local_heads, rows_local)
    out_attn, out_conv = (
        lax.all_gather(w_out_attn, "sp", axis=1, tiled=True),
        lax.all_gather(w_out_conv, "sp", axis=1, tiled=True),
    )
    mixed = lax.psum_scatter(
        (
            jnp.dot(attended, out_attn, preferred_element_type=jnp.float32)
            + jnp.dot(conv_out, out_conv, preferred_element_type=jnp.float32)
        ).astype(jnp.bfloat16),
        "tp",
        scatter_dimension=0,
        tiled=True,
    )
    return (mixed, log_weight_sum)


def fused_kernel(
    Z, X,
    tok_ref, gain_ref, wq_ref, wk_ref, wv_ref, wpost_ref, wpre_ref, wcin_ref, oa_ref, oc_ref, taps_ref, sink_ref,
    out_ref, lse_ref,
    cos_ref, sin_ref, tok, normed, win_a, win_b, wo, acc_a, acc_b, qbuf, kvp, cf, ac, acg, ext, lse_buf,
    keep, send1, recv1, send2, recv2, gout, gin,
    tok_send, tok_recv, wz_send, wd_send, w_recv, sw_send, sw_recv, halo_sem, r_send, r_recv, g_send, g_recv, loc_sem,
):
    S = Z * X
    rows, width = tok_ref.shape
    depth = wq_ref.shape[0]
    ow, cols = oa_ref.shape
    qw = qbuf.shape[1]
    cw = cf.shape[1]
    kw = 2 * HEAD_DIM
    TP = tok.shape[0] - 1
    chunk = rows // TP
    sp = lax.axis_index("sp")
    tp = lax.axis_index("tp")
    z, x = sp // X, sp % X
    c, y = tp % 2, tp // 2
    vs = z * X + c
    home, foreign = c == x, c != x
    role = jnp.where(home, 0, 1)
    sib = (sp, y * 2 + 1 - c)
    ynb = (sp, (1 - y) * 2 + c)
    yoth = (sp, (1 - y) * 2 + 1 - c)
    xnb = (z * X + 1 - x, tp)
    swp = (z * X + 1 - x, y * 2 + 1 - c)
    low, high = (sp - X, tp), (sp + X, tp)
    has_low, has_high = z > 0, z < Z - 1
    has_prev, has_next = vs > 0, vs < S - 1
    vn, vp = vs + 1, vs - 1 + S
    next_dev = ((vn // X) * X + x, y * 2 + vn % X)
    prev_dev = ((vp // X - Z) * X + x, y * 2 + vp % X)

    barrier = pltpu.get_barrier_semaphore()

    def greet(dev):
        pl.semaphore_signal(barrier, inc=1, device_id=dev, device_id_type=MESH)

    for dev in (sib, ynb, yoth, xnb, swp):
        greet(dev)
    peers = 5
    across_z = ((has_low, low), (has_high, high), (has_prev & (c == 0), prev_dev), (has_next & (c == 1), next_dev))
    for cond, dev in across_z:
        @pl.when(cond)
        def _(dev=dev):
            greet(dev)
        peers = peers + jnp.where(cond, 1, 0)

    pslot = jnp.where(home, sp, S)
    own_tok = jnp.where(home, tp, TP)
    load_tok = pltpu.make_async_copy(tok_ref, tok.at[own_tok], loc_sem.at[0])
    load_a = pltpu.make_async_copy(wq_ref, win_a.at[pslot, :, pl.ds(0, qw)], loc_sem.at[1])
    load_b = [
        pltpu.make_async_copy(ref, win_b.at[pslot, :, pl.ds(part * cw, cw)], loc_sem.at[2])
        for part, ref in enumerate((wpost_ref, wpre_ref, wcin_ref))
    ]
    load_c = [
        pltpu.make_async_copy(ref, wo.at[pslot, pl.ds(part * ow, ow)], loc_sem.at[3])
        for part, ref in enumerate((oa_ref, oc_ref))
    ]
    for copy in (load_a, load_tok, *load_b, *load_c):
        copy.start()
    kv_t = jnp.concatenate([wk_ref[...], wv_ref[...]], axis=0).astype(jnp.float32)
    win_a[pslot, :, qw:qw + kw] = jnp.transpose(kv_t).astype(jnp.bfloat16)
    heads = qw // HEAD_DIM
    ext[0] = jnp.zeros(ext.shape[1:], jnp.float32)
    ext[0, 0:3, :] = taps_ref[...]
    for h in range(heads):
        ext[0, 3 + h:4 + h, :] = jnp.full((1, cw), sink_ref[h], jnp.float32)

    pl.semaphore_wait(barrier, peers)

    def remote(src, dst, ssem, rsem, dev):
        return pltpu.make_async_remote_copy(
            src_ref=src, dst_ref=dst, send_sem=ssem, recv_sem=rsem,
            device_id=dev, device_id_type=MESH,
        )

    bufs = (win_a, win_b, wo)
    targets = (low, high, sib)

    def wcopy(kind, slot, direction):
        block = bufs[kind].at[slot]
        ssem = (wz_send, wz_send, wd_send)[direction].at[kind]
        return remote(block, block, ssem, w_recv.at[kind, slot], targets[direction])

    up_light = 2 * z + 1 < Z
    far = jnp.where(up_light, Z - 1, 0)
    inner = has_low & has_high
    outer = jnp.logical_not(inner)

    def sent(block, sem):
        remote(block, block, sem, sem, sib).wait_send()

    def own_far(kind):
        for direction, cond in ((0, has_low & jnp.logical_not(up_light)), (1, has_high & up_light)):
            @pl.when(cond)
            def _(direction=direction):
                wcopy(kind, vs, direction).start()
        wcopy(kind, vs, 2).start()

    def own_near(kind):
        for direction, cond in ((0, has_low & up_light), (1, has_high & jnp.logical_not(up_light))):
            @pl.when(cond)
            def _(direction=direction):
                wcopy(kind, vs, direction).start()

    def own_start(kind):
        own_near(kind)
        own_far(kind)

    def swap(i, slot):
        src, dst = (
            (win_a.at[S], win_a.at[slot]),
            (win_b.at[S], win_b.at[slot]),
            (wo.at[S], wo.at[slot]),
            (ext.at[0], ext.at[1]),
            (lse_buf.at[0], lse_buf.at[1]),
        )[i]
        return remote(src, dst, sw_send.at[i], sw_recv.at[i], swp)

    TH = 2
    part_rows = rows // TH

    def tok_copy(src, q, i, part, dev):
        r = pl.ds(part * part_rows, part_rows)
        return remote(src.at[r], tok.at[q, r], tok_send.at[i], tok_recv.at[q, part], dev)

    tok_d = [tok_copy(tok.at[own_tok], tp, 1, part, sib) for part in range(TH)]
    tok_y = [tok_copy(tok.at[own_tok], tp, 0, part, (sp, (1 - y) * 2 + x)) for part in range(TH)]
    tok_x = [tok_copy(tok.at[own_tok], tp, 0, part, (z * X + 1 - x, y * 2 + x)) for part in range(TH)]
    load_a.wait()

    @pl.when(home)
    def _():
        own_start(0)

    @pl.when(foreign)
    def _():
        swap(0, sp).start()

    load_tok.wait()
    for part in range(TH):
        tok_x[part].start()
        tok_y[part].start()

    @pl.when(foreign)
    def _():
        for copy in tok_d:
            copy.start()

    def loaded(block, sem):
        pltpu.make_async_copy(block, block, sem).wait()

    loaded(win_b.at[pslot], loc_sem.at[2])
    loaded(wo.at[pslot], loc_sem.at[3])

    @pl.when(home)
    def _():
        own_start(1)

    @pl.when(foreign)
    def _():
        for i in (1, 3, 2):
            swap(i, sp).start()

    MB = 128
    quarter = HEAD_DIM // 4

    def angles(i, carry):
        r = pl.ds(pl.multiple_of(i * MB, MB), MB)
        pos = vs * rows + i * MB + lax.broadcasted_iota(jnp.int32, (MB, kw), 0)
        lane = lax.broadcasted_iota(jnp.int32, (MB, kw), 1) % HEAD_DIM
        freq = jnp.exp((lane % quarter).astype(jnp.float32) * (-4.0 / HEAD_DIM * math.log(rope_base)))
        index = jnp.where(lane >= 2 * quarter, pos % GRID_W, pos // GRID_W)
        angle = index.astype(jnp.float32) * freq
        cos_ref[r, :] = jnp.cos(angle)
        sin_ref[r, :] = jnp.where(lane % (2 * quarter) < quarter, -1.0, 1.0) * jnp.sin(angle)
        return carry

    def comm(kind, dist, only=None, forward=True):
        for up in (0, 1):
            zz = z + dist * (2 * up - 1)
            valid = (zz >= 0) & (zz < Z)
            if only is not None:
                valid = valid & only

            @pl.when(valid)
            def _(zz=zz, up=up):
                slot = zz * X + c
                wcopy(kind, slot, 2).wait_recv()

                if forward:
                    @pl.when(has_low if up else has_high)
                    def _():
                        wcopy(kind, slot, 0 if up else 1).start()
                wcopy(kind, slot, 2).start()

    def relay(cc, part):
        q = y * 2 + cc
        return tok_copy(tok.at[q], q, 1, part, ynb)

    def tok_wait(q, part):
        tok_copy(tok.at[q], q, 0, part, ynb).wait_recv()

    RB = 64

    def norm_rows(i, carry):
        r = pl.ds(pl.multiple_of(i * RB, RB), RB)
        total = jnp.zeros((RB, 1), jnp.float32)
        for t in range(TP):
            v = tok[t, r, :].astype(jnp.float32)
            total += jnp.sum(v * v, axis=1, keepdims=True)
        scale = lax.rsqrt(total / (TP * width) + norm_eps)
        for t in range(TP):
            v = tok[t, r, :].astype(jnp.float32)
            g = gain_ref[:, t * width:(t + 1) * width]
            normed[r, t * width:(t + 1) * width] = (v * scale * g).astype(jnp.bfloat16)
        return carry

    pdepth = X * depth

    def project(kind, first, planes, fresh):
        win, acc = ((win_a, acc_a), (win_b, acc_b))[kind]
        n = acc.shape[1]
        kk = planes * pdepth
        for p in range(planes):
            wcopy(kind, (first + p) * X + 1 - c, 2).wait_recv()
        pb = acc.shape[0] // 2

        def body(i, carry):
            r = pl.ds(pl.multiple_of(i * pb, 16), pb)
            k = pl.ds(pl.multiple_of(first * pdepth, pdepth), kk)
            weight = win[pl.ds(first * X, planes * X)].reshape(kk, n)
            prod = jnp.dot(normed[r, k], weight, preferred_element_type=jnp.float32)
            if fresh:
                acc[r, :] = prod
            else:
                acc[r, :] += prod
            return carry
        lax.fori_loop(0, 2, body, 0)

    def each_side(dist, fn):
        def step(side, carry):
            zz = z + dist * (2 * side - 1)

            @pl.when((zz >= 0) & (zz < Z))
            def _():
                fn(zz)
            return carry
        lax.fori_loop(0, 2, step, 0)

    def halo(i, src, dst, dev):
        return remote(src, dst, halo_sem.at[2 * i], halo_sem.at[2 * i + 1], dev)

    kv_next = halo(0, kvp.at[pl.ds(rows, WINDOW)], kvp.at[pl.ds(0, WINDOW)], next_dev)
    kv_prev = halo(1, kvp.at[pl.ds(WINDOW, WINDOW)], kvp.at[pl.ds(WINDOW + rows, WINDOW)], prev_dev)
    n_next = halo(2, normed.at[pl.ds(rows - NEAR, NEAR)], normed.at[pl.ds(rows + EDGE - NEAR, NEAR)], next_dev)
    n_prev = halo(3, normed.at[pl.ds(0, NEAR)], normed.at[pl.ds(rows + EDGE, NEAR)], prev_dev)

    lax.fori_loop(0, rows // MB, angles, 0)

    @pl.when(foreign)
    def _():
        swap(0, vs).wait_recv()
        own_start(0)
        for cc in (c, 1 - c):
            tok_wait(y * 2 + cc, 0)
            relay(cc, 0).start()

    comm(0, 1)

    @pl.when(foreign)
    def _():
        for cc in (c, 1 - c):
            tok_wait(y * 2 + cc, 1)
            relay(cc, 1).start()

    @pl.when(home)
    def _():
        comm(1, 1)
    comm(0, 2)

    @pl.when(foreign)
    def _():
        swap(1, vs).wait_recv()
        own_start(1)
        swap(3, vs).wait_recv()

    @pl.when(home)
    def _():
        own_far(2)
        for part in range(TH):
            tok_wait(y * 2 + 1 - c, part)
    for part in range(TH):
        if part == TH - 1:
            for dist in range(3, Z):
                comm(0, dist)
        for cc in range(2):
            tok_wait((1 - y) * 2 + cc, part)
        lax.fori_loop(part * (part_rows // RB), (part + 1) * (part_rows // RB), norm_rows, 0)

    @pl.when(has_next)
    def _():
        n_next.start()

    @pl.when(has_prev)
    def _():
        n_prev.start()

    @pl.when(home)
    def _():
        comm(1, 2)

    project(0, jnp.int32(0), Z, True)

    @pl.when(foreign)
    def _():
        comm(1, 1, inner)
        swap(2, vs).wait_recv()
        own_far(2)
        comm(1, 1, outer)

    def turned(v, cosv, sinv):
        lane = lax.broadcasted_iota(jnp.int32, v.shape, 1)
        partner = jnp.where(
            lane % (2 * quarter) < quarter,
            pltpu.roll(v, v.shape[1] - quarter, 1),
            pltpu.roll(v, quarter, 1),
        )
        return v * cosv + partner * sinv

    def k_rows(i, carry):
        r = pl.ds(pl.multiple_of(i * MB, MB), MB)
        v = acc_a[r, qw:qw + kw]
        lane = lax.broadcasted_iota(jnp.int32, v.shape, 1)
        kv = jnp.where(lane < HEAD_DIM, turned(v, cos_ref[r, :], sin_ref[r, :]), v)
        kvp[pl.ds(pl.multiple_of(WINDOW + i * MB, MB), MB), :] = kv.astype(jnp.bfloat16)
        return carry

    lax.fori_loop(0, rows // MB, k_rows, 0)

    @pl.when(has_next)
    def _():
        kv_next.start()

    @pl.when(has_prev)
    def _():
        kv_prev.start()

    def q_rows(i, carry):
        r = pl.ds(pl.multiple_of(i * MB, MB), MB)
        for k in range(qw // kw):
            qbuf[r, k * kw:(k + 1) * kw] = turned(
                acc_a[r, k * kw:(k + 1) * kw], cos_ref[r, :], sin_ref[r, :]
            ).astype(jnp.bfloat16)
        return carry

    lax.fori_loop(0, rows // MB, q_rows, 0)

    K3 = 3 * WINDOW
    total_tokens = rows * S

    guest_dev = (sp + X * jnp.where(inner == up_light, -1, 1), tp)

    def guest_copy(half, r):
        return remote(ac.at[half, r], acg.at[half, r], g_send.at[half], g_recv.at[half], guest_dev)

    def attend(b, carry):
        r = pl.ds(pl.multiple_of(b * WINDOW, WINDOW), WINDOW)
        kv = kvp[pl.ds(pl.multiple_of(b * WINDOW, WINDOW), K3), :].astype(jnp.float32)
        lane = lax.broadcasted_iota(jnp.int32, (K3, kw), 1)
        swapped = pltpu.roll(kv, HEAD_DIM, 1)
        kk = jnp.where(lane < HEAD_DIM, kv, swapped).astype(jnp.bfloat16)
        vv = jnp.where(lane < HEAD_DIM, swapped, kv).astype(jnp.bfloat16)
        k_half = [jnp.where(lane < HEAD_DIM, kk, 0), jnp.where(lane < HEAD_DIM, 0, kk)]
        v_half = [jnp.where(lane < HEAD_DIM, vv, 0), jnp.where(lane < HEAD_DIM, 0, vv)]
        qi = lax.broadcasted_iota(jnp.int32, (WINDOW, K3), 0)
        ki = lax.broadcasted_iota(jnp.int32, (WINDOW, K3), 1)
        first = vs * rows + b * WINDOW - WINDOW
        allowed = (ki >= qi) & (ki <= qi + 2 * WINDOW) & (ki + first >= 0) & (ki + first < total_tokens)
        lse_lane = lax.broadcasted_iota(jnp.int32, (WINDOW, WINDOW), 1)
        lse_all = jnp.zeros((WINDOW, WINDOW), jnp.float32)
        for pair in range(heads // 2):
            q = qbuf[r, pair * kw:(pair + 1) * kw]
            total = jnp.zeros((WINDOW, kw), jnp.float32)
            for side in range(2):
                h = pair * 2 + side
                s = lax.dot_general(
                    q, k_half[side], (((1,), (1,)), ((), ())), preferred_element_type=jnp.float32
                ) * HEAD_DIM ** (-0.5)
                s = jnp.where(allowed, s, -jnp.inf)
                sink = ext[role, 3 + h:4 + h, 0:WINDOW]
                top = jnp.maximum(jnp.max(s, axis=1, keepdims=True), sink)
                e = jnp.exp(s - jnp.concatenate([top] * 3, axis=1))
                den = jnp.sum(e, axis=1, keepdims=True) + jnp.exp(sink - top)
                w = (e * jnp.concatenate([1.0 / den] * 3, axis=1)).astype(jnp.bfloat16)
                total += jnp.dot(w, v_half[side], preferred_element_type=jnp.float32)
                lse_all = jnp.where(lse_lane == h, top + jnp.log(den), lse_all)
            ac[0, r, pair * kw:(pair + 1) * kw] = total.astype(jnp.bfloat16)

        @pl.when(outer)
        def _():
            guest_copy(0, r).start()
        lse_buf[0, :, r] = jnp.transpose(lse_all)[0:heads, :]
        return carry

    blocks = rows // WINDOW
    zero_kv = jnp.zeros((WINDOW, kw), jnp.bfloat16)

    def prev_ready():
        @pl.when(has_prev)
        def _():
            kv_next.wait_recv()

        @pl.when(jnp.logical_not(has_prev))
        def _():
            kvp[0:WINDOW, :] = zero_kv

    def next_ready():
        @pl.when(has_next)
        def _():
            kv_prev.wait_recv()

        @pl.when(jnp.logical_not(has_next))
        def _():
            kvp[WINDOW + rows:, :] = zero_kv

    def edge_ready(at_start):
        @pl.when(at_start)
        def _():
            prev_ready()

        @pl.when(jnp.logical_not(at_start))
        def _():
            next_ready()

    def attend_from(i, carry):
        near = jnp.where(c == 0, blocks - 1, 0)
        edge_block = jnp.where(i == blocks - 2, near, blocks - 1 - near)
        return attend(jnp.where(i < blocks - 2, i + 1, edge_block), carry)

    def b_ready():
        @pl.when(has_prev)
        def _():
            n_next.wait_recv()

        @pl.when(has_next)
        def _():
            n_prev.wait_recv()

        zero_n = jnp.zeros((NEAR, TP * width), jnp.bfloat16)
        normed[rows:rows + EDGE - NEAR, :] = zero_n
        normed[rows + EDGE + NEAR:, :] = zero_n

        @pl.when(jnp.logical_not(has_prev))
        def _():
            normed[rows + EDGE - NEAR:rows + EDGE, :] = zero_n

        @pl.when(jnp.logical_not(has_next))
        def _():
            normed[rows + EDGE:rows + EDGE + NEAR, :] = zero_n

    @pl.when(home)
    def _():
        for dist in range(3, Z):
            comm(1, dist)

    lax.fori_loop(0, blocks - 2, attend_from, 0)
    edge_ready(c == 1)
    b_ready()

    @pl.when(foreign)
    def _():
        comm(1, 2)
        own_near(2)
    lax.fori_loop(blocks - 2, blocks - 1, attend_from, 0)
    edge_ready(c == 0)
    lax.fori_loop(blocks - 1, blocks, attend_from, 0)

    @pl.when(foreign)
    def _():
        swap(4, sp).start()

    project(1, jnp.where(up_light, 0, 1), Z - 1, True)

    @pl.when(home)
    def _():
        own_near(2)

    @pl.when(foreign)
    def _():
        for dist in range(3, Z):
            comm(1, dist)
    project(1, far, 1, False)
    comm(2, 1, inner)

    def gated(lo, n):
        return (acc_b[lo:lo + n, cw:2 * cw] * acc_b[lo:lo + n, 2 * cw:3 * cw]).astype(jnp.bfloat16)

    for i in range(rows // MB):
        cf[8 + i * MB:8 + (i + 1) * MB, :] = gated(i * MB, MB).astype(jnp.float32)
    edge = gated(rows, 2 * EDGE).astype(jnp.float32)
    cf[0:8, :] = edge[EDGE - 8:EDGE, :]
    cf[8 + rows:16 + rows, :] = edge[EDGE:EDGE + 8, :]

    taps = [ext[role, t:t + 1, :] for t in range(3)]
    for i in range(rows // MB):
        a = 8 + i * MB
        conv = (
            taps[0] * cf[a - 1:a - 1 + MB, :]
            + taps[1] * cf[a:a + MB, :]
            + taps[2] * cf[a + 1:a + 1 + MB, :]
        )
        ac[1, i * MB:(i + 1) * MB, :] = (acc_b[i * MB:(i + 1) * MB, 0:cw] * conv).astype(jnp.bfloat16)

        @pl.when(outer)
        def _(i=i):
            guest_copy(1, pl.ds(i * MB, MB)).start()

    mine_dev = (z * X + c, y * 2 + c)
    other_dev = (z * X + c, y * 2 + 1 - c)

    def r1(s, src, dst, dev, extra=0):
        return remote(send1.at[s, src], recv1.at[s, dst], r_send.at[extra], r_recv.at[s, dst], dev)

    def r2(s, src, dst, dev, sem, extra=0):
        return remote(send2.at[s, src], recv2.at[s, dst], r_send.at[2 + extra], r_recv.at[s, sem], dev)

    def out_dot(src, w, yo, m):
        co = c if m == 0 else 1 - c
        r = pl.ds(pl.multiple_of((2 * yo + co) * chunk, chunk), chunk)
        both = jnp.concatenate([src[0, r, :], src[1, r, :]], axis=1)
        return jnp.dot(both, wo[w], preferred_element_type=jnp.float32)

    def produce_x(s, w, src):
        for m in (1, 0):
            for yo in range(2):
                v = out_dot(src, w, yo, m)
                if m == 0:
                    keep[s, yo] = v
                send1[s, m, yo] = v.astype(jnp.bfloat16)
            if m == 1:
                r1(s, 1, role, other_dev).start()

        @pl.when(foreign)
        def _():
            r1(s, 0, 1, mine_dev, 1).start()

    def produce_y(s, w, src):
        for m in range(2):
            send1[s, 0, m] = out_dot(src, w, 1 - y, m).astype(jnp.bfloat16)
        r1(s, 0, 0, ynb).start()
        for m in range(2):
            keep[s, m] = out_dot(src, w, y, m)

    def stage_x(s):
        r1(s, 0, 1, mine_dev).wait_recv()

        def pass_on(base):
            send2[s, 0] = (base(1 - y) + recv1[s, 1, 1 - y].astype(jnp.float32)).astype(jnp.bfloat16)
            r2(s, 0, 0, ynb, 2).start()
            keep[s, y] = base(y) + recv1[s, 1, y].astype(jnp.float32)

        @pl.when(home)
        def _():
            pass_on(lambda yo: keep[s, yo])

        @pl.when(foreign)
        def _():
            r1(s, 1, 0, other_dev).wait_recv()
            pass_on(lambda yo: recv1[s, 0, yo].astype(jnp.float32))

    def stage_y(s):
        r1(s, 0, 0, ynb).wait_recv()
        send2[s, 1] = (keep[s, 1] + recv1[s, 0, 1].astype(jnp.float32)).astype(jnp.bfloat16)
        r2(s, 1, role, other_dev, 1 + role).start()
        mine = keep[s, 0] + recv1[s, 0, 0].astype(jnp.float32)

        @pl.when(home)
        def _():
            keep[s, 0] = mine

        @pl.when(foreign)
        def _():
            send2[s, 0] = mine.astype(jnp.bfloat16)
            r2(s, 0, 1, mine_dev, 2, 1).start()

    def place(s, v):
        out_ref[:, pl.ds(pl.multiple_of(s * cols, cols), cols)] = v.astype(jnp.bfloat16)

    def finish_x(s, place=place):
        r2(s, 0, 0, ynb, 2).wait_recv()
        place(s, keep[s, y] + recv2[s, 0].astype(jnp.float32))

    def finish_y(s, place=place):
        r2(s, 0, 1, mine_dev, 2).wait_recv()
        arrived = recv2[s, 1].astype(jnp.float32)

        @pl.when(home)
        def _():
            place(s, keep[s, 0] + arrived)

        @pl.when(foreign)
        def _():
            r2(s, 1, 0, other_dev, 1).wait_recv()
            place(s, recv2[s, 0].astype(jnp.float32) + arrived)

    def produce_from(b, zz, src):
        produce_x(b, zz * X, src)
        produce_y(b + 1, zz * X + 1, src)

    def produce(zz):
        def sibling_ready():
            wcopy(2, zz * X + 1 - c, 2).wait_recv()

        @pl.when(c == 0)
        def _():
            produce_x(zz * X, zz * X, ac)
            sibling_ready()
            produce_y(zz * X + 1, zz * X + 1, ac)

        @pl.when(c == 1)
        def _():
            produce_y(zz * X + 1, zz * X + 1, ac)
            sibling_ready()
            produce_x(zz * X, zz * X, ac)

    def stage(zz):
        stage_x(zz * X)
        stage_y(zz * X + 1)

    def finish(zz):
        finish_x(zz * X)
        finish_y(zz * X + 1)

    def hand_back(i):
        return remote(gout.at[i], gin.at[i], g_send.at[2 + i], g_recv.at[2 + i], guest_dev)

    def back(i):
        def put(s, v):
            gout[i] = v.astype(jnp.bfloat16)
            hand_back(i).start()
        return put

    produce(z)
    comm(2, 1, outer)
    each_side(1, produce)
    comm(2, 2, inner, False)
    stage(z)
    comm(2, 2, outer, False)

    @pl.when(outer)
    def _():
        each_side(2, produce)
        each_side(1, stage)

    @pl.when(inner)
    def _():
        for half in range(2):
            remote(acg.at[half], acg.at[half], g_send.at[half], g_recv.at[half], guest_dev).wait_recv()
        wcopy(2, far * X + 1 - c, 2).wait_recv()
        produce_from(S, far, acg)
        each_side(1, stage)
        stage(Z)
        produce_from(far * X, far, ac)
    @pl.when(inner)
    def _():
        finish_x(S, back(0))
        finish_y(S + 1, back(1))
    each_side(2, stage)
    finish(z)
    each_side(1, finish)
    each_side(2, finish)

    @pl.when(inner)
    def _():
        for i in range(2):
            hand_back(i).wait_send()

    @pl.when(outer)
    def _():
        for i in range(2):
            hand_back(i).wait_recv()
            place(far * X + i, gin[i])
        for half in range(2):
            sent(ac.at[half], g_send.at[half])

    @pl.when(home)
    def _():
        lse_ref[...] = lse_buf[0]

    @pl.when(foreign)
    def _():
        swap(4, vs).wait_recv()
        lse_ref[...] = lse_buf[1]
        for i in range(5):
            swap(i, sp).wait_send()

    @pl.when(has_next)
    def _():
        kv_next.wait_send()
        n_next.wait_send()

    @pl.when(has_prev)
    def _():
        kv_prev.wait_send()
        n_prev.wait_send()

    sent(tok.at[pl.ds(0, 2)], tok_send.at[0])
    for cond, pairs, along in ((inner, Z + 1, Z + 1), (outer, Z - 1, 1)):
        @pl.when(cond)
        def _(pairs=pairs, along=along):
            for kind in range(3):
                fewer = 1 if kind == 2 and along > 1 else 0
                sent(bufs[kind].at[pl.ds(0, along - fewer)], wz_send.at[kind])
                sent(bufs[kind].at[pl.ds(0, Z if kind < 2 else min(pairs, Z))], wd_send.at[kind])
            sent(send1.at[pl.ds(0, pairs)], r_send.at[0])
            sent(send2.at[pl.ds(0, pairs)], r_send.at[2])

            @pl.when(foreign)
            def _():
                sent(send1.at[pl.ds(0, pairs), 0], r_send.at[1])
                sent(send2.at[pl.ds(0, pairs), 0], r_send.at[3])

    @pl.when(foreign)
    def _():
        sent(tok.at[pl.ds(0, 3)], tok_send.at[1])


def fused(
    tokens, norm_gain, w_query, w_key, w_value, w_post_gate, w_pre_gate, w_conv_in,
    conv_taps, sink_logit, w_out_attn, w_out_conv,
):
    S, TP = lax.axis_size("sp"), lax.axis_size("tp")
    X = 2
    Z = S // X
    rows, width = tokens.shape
    depth, qw = w_query.shape
    cw = w_post_gate.shape[1]
    ow, cols = w_out_attn.shape
    heads = qw // HEAD_DIM
    kw = 2 * HEAD_DIM
    chunk = rows // TP
    bf, f32 = jnp.bfloat16, jnp.float32
    dma = pltpu.SemaphoreType.DMA
    return pl.pallas_call(
        functools.partial(fused_kernel, Z, X),
        out_shape=(
            pltpu.VMEM((chunk, S * cols), bf),
            pltpu.VMEM((heads, rows), f32),
        ),
        in_specs=[
            pl.BlockSpec(memory_space=space)
            for space in (pl.ANY, pltpu.VMEM, pl.ANY, *[pltpu.VMEM] * 2, *[pl.ANY] * 5, pltpu.VMEM, pltpu.SMEM)
        ],
        out_specs=(pl.BlockSpec(memory_space=pltpu.VMEM),) * 2,
        scratch_shapes=[
            pltpu.VMEM((rows, kw), f32),
            pltpu.VMEM((rows, kw), f32),
            pltpu.VMEM((TP + 1, rows, width), bf),
            pltpu.VMEM((rows + 2 * EDGE, TP * width), bf),
            pltpu.VMEM((S + 1, depth, qw + kw), bf),
            pltpu.VMEM((S + 1, depth, 3 * cw), bf),
            pltpu.VMEM((S + 1, ow + cw, cols), bf),
            pltpu.VMEM((rows, qw + kw), f32),
            pltpu.VMEM((rows + 2 * EDGE, 3 * cw), f32),
            pltpu.VMEM((rows, qw), bf),
            pltpu.VMEM((rows + 2 * WINDOW, kw), bf),
            pltpu.VMEM((rows + 16, cw), f32),
            pltpu.VMEM((2, rows, qw), bf),
            pltpu.VMEM((2, rows, qw), bf),
            pltpu.VMEM((2, -(-(3 + heads) // 8) * 8, cw), f32),
            pltpu.VMEM((2, heads, rows), f32),
            pltpu.VMEM((S + X, 2, chunk, cols), f32),
            pltpu.VMEM((S + X, 2, 2, chunk, cols), bf),
            pltpu.VMEM((S + X, 2, 2, chunk, cols), bf),
            pltpu.VMEM((S + X, 2, chunk, cols), bf),
            pltpu.VMEM((S + X, 2, chunk, cols), bf),
            pltpu.VMEM((X, chunk, cols), bf),
            pltpu.VMEM((X, chunk, cols), bf),
            dma((2,)), dma((TP, 2)),
            dma((3,)), dma((3,)), dma((3, S)),
            dma((5,)), dma((5,)),
            dma((8,)),
            dma((4,)), dma((S + X, 3)),
            dma((4,)), dma((4,)),
            dma((4,)),
        ],
        compiler_params=pltpu.CompilerParams(
            collective_id=0, has_side_effects=True, vmem_limit_bytes=60 * 1024 * 1024
        ),
    )(
        tokens, norm_gain[None, :], w_query, w_key.T, w_value.T, w_post_gate, w_pre_gate, w_conv_in,
        w_out_attn, w_out_conv, conv_taps, sink_logit,
    )


def fits(
    tokens, norm_gain, w_query, w_key, w_value, w_post_gate, w_pre_gate, w_conv_in,
    conv_taps, sink_logit, w_out_attn, w_out_conv,
):
    S, TP = lax.axis_size("sp"), lax.axis_size("tp")
    return (
        TP == 4
        and S % 2 == 0
        and S == 8
        and w_key.shape[1] == HEAD_DIM
        and w_query.shape[0] % 128 == 0
        and w_query.shape[1] % 128 == 0
        and w_post_gate.shape[1] == w_query.shape[1]
        and w_out_attn.shape[1] % 128 == 0
        and tokens.shape[0] % (TP * WINDOW) == 0
        and tokens.shape[1] % 128 == 0
    )


def either(*args):
    return fused(*args) if fits(*args) else on_device(*args)


def solution(mesh):
    placed = (
        P("sp", "tp"),
        P(),
        P("sp", "tp"),
        P("sp", "tp"),
        P("sp", "tp"),
        P("sp", "tp"),
        P("sp", "tp"),
        P("sp", "tp"),
        P(None, "tp"),
        P("tp"),
        P("tp", "sp"),
        P("tp", "sp"),
    )
    return jax.shard_map(
        either,
        mesh=mesh,
        in_specs=placed,
        out_specs=(P(("sp", "tp"), None), P("tp", "sp")),
        check_vma=False,
    )
```

```python
import functools
import math

import jax
import jax.numpy as jnp
from jax import lax
from jax.experimental import pallas as pl
from jax.experimental.pallas import tpu as pltpu
from jax.sharding import PartitionSpec as P

MESH = pl.DeviceIdType.MESH

HEAD_DIM = 64
WINDOW = 128
GRID_W = 64
EDGE = 16
NEAR = 8


rope_base = 10000.0
norm_eps = 1e-06


def padded(block, sides, width):
    for axis, dim in sides:
        count = lax.axis_size(axis)
        forward = [(i, i + 1) for i in range(count - 1)]
        backward = [(target, source) for source, target in forward]
        low = lax.ppermute(
            lax.slice_in_dim(block, block.shape[dim] - width, None, axis=dim), axis, forward
        )
        high = lax.ppermute(lax.slice_in_dim(block, 0, width, axis=dim), axis, backward)
        block = jnp.concatenate([low, block, high], axis=dim)
    return block


def rotate_pair(values, angles):
    first_half, second_half = jnp.split(values, 2, axis=-1)
    cosine = jnp.cos(angles)[:, None, :]
    sine_part = jnp.sin(angles)[:, None, :]
    return jnp.concatenate(
        [
            first_half * cosine - second_half * sine_part,
            first_half * sine_part + second_half * cosine,
        ],
        axis=-1,
    )


def axial_rotate(values, positions):
    half_dim = values.shape[-1] // 2
    inv_freq = rope_base ** (-jnp.arange(0, half_dim, 2).astype(jnp.float32) / half_dim)
    row_angle = (positions // GRID_W).astype(jnp.float32)[:, None] * inv_freq
    col_angle = (positions % GRID_W).astype(jnp.float32)[:, None] * inv_freq
    row_part, col_part = jnp.split(values, 2, axis=-1)
    return jnp.concatenate(
        [rotate_pair(row_part, row_angle), rotate_pair(col_part, col_angle)], axis=-1
    )


def block_windows(source, rows_local, blocks):
    pieces = [
        source[step * WINDOW : step * WINDOW + rows_local].reshape(
            (blocks, WINDOW) + source.shape[1:]
        )
        for step in range(3)
    ]
    return jnp.concatenate(pieces, axis=1)


def on_device(
    tokens,
    norm_gain,
    w_query,
    w_key,
    w_value,
    w_post_gate,
    w_pre_gate,
    w_conv_in,
    conv_taps,
    sink_logit,
    w_out_attn,
    w_out_conv,
):
    whole = lax.all_gather(tokens, "tp", axis=1, tiled=True)
    rows_local = whole.shape[0]
    whole_float = whole.astype(jnp.float32)
    mean_square = jnp.mean(whole_float * whole_float, axis=1, keepdims=True)
    normed = (whole_float * lax.rsqrt(mean_square + norm_eps) * norm_gain).astype(jnp.bfloat16)
    col_widths = [
        w_query.shape[1],
        w_key.shape[1],
        w_value.shape[1],
        w_post_gate.shape[1],
        w_pre_gate.shape[1],
        w_conv_in.shape[1],
    ]
    joined = jnp.concatenate(
        (
            lax.all_gather(w_query, "sp", axis=0, tiled=True),
            lax.all_gather(w_key, "sp", axis=0, tiled=True),
            lax.all_gather(w_value, "sp", axis=0, tiled=True),
            lax.all_gather(w_post_gate, "sp", axis=0, tiled=True),
            lax.all_gather(w_pre_gate, "sp", axis=0, tiled=True),
            lax.all_gather(w_conv_in, "sp", axis=0, tiled=True),
        ),
        axis=1,
    )
    projected = jnp.dot(normed, joined, preferred_element_type=jnp.float32)
    bounds = []
    running = 0
    for col_width in col_widths[:-1]:
        running += col_width
        bounds.append(running)
    query_raw, key_raw, value_raw, post_gate, pre_gate, conv_input = jnp.split(
        projected, bounds, axis=1
    )
    offset = lax.axis_index("sp") * rows_local
    positions = offset + jnp.arange(rows_local, dtype=jnp.int32)
    local_heads = w_query.shape[1] // HEAD_DIM
    local_groups = w_key.shape[1] // HEAD_DIM
    group_size = local_heads // local_groups
    queries = axial_rotate(query_raw.reshape(rows_local, local_heads, HEAD_DIM), positions).astype(
        jnp.bfloat16
    )
    keys_rot = axial_rotate(key_raw.reshape(rows_local, local_groups, HEAD_DIM), positions).astype(
        jnp.bfloat16
    )
    key_value = jnp.concatenate(
        [keys_rot.reshape(rows_local, local_groups * HEAD_DIM), value_raw.astype(jnp.bfloat16)],
        axis=1,
    )
    mixed_input = (pre_gate * conv_input).astype(jnp.bfloat16)
    kv_padded = padded(key_value, (("sp", 0),), WINDOW)
    conv_padded = padded(mixed_input, (("sp", 0),), 1)
    conv_float = conv_padded.astype(jnp.float32)
    convolved = (
        conv_taps[0] * conv_float[:-2]
        + conv_taps[1] * conv_float[1:-1]
        + conv_taps[2] * conv_float[2:]
    )
    conv_out = (post_gate * convolved).astype(jnp.bfloat16)
    total_tokens = rows_local * lax.axis_size("sp")
    blocks = rows_local // WINDOW
    padded_rows = rows_local + 2 * WINDOW
    block_queries = queries.reshape(blocks, WINDOW, local_groups, group_size, HEAD_DIM)
    block_keys = block_windows(
        kv_padded[:, : local_groups * HEAD_DIM].reshape(padded_rows, local_groups, HEAD_DIM),
        rows_local,
        blocks,
    )
    block_values = block_windows(
        kv_padded[:, local_groups * HEAD_DIM :].reshape(padded_rows, local_groups, HEAD_DIM),
        rows_local,
        blocks,
    )
    scores = jnp.einsum(
        "nqkgd,nskd->nkgqs", block_queries, block_keys, preferred_element_type=jnp.float32
    ) * HEAD_DIM ** (-0.5)
    query_pos = positions.reshape(blocks, WINDOW)
    key_pos = (
        offset
        - WINDOW
        + (jnp.arange(blocks, dtype=jnp.int32) * WINDOW)[:, None]
        + jnp.arange(3 * WINDOW, dtype=jnp.int32)[None, :]
    )
    distance = key_pos[:, None, :] - query_pos[:, :, None]
    allowed = (
        (jnp.abs(distance) <= WINDOW)
        & (key_pos >= 0)[:, None, :]
        & (key_pos < total_tokens)[:, None, :]
    )
    scores = jnp.where(allowed[:, None, None], scores, -jnp.inf)
    sink_values = sink_logit.reshape(local_groups, group_size)[None, :, :, None]
    row_max = jnp.maximum(jnp.max(scores, axis=-1), sink_values)
    exp_scores = jnp.exp(scores - row_max[..., None])
    denominator = jnp.sum(exp_scores, axis=-1) + jnp.exp(sink_values - row_max)
    weights = (exp_scores / denominator[..., None]).astype(jnp.bfloat16)
    attended = (
        jnp.einsum("nkgqs,nskd->nqkgd", weights, block_values, preferred_element_type=jnp.float32)
        .astype(jnp.bfloat16)
        .reshape(rows_local, local_heads * HEAD_DIM)
    )
    log_sum = row_max + jnp.log(denominator)
    log_weight_sum = jnp.transpose(log_sum, (1, 2, 0, 3)).reshape(local_heads, rows_local)
    out_attn, out_conv = (
        lax.all_gather(w_out_attn, "sp", axis=1, tiled=True),
        lax.all_gather(w_out_conv, "sp", axis=1, tiled=True),
    )
    mixed = lax.psum_scatter(
        (
            jnp.dot(attended, out_attn, preferred_element_type=jnp.float32)
            + jnp.dot(conv_out, out_conv, preferred_element_type=jnp.float32)
        ).astype(jnp.bfloat16),
        "tp",
        scatter_dimension=0,
        tiled=True,
    )
    return (mixed, log_weight_sum)


def fused_kernel(
    Z, X,
    tok_ref, gain_ref, wq_ref, wk_ref, wv_ref, wpost_ref, wpre_ref, wcin_ref, oa_ref, oc_ref, taps_ref, sink_ref,
    out_ref, lse_ref,
    cos_ref, sin_ref, tok, normed, win_a, win_b, wo, acc_a, acc_b, qbuf, kvp, cf, ac, acg, ext, lse_buf,
    keep, send1, recv1, send2, recv2, gout, gin,
    tok_send, tok_recv, wz_send, wd_send, w_recv, sw_send, sw_recv, halo_sem, r_send, r_recv, g_send, g_recv, loc_sem,
):
    S = Z * X
    rows, width = tok_ref.shape
    depth = wq_ref.shape[0]
    ow, cols = oa_ref.shape
    qw = qbuf.shape[1]
    cw = cf.shape[1]
    kw = 2 * HEAD_DIM
    TP = tok.shape[0] - 1
    chunk = rows // TP
    sp = lax.axis_index("sp")
    tp = lax.axis_index("tp")
    z, x = sp // X, sp % X
    c, y = tp % 2, tp // 2
    vs = z * X + c
    home, foreign = c == x, c != x
    role = jnp.where(home, 0, 1)
    sib = (sp, y * 2 + 1 - c)
    ynb = (sp, (1 - y) * 2 + c)
    yoth = (sp, (1 - y) * 2 + 1 - c)
    xnb = (z * X + 1 - x, tp)
    swp = (z * X + 1 - x, y * 2 + 1 - c)
    low, high = (sp - X, tp), (sp + X, tp)
    has_low, has_high = z > 0, z < Z - 1
    has_prev, has_next = vs > 0, vs < S - 1
    vn, vp = vs + 1, vs - 1 + S
    next_dev = ((vn // X) * X + x, y * 2 + vn % X)
    prev_dev = ((vp // X - Z) * X + x, y * 2 + vp % X)

    barrier = pltpu.get_barrier_semaphore()

    def greet(dev):
        pl.semaphore_signal(barrier, inc=1, device_id=dev, device_id_type=MESH)

    for dev in (sib, ynb, yoth, xnb, swp):
        greet(dev)
    peers = 5
    across_z = ((has_low, low), (has_high, high), (has_prev & (c == 0), prev_dev), (has_next & (c == 1), next_dev))
    for cond, dev in across_z:
        @pl.when(cond)
        def _(dev=dev):
            greet(dev)
        peers = peers + jnp.where(cond, 1, 0)

    pslot = jnp.where(home, sp, S)
    own_tok = jnp.where(home, tp, TP)
    load_tok = pltpu.make_async_copy(tok_ref, tok.at[own_tok], loc_sem.at[0])
    load_a = pltpu.make_async_copy(wq_ref, win_a.at[pslot, :, pl.ds(0, qw)], loc_sem.at[1])
    load_b = [
        pltpu.make_async_copy(ref, win_b.at[pslot, :, pl.ds(part * cw, cw)], loc_sem.at[2])
        for part, ref in enumerate((wpost_ref, wpre_ref, wcin_ref))
    ]
    load_c = [
        pltpu.make_async_copy(ref, wo.at[pslot, pl.ds(part * ow, ow)], loc_sem.at[3])
        for part, ref in enumerate((oa_ref, oc_ref))
    ]
    for copy in (load_a, load_tok, *load_b, *load_c):
        copy.start()
    kv_t = jnp.concatenate([wk_ref[...], wv_ref[...]], axis=0).astype(jnp.float32)
    win_a[pslot, :, qw:qw + kw] = jnp.transpose(kv_t).astype(jnp.bfloat16)
    heads = qw // HEAD_DIM
    ext[0] = jnp.zeros(ext.shape[1:], jnp.float32)
    ext[0, 0:3, :] = taps_ref[...]
    for h in range(heads):
        ext[0, 3 + h:4 + h, :] = jnp.full((1, cw), sink_ref[h], jnp.float32)

    pl.semaphore_wait(barrier, peers)

    def remote(src, dst, ssem, rsem, dev):
        return pltpu.make_async_remote_copy(
            src_ref=src, dst_ref=dst, send_sem=ssem, recv_sem=rsem,
            device_id=dev, device_id_type=MESH,
        )

    bufs = (win_a, win_b, wo)
    targets = (low, high, sib)

    def wcopy(kind, slot, direction):
        block = bufs[kind].at[slot]
        ssem = (wz_send, wz_send, wd_send)[direction].at[kind]
        return remote(block, block, ssem, w_recv.at[kind, slot], targets[direction])

    up_light = 2 * z + 1 < Z
    far = jnp.where(up_light, Z - 1, 0)
    inner = has_low & has_high
    outer = jnp.logical_not(inner)

    def sent(block, sem):
        remote(block, block, sem, sem, sib).wait_send()

    def own_far(kind):
        for direction, cond in ((0, has_low & jnp.logical_not(up_light)), (1, has_high & up_light)):
            @pl.when(cond)
            def _(direction=direction):
                wcopy(kind, vs, direction).start()
        wcopy(kind, vs, 2).start()

    def own_near(kind):
        for direction, cond in ((0, has_low & up_light), (1, has_high & jnp.logical_not(up_light))):
            @pl.when(cond)
            def _(direction=direction):
                wcopy(kind, vs, direction).start()

    def own_start(kind):
        own_near(kind)
        own_far(kind)

    def swap(i, slot):
        src, dst = (
            (win_a.at[S], win_a.at[slot]),
            (win_b.at[S], win_b.at[slot]),
            (wo.at[S], wo.at[slot]),
            (ext.at[0], ext.at[1]),
            (lse_buf.at[0], lse_buf.at[1]),
        )[i]
        return remote(src, dst, sw_send.at[i], sw_recv.at[i], swp)

    TH = 2
    part_rows = rows // TH

    def tok_copy(src, q, i, part, dev):
        r = pl.ds(part * part_rows, part_rows)
        return remote(src.at[r], tok.at[q, r], tok_send.at[i], tok_recv.at[q, part], dev)

    tok_d = [tok_copy(tok.at[own_tok], tp, 1, part, sib) for part in range(TH)]
    tok_y = [tok_copy(tok.at[own_tok], tp, 0, part, (sp, (1 - y) * 2 + x)) for part in range(TH)]
    tok_x = [tok_copy(tok.at[own_tok], tp, 0, part, (z * X + 1 - x, y * 2 + x)) for part in range(TH)]
    load_a.wait()

    @pl.when(home)
    def _():
        own_start(0)

    @pl.when(foreign)
    def _():
        swap(0, sp).start()

    load_tok.wait()
    for part in range(TH):
        tok_x[part].start()
        tok_y[part].start()

    @pl.when(foreign)
    def _():
        for copy in tok_d:
            copy.start()

    def loaded(block, sem):
        pltpu.make_async_copy(block, block, sem).wait()

    loaded(win_b.at[pslot], loc_sem.at[2])
    loaded(wo.at[pslot], loc_sem.at[3])

    @pl.when(home)
    def _():
        own_start(1)

    @pl.when(foreign)
    def _():
        for i in (1, 3, 2):
            swap(i, sp).start()

    MB = 128
    quarter = HEAD_DIM // 4

    def angles(i, carry):
        r = pl.ds(pl.multiple_of(i * MB, MB), MB)
        pos = vs * rows + i * MB + lax.broadcasted_iota(jnp.int32, (MB, kw), 0)
        lane = lax.broadcasted_iota(jnp.int32, (MB, kw), 1) % HEAD_DIM
        freq = jnp.exp((lane % quarter).astype(jnp.float32) * (-4.0 / HEAD_DIM * math.log(rope_base)))
        index = jnp.where(lane >= 2 * quarter, pos % GRID_W, pos // GRID_W)
        angle = index.astype(jnp.float32) * freq
        cos_ref[r, :] = jnp.cos(angle)
        sin_ref[r, :] = jnp.where(lane % (2 * quarter) < quarter, -1.0, 1.0) * jnp.sin(angle)
        return carry

    def comm(kind, dist, only=None, forward=True):
        for up in (0, 1):
            zz = z + dist * (2 * up - 1)
            valid = (zz >= 0) & (zz < Z)
            if only is not None:
                valid = valid & only

            @pl.when(valid)
            def _(zz=zz, up=up):
                slot = zz * X + c
                wcopy(kind, slot, 2).wait_recv()

                if forward:
                    @pl.when(has_low if up else has_high)
                    def _():
                        wcopy(kind, slot, 0 if up else 1).start()
                wcopy(kind, slot, 2).start()

    def relay(cc, part):
        q = y * 2 + cc
        return tok_copy(tok.at[q], q, 1, part, ynb)

    def tok_wait(q, part):
        tok_copy(tok.at[q], q, 0, part, ynb).wait_recv()

    RB = 64

    def norm_rows(i, carry):
        r = pl.ds(pl.multiple_of(i * RB, RB), RB)
        total = jnp.zeros((RB, 1), jnp.float32)
        for t in range(TP):
            v = tok[t, r, :].astype(jnp.float32)
            total += jnp.sum(v * v, axis=1, keepdims=True)
        scale = lax.rsqrt(total / (TP * width) + norm_eps)
        for t in range(TP):
            v = tok[t, r, :].astype(jnp.float32)
            g = gain_ref[:, t * width:(t + 1) * width]
            normed[r, t * width:(t + 1) * width] = (v * scale * g).astype(jnp.bfloat16)
        return carry

    pdepth = X * depth

    def project(kind, first, planes, fresh):
        win, acc = ((win_a, acc_a), (win_b, acc_b))[kind]
        n = acc.shape[1]
        kk = planes * pdepth
        for p in range(planes):
            wcopy(kind, (first + p) * X + 1 - c, 2).wait_recv()
        pb = acc.shape[0] // 2

        def body(i, carry):
            r = pl.ds(pl.multiple_of(i * pb, 16), pb)
            k = pl.ds(pl.multiple_of(first * pdepth, pdepth), kk)
            weight = win[pl.ds(first * X, planes * X)].reshape(kk, n)
            prod = jnp.dot(normed[r, k], weight, preferred_element_type=jnp.float32)
            if fresh:
                acc[r, :] = prod
            else:
                acc[r, :] += prod
            return carry
        lax.fori_loop(0, 2, body, 0)

    def each_side(dist, fn):
        def step(side, carry):
            zz = z + dist * (2 * side - 1)

            @pl.when((zz >= 0) & (zz < Z))
            def _():
                fn(zz)
            return carry
        lax.fori_loop(0, 2, step, 0)

    def halo(i, src, dst, dev):
        return remote(src, dst, halo_sem.at[2 * i], halo_sem.at[2 * i + 1], dev)

    kv_next = halo(0, kvp.at[pl.ds(rows, WINDOW)], kvp.at[pl.ds(0, WINDOW)], next_dev)
    kv_prev = halo(1, kvp.at[pl.ds(WINDOW, WINDOW)], kvp.at[pl.ds(WINDOW + rows, WINDOW)], prev_dev)
    n_next = halo(2, normed.at[pl.ds(rows - NEAR, NEAR)], normed.at[pl.ds(rows + EDGE - NEAR, NEAR)], next_dev)
    n_prev = halo(3, normed.at[pl.ds(0, NEAR)], normed.at[pl.ds(rows + EDGE, NEAR)], prev_dev)

    lax.fori_loop(0, rows // MB, angles, 0)

    @pl.when(foreign)
    def _():
        swap(0, vs).wait_recv()
        own_start(0)
        for cc in (c, 1 - c):
            tok_wait(y * 2 + cc, 0)
            relay(cc, 0).start()

    comm(0, 1)

    @pl.when(foreign)
    def _():
        for cc in (c, 1 - c):
            tok_wait(y * 2 + cc, 1)
            relay(cc, 1).start()

    @pl.when(home)
    def _():
        comm(1, 1)
    comm(0, 2)

    @pl.when(foreign)
    def _():
        swap(1, vs).wait_recv()
        own_start(1)
        swap(3, vs).wait_recv()

    @pl.when(home)
    def _():
        own_far(2)
        for part in range(TH):
            tok_wait(y * 2 + 1 - c, part)
    for part in range(TH):
        if part == TH - 1:
            for dist in range(3, Z):
                comm(0, dist)
        for cc in range(2):
            tok_wait((1 - y) * 2 + cc, part)
        lax.fori_loop(part * (part_rows // RB), (part + 1) * (part_rows // RB), norm_rows, 0)

    @pl.when(has_next)
    def _():
        n_next.start()

    @pl.when(has_prev)
    def _():
        n_prev.start()

    @pl.when(home)
    def _():
        comm(1, 2)

    project(0, jnp.int32(0), Z, True)

    @pl.when(foreign)
    def _():
        comm(1, 1, inner)
        swap(2, vs).wait_recv()
        own_far(2)
        comm(1, 1, outer)

    def turned(v, cosv, sinv):
        lane = lax.broadcasted_iota(jnp.int32, v.shape, 1)
        partner = jnp.where(
            lane % (2 * quarter) < quarter,
            pltpu.roll(v, v.shape[1] - quarter, 1),
            pltpu.roll(v, quarter, 1),
        )
        return v * cosv + partner * sinv

    def k_rows(i, carry):
        r = pl.ds(pl.multiple_of(i * MB, MB), MB)
        v = acc_a[r, qw:qw + kw]
        lane = lax.broadcasted_iota(jnp.int32, v.shape, 1)
        kv = jnp.where(lane < HEAD_DIM, turned(v, cos_ref[r, :], sin_ref[r, :]), v)
        kvp[pl.ds(pl.multiple_of(WINDOW + i * MB, MB), MB), :] = kv.astype(jnp.bfloat16)
        return carry

    lax.fori_loop(0, rows // MB, k_rows, 0)

    @pl.when(has_next)
    def _():
        kv_next.start()

    @pl.when(has_prev)
    def _():
        kv_prev.start()

    def q_rows(i, carry):
        r = pl.ds(pl.multiple_of(i * MB, MB), MB)
        for k in range(qw // kw):
            qbuf[r, k * kw:(k + 1) * kw] = turned(
                acc_a[r, k * kw:(k + 1) * kw], cos_ref[r, :], sin_ref[r, :]
            ).astype(jnp.bfloat16)
        return carry

    lax.fori_loop(0, rows // MB, q_rows, 0)

    K3 = 3 * WINDOW
    total_tokens = rows * S

    guest_dev = (sp + X * jnp.where(inner == up_light, -1, 1), tp)

    def guest_copy(half, r):
        return remote(ac.at[half, r], acg.at[half, r], g_send.at[half], g_recv.at[half], guest_dev)

    def attend(b, carry):
        r = pl.ds(pl.multiple_of(b * WINDOW, WINDOW), WINDOW)
        kv = kvp[pl.ds(pl.multiple_of(b * WINDOW, WINDOW), K3), :].astype(jnp.float32)
        lane = lax.broadcasted_iota(jnp.int32, (K3, kw), 1)
        swapped = pltpu.roll(kv, HEAD_DIM, 1)
        kk = jnp.where(lane < HEAD_DIM, kv, swapped).astype(jnp.bfloat16)
        vv = jnp.where(lane < HEAD_DIM, swapped, kv).astype(jnp.bfloat16)
        k_half = [jnp.where(lane < HEAD_DIM, kk, 0), jnp.where(lane < HEAD_DIM, 0, kk)]
        v_half = [jnp.where(lane < HEAD_DIM, vv, 0), jnp.where(lane < HEAD_DIM, 0, vv)]
        qi = lax.broadcasted_iota(jnp.int32, (WINDOW, K3), 0)
        ki = lax.broadcasted_iota(jnp.int32, (WINDOW, K3), 1)
        first = vs * rows + b * WINDOW - WINDOW
        allowed = (ki >= qi) & (ki <= qi + 2 * WINDOW) & (ki + first >= 0) & (ki + first < total_tokens)
        lse_lane = lax.broadcasted_iota(jnp.int32, (WINDOW, WINDOW), 1)
        lse_all = jnp.zeros((WINDOW, WINDOW), jnp.float32)
        for pair in range(heads // 2):
            q = qbuf[r, pair * kw:(pair + 1) * kw]
            total = jnp.zeros((WINDOW, kw), jnp.float32)
            for side in range(2):
                h = pair * 2 + side
                s = lax.dot_general(
                    q, k_half[side], (((1,), (1,)), ((), ())), preferred_element_type=jnp.float32
                ) * HEAD_DIM ** (-0.5)
                s = jnp.where(allowed, s, -jnp.inf)
                sink = ext[role, 3 + h:4 + h, 0:WINDOW]
                top = jnp.maximum(jnp.max(s, axis=1, keepdims=True), sink)
                e = jnp.exp(s - jnp.concatenate([top] * 3, axis=1))
                den = jnp.sum(e, axis=1, keepdims=True) + jnp.exp(sink - top)
                w = (e * jnp.concatenate([1.0 / den] * 3, axis=1)).astype(jnp.bfloat16)
                total += jnp.dot(w, v_half[side], preferred_element_type=jnp.float32)
                lse_all = jnp.where(lse_lane == h, top + jnp.log(den), lse_all)
            ac[0, r, pair * kw:(pair + 1) * kw] = total.astype(jnp.bfloat16)

        @pl.when(outer)
        def _():
            guest_copy(0, r).start()
        lse_buf[0, :, r] = jnp.transpose(lse_all)[0:heads, :]
        return carry

    blocks = rows // WINDOW
    zero_kv = jnp.zeros((WINDOW, kw), jnp.bfloat16)

    def prev_ready():
        @pl.when(has_prev)
        def _():
            kv_next.wait_recv()

        @pl.when(jnp.logical_not(has_prev))
        def _():
            kvp[0:WINDOW, :] = zero_kv

    def next_ready():
        @pl.when(has_next)
        def _():
            kv_prev.wait_recv()

        @pl.when(jnp.logical_not(has_next))
        def _():
            kvp[WINDOW + rows:, :] = zero_kv

    def edge_ready(at_start):
        @pl.when(at_start)
        def _():
            prev_ready()

        @pl.when(jnp.logical_not(at_start))
        def _():
            next_ready()

    def attend_from(i, carry):
        near = jnp.where(c == 0, blocks - 1, 0)
        edge_block = jnp.where(i == blocks - 2, near, blocks - 1 - near)
        return attend(jnp.where(i < blocks - 2, i + 1, edge_block), carry)

    def b_ready():
        @pl.when(has_prev)
        def _():
            n_next.wait_recv()

        @pl.when(has_next)
        def _():
            n_prev.wait_recv()

        zero_n = jnp.zeros((NEAR, TP * width), jnp.bfloat16)
        normed[rows:rows + EDGE - NEAR, :] = zero_n
        normed[rows + EDGE + NEAR:, :] = zero_n

        @pl.when(jnp.logical_not(has_prev))
        def _():
            normed[rows + EDGE - NEAR:rows + EDGE, :] = zero_n

        @pl.when(jnp.logical_not(has_next))
        def _():
            normed[rows + EDGE:rows + EDGE + NEAR, :] = zero_n

    @pl.when(home)
    def _():
        for dist in range(3, Z):
            comm(1, dist)

    lax.fori_loop(0, blocks - 2, attend_from, 0)
    edge_ready(c == 1)
    b_ready()

    @pl.when(foreign)
    def _():
        comm(1, 2)
        own_near(2)
    lax.fori_loop(blocks - 2, blocks - 1, attend_from, 0)
    edge_ready(c == 0)
    lax.fori_loop(blocks - 1, blocks, attend_from, 0)

    @pl.when(foreign)
    def _():
        swap(4, sp).start()

    project(1, jnp.where(up_light, 0, 1), Z - 1, True)

    @pl.when(foreign)
    def _():
        for dist in range(3, Z):
            comm(1, dist)
    project(1, far, 1, False)
    @pl.when(home)
    def _():
        own_near(2)

    comm(2, 1, inner)

    def gated(lo, n):
        return (acc_b[lo:lo + n, cw:2 * cw] * acc_b[lo:lo + n, 2 * cw:3 * cw]).astype(jnp.bfloat16)

    for i in range(rows // MB):
        cf[8 + i * MB:8 + (i + 1) * MB, :] = gated(i * MB, MB).astype(jnp.float32)
    edge = gated(rows, 2 * EDGE).astype(jnp.float32)
    cf[0:8, :] = edge[EDGE - 8:EDGE, :]
    cf[8 + rows:16 + rows, :] = edge[EDGE:EDGE + 8, :]

    taps = [ext[role, t:t + 1, :] for t in range(3)]
    for i in range(rows // MB):
        a = 8 + i * MB
        conv = (
            taps[0] * cf[a - 1:a - 1 + MB, :]
            + taps[1] * cf[a:a + MB, :]
            + taps[2] * cf[a + 1:a + 1 + MB, :]
        )
        ac[1, i * MB:(i + 1) * MB, :] = (acc_b[i * MB:(i + 1) * MB, 0:cw] * conv).astype(jnp.bfloat16)

        @pl.when(outer)
        def _(i=i):
            guest_copy(1, pl.ds(i * MB, MB)).start()

    mine_dev = (z * X + c, y * 2 + c)
    other_dev = (z * X + c, y * 2 + 1 - c)

    def r1(s, src, dst, dev, extra=0):
        return remote(send1.at[s, src], recv1.at[s, dst], r_send.at[extra], r_recv.at[s, dst], dev)

    def r2(s, src, dst, dev, sem, extra=0):
        return remote(send2.at[s, src], recv2.at[s, dst], r_send.at[2 + extra], r_recv.at[s, sem], dev)

    def out_dot(src, w, yo):
        r = pl.ds(pl.multiple_of(yo * 2 * chunk, chunk), 2 * chunk)
        both = jnp.concatenate([src[0, r, :], src[1, r, :]], axis=1)
        v = jnp.dot(both, wo[w], preferred_element_type=jnp.float32)
        return v[0:chunk], v[chunk:2 * chunk]

    def produce_x(s, w, src, core):
        for yo in range(2):
            v = out_dot(src, w, yo)
            keep[s, yo] = v[core]
            send1[s, 0, yo] = v[core].astype(jnp.bfloat16)
            send1[s, 1, yo] = v[1 - core].astype(jnp.bfloat16)
        r1(s, 1, role, other_dev).start()

        @pl.when(foreign)
        def _():
            r1(s, 0, 1, mine_dev, 1).start()

    def produce_y(s, w, src, core):
        v = out_dot(src, w, 1 - y)
        send1[s, 0, 0] = v[core].astype(jnp.bfloat16)
        send1[s, 0, 1] = v[1 - core].astype(jnp.bfloat16)
        r1(s, 0, 0, ynb).start()
        v = out_dot(src, w, y)
        keep[s, 0] = v[core]
        keep[s, 1] = v[1 - core]

    def stage_x(s):
        r1(s, 0, 1, mine_dev).wait_recv()

        def pass_on(base):
            send2[s, 0] = (base(1 - y) + recv1[s, 1, 1 - y].astype(jnp.float32)).astype(jnp.bfloat16)
            r2(s, 0, 0, ynb, 2).start()
            keep[s, y] = base(y) + recv1[s, 1, y].astype(jnp.float32)

        @pl.when(home)
        def _():
            pass_on(lambda yo: keep[s, yo])

        @pl.when(foreign)
        def _():
            r1(s, 1, 0, other_dev).wait_recv()
            pass_on(lambda yo: recv1[s, 0, yo].astype(jnp.float32))

    def stage_y(s):
        r1(s, 0, 0, ynb).wait_recv()
        send2[s, 1] = (keep[s, 1] + recv1[s, 0, 1].astype(jnp.float32)).astype(jnp.bfloat16)
        r2(s, 1, role, other_dev, 1 + role).start()
        mine = keep[s, 0] + recv1[s, 0, 0].astype(jnp.float32)

        @pl.when(home)
        def _():
            keep[s, 0] = mine

        @pl.when(foreign)
        def _():
            send2[s, 0] = mine.astype(jnp.bfloat16)
            r2(s, 0, 1, mine_dev, 2, 1).start()

    def place(s, v):
        out_ref[:, pl.ds(pl.multiple_of(s * cols, cols), cols)] = v.astype(jnp.bfloat16)

    def finish_x(s, place=place):
        r2(s, 0, 0, ynb, 2).wait_recv()
        place(s, keep[s, y] + recv2[s, 0].astype(jnp.float32))

    def finish_y(s, place=place):
        r2(s, 0, 1, mine_dev, 2).wait_recv()
        arrived = recv2[s, 1].astype(jnp.float32)

        @pl.when(home)
        def _():
            place(s, keep[s, 0] + arrived)

        @pl.when(foreign)
        def _():
            r2(s, 1, 0, other_dev, 1).wait_recv()
            place(s, recv2[s, 0].astype(jnp.float32) + arrived)

    def produce_from(b, zz, src, sibling_ready=lambda: None):
        @pl.when(c == 0)
        def _():
            produce_x(b, zz * X, src, 0)
            sibling_ready()
            produce_y(b + 1, zz * X + 1, src, 0)

        @pl.when(c == 1)
        def _():
            produce_y(b + 1, zz * X + 1, src, 1)
            sibling_ready()
            produce_x(b, zz * X, src, 1)

    def produce(zz):
        produce_from(zz * X, zz, ac, lambda: wcopy(2, zz * X + 1 - c, 2).wait_recv())

    def stage(zz):
        stage_x(zz * X)
        stage_y(zz * X + 1)

    def finish(zz):
        finish_x(zz * X)
        finish_y(zz * X + 1)

    def hand_back(i):
        return remote(gout.at[i], gin.at[i], g_send.at[2 + i], g_recv.at[2 + i], guest_dev)

    def back(i):
        def put(s, v):
            gout[i] = v.astype(jnp.bfloat16)
            hand_back(i).start()
        return put

    produce(z)
    comm(2, 1, outer)
    each_side(1, produce)
    comm(2, 2, inner, False)
    stage(z)
    comm(2, 2, outer, False)

    @pl.when(outer)
    def _():
        each_side(2, produce)
        each_side(1, stage)

    @pl.when(inner)
    def _():
        for half in range(2):
            remote(acg.at[half], acg.at[half], g_send.at[half], g_recv.at[half], guest_dev).wait_recv()
        wcopy(2, far * X + 1 - c, 2).wait_recv()
        produce_from(S, far, acg)
        each_side(1, stage)
        stage(Z)
        produce_from(far * X, far, ac)
    @pl.when(inner)
    def _():
        finish_x(S, back(0))
        finish_y(S + 1, back(1))
    each_side(2, stage)
    finish(z)
    each_side(1, finish)
    each_side(2, finish)

    @pl.when(inner)
    def _():
        for i in range(2):
            hand_back(i).wait_send()

    @pl.when(outer)
    def _():
        for i in range(2):
            hand_back(i).wait_recv()
            place(far * X + i, gin[i])
        for half in range(2):
            sent(ac.at[half], g_send.at[half])

    @pl.when(home)
    def _():
        lse_ref[...] = lse_buf[0]

    @pl.when(foreign)
    def _():
        swap(4, vs).wait_recv()
        lse_ref[...] = lse_buf[1]
        for i in range(5):
            swap(i, sp).wait_send()

    @pl.when(has_next)
    def _():
        kv_next.wait_send()
        n_next.wait_send()

    @pl.when(has_prev)
    def _():
        kv_prev.wait_send()
        n_prev.wait_send()

    sent(tok.at[pl.ds(0, 2)], tok_send.at[0])
    for cond, pairs, along in ((inner, Z + 1, Z + 1), (outer, Z - 1, 1)):
        @pl.when(cond)
        def _(pairs=pairs, along=along):
            for kind in range(3):
                fewer = 1 if kind == 2 and along > 1 else 0
                sent(bufs[kind].at[pl.ds(0, along - fewer)], wz_send.at[kind])
                sent(bufs[kind].at[pl.ds(0, Z if kind < 2 else min(pairs, Z))], wd_send.at[kind])
            sent(send1.at[pl.ds(0, pairs)], r_send.at[0])
            sent(send2.at[pl.ds(0, pairs)], r_send.at[2])

            @pl.when(foreign)
            def _():
                sent(send1.at[pl.ds(0, pairs), 0], r_send.at[1])
                sent(send2.at[pl.ds(0, pairs), 0], r_send.at[3])

    @pl.when(foreign)
    def _():
        sent(tok.at[pl.ds(0, 3)], tok_send.at[1])


def fused(
    tokens, norm_gain, w_query, w_key, w_value, w_post_gate, w_pre_gate, w_conv_in,
    conv_taps, sink_logit, w_out_attn, w_out_conv,
):
    S, TP = lax.axis_size("sp"), lax.axis_size("tp")
    X = 2
    Z = S // X
    rows, width = tokens.shape
    depth, qw = w_query.shape
    cw = w_post_gate.shape[1]
    ow, cols = w_out_attn.shape
    heads = qw // HEAD_DIM
    kw = 2 * HEAD_DIM
    chunk = rows // TP
    bf, f32 = jnp.bfloat16, jnp.float32
    dma = pltpu.SemaphoreType.DMA
    mixed, log_sum = pl.pallas_call(
        functools.partial(fused_kernel, Z, X),
        out_shape=(
            pltpu.VMEM((chunk, S * cols), bf),
            pltpu.VMEM((heads, rows), f32),
        ),
        in_specs=[
            pl.BlockSpec(memory_space=space)
            for space in (pl.ANY, pltpu.VMEM, pl.ANY, *[pltpu.VMEM] * 2, *[pl.ANY] * 5, pltpu.VMEM, pltpu.SMEM)
        ],
        out_specs=(pl.BlockSpec(memory_space=pltpu.VMEM),) * 2,
        scratch_shapes=[
            pltpu.VMEM((rows, kw), f32),
            pltpu.VMEM((rows, kw), f32),
            pltpu.VMEM((TP + 1, rows, width), bf),
            pltpu.VMEM((rows + 2 * EDGE, TP * width), bf),
            pltpu.VMEM((S + 1, depth, qw + kw), bf),
            pltpu.VMEM((S + 1, depth, 3 * cw), bf),
            pltpu.VMEM((S + 1, ow + cw, cols), bf),
            pltpu.VMEM((rows, qw + kw), f32),
            pltpu.VMEM((rows + 2 * EDGE, 3 * cw), f32),
            pltpu.VMEM((rows, qw), bf),
            pltpu.VMEM((rows + 2 * WINDOW, kw), bf),
            pltpu.VMEM((rows + 16, cw), f32),
            pltpu.VMEM((2, rows, qw), bf),
            pltpu.VMEM((2, rows, qw), bf),
            pltpu.VMEM((2, -(-(3 + heads) // 8) * 8, cw), f32),
            pltpu.VMEM((2, heads, rows), f32),
            pltpu.VMEM((S + X, 2, chunk, cols), f32),
            pltpu.VMEM((S + X, 2, 2, chunk, cols), bf),
            pltpu.VMEM((S + X, 2, 2, chunk, cols), bf),
            pltpu.VMEM((S + X, 2, chunk, cols), bf),
            pltpu.VMEM((S + X, 2, chunk, cols), bf),
            pltpu.VMEM((X, chunk, cols), bf),
            pltpu.VMEM((X, chunk, cols), bf),
            dma((2,)), dma((TP, 2)),
            dma((3,)), dma((3,)), dma((3, S)),
            dma((5,)), dma((5,)),
            dma((8,)),
            dma((4,)), dma((S + X, 3)),
            dma((4,)), dma((4,)),
            dma((4,)),
        ],
        compiler_params=pltpu.CompilerParams(
            collective_id=0, has_side_effects=True, vmem_limit_bytes=60 * 1024 * 1024
        ),
    )(
        tokens, norm_gain[None, :], w_query, w_key.T, w_value.T, w_post_gate, w_pre_gate, w_conv_in,
        w_out_attn, w_out_conv, conv_taps, sink_logit,
    )
    return pl.pallas_call(
        store_kernel,
        out_shape=(jax.ShapeDtypeStruct(mixed.shape, bf), jax.ShapeDtypeStruct(log_sum.shape, f32)),
        in_specs=[pl.BlockSpec(memory_space=pltpu.VMEM)] * 2,
        out_specs=(pl.BlockSpec(memory_space=pl.ANY),) * 2,
        scratch_shapes=[dma((2,))],
    )(*(pltpu.with_memory_space_constraint(v, pltpu.VMEM) for v in (mixed, log_sum)))


def store_kernel(mixed_ref, log_sum_ref, out_ref, lse_ref, sem):
    copies = [
        pltpu.make_async_copy(src, dst, sem.at[i])
        for i, (src, dst) in enumerate(((log_sum_ref, lse_ref), (mixed_ref, out_ref)))
    ]
    for copy in copies:
        copy.start()
    for copy in copies:
        copy.wait()


def fits(
    tokens, norm_gain, w_query, w_key, w_value, w_post_gate, w_pre_gate, w_conv_in,
    conv_taps, sink_logit, w_out_attn, w_out_conv,
):
    S, TP = lax.axis_size("sp"), lax.axis_size("tp")
    return (
        TP == 4
        and S % 2 == 0
        and S == 8
        and w_key.shape[1] == HEAD_DIM
        and w_query.shape[0] % 128 == 0
        and w_query.shape[1] % 128 == 0
        and w_post_gate.shape[1] == w_query.shape[1]
        and w_out_attn.shape[1] % 128 == 0
        and tokens.shape[0] % (TP * WINDOW) == 0
        and tokens.shape[1] % 128 == 0
    )


def either(*args):
    return fused(*args) if fits(*args) else on_device(*args)


def solution(mesh):
    placed = (
        P("sp", "tp"),
        P(),
        P("sp", "tp"),
        P("sp", "tp"),
        P("sp", "tp"),
        P("sp", "tp"),
        P("sp", "tp"),
        P("sp", "tp"),
        P(None, "tp"),
        P("tp"),
        P("tp", "sp"),
        P("tp", "sp"),
    )
    return jax.shard_map(
        either,
        mesh=mesh,
        in_specs=placed,
        out_specs=(P(("sp", "tp"), None), P("tp", "sp")),
        check_vma=False,
    )
```

```python
import functools
import math

import jax
import jax.numpy as jnp
from jax import lax
from jax.experimental import pallas as pl
from jax.experimental.pallas import tpu as pltpu
from jax.sharding import PartitionSpec as P

MESH = pl.DeviceIdType.MESH

HEAD_DIM = 64
WINDOW = 128
GRID_W = 64
EDGE = 16
NEAR = 8


rope_base = 10000.0
norm_eps = 1e-06


def padded(block, sides, width):
    for axis, dim in sides:
        count = lax.axis_size(axis)
        forward = [(i, i + 1) for i in range(count - 1)]
        backward = [(target, source) for source, target in forward]
        low = lax.ppermute(
            lax.slice_in_dim(block, block.shape[dim] - width, None, axis=dim), axis, forward
        )
        high = lax.ppermute(lax.slice_in_dim(block, 0, width, axis=dim), axis, backward)
        block = jnp.concatenate([low, block, high], axis=dim)
    return block


def rotate_pair(values, angles):
    first_half, second_half = jnp.split(values, 2, axis=-1)
    cosine = jnp.cos(angles)[:, None, :]
    sine_part = jnp.sin(angles)[:, None, :]
    return jnp.concatenate(
        [
            first_half * cosine - second_half * sine_part,
            first_half * sine_part + second_half * cosine,
        ],
        axis=-1,
    )


def axial_rotate(values, positions):
    half_dim = values.shape[-1] // 2
    inv_freq = rope_base ** (-jnp.arange(0, half_dim, 2).astype(jnp.float32) / half_dim)
    row_angle = (positions // GRID_W).astype(jnp.float32)[:, None] * inv_freq
    col_angle = (positions % GRID_W).astype(jnp.float32)[:, None] * inv_freq
    row_part, col_part = jnp.split(values, 2, axis=-1)
    return jnp.concatenate(
        [rotate_pair(row_part, row_angle), rotate_pair(col_part, col_angle)], axis=-1
    )


def block_windows(source, rows_local, blocks):
    pieces = [
        source[step * WINDOW : step * WINDOW + rows_local].reshape(
            (blocks, WINDOW) + source.shape[1:]
        )
        for step in range(3)
    ]
    return jnp.concatenate(pieces, axis=1)


def on_device(
    tokens,
    norm_gain,
    w_query,
    w_key,
    w_value,
    w_post_gate,
    w_pre_gate,
    w_conv_in,
    conv_taps,
    sink_logit,
    w_out_attn,
    w_out_conv,
):
    whole = lax.all_gather(tokens, "tp", axis=1, tiled=True)
    rows_local = whole.shape[0]
    whole_float = whole.astype(jnp.float32)
    mean_square = jnp.mean(whole_float * whole_float, axis=1, keepdims=True)
    normed = (whole_float * lax.rsqrt(mean_square + norm_eps) * norm_gain).astype(jnp.bfloat16)
    col_widths = [
        w_query.shape[1],
        w_key.shape[1],
        w_value.shape[1],
        w_post_gate.shape[1],
        w_pre_gate.shape[1],
        w_conv_in.shape[1],
    ]
    joined = jnp.concatenate(
        (
            lax.all_gather(w_query, "sp", axis=0, tiled=True),
            lax.all_gather(w_key, "sp", axis=0, tiled=True),
            lax.all_gather(w_value, "sp", axis=0, tiled=True),
            lax.all_gather(w_post_gate, "sp", axis=0, tiled=True),
            lax.all_gather(w_pre_gate, "sp", axis=0, tiled=True),
            lax.all_gather(w_conv_in, "sp", axis=0, tiled=True),
        ),
        axis=1,
    )
    projected = jnp.dot(normed, joined, preferred_element_type=jnp.float32)
    bounds = []
    running = 0
    for col_width in col_widths[:-1]:
        running += col_width
        bounds.append(running)
    query_raw, key_raw, value_raw, post_gate, pre_gate, conv_input = jnp.split(
        projected, bounds, axis=1
    )
    offset = lax.axis_index("sp") * rows_local
    positions = offset + jnp.arange(rows_local, dtype=jnp.int32)
    local_heads = w_query.shape[1] // HEAD_DIM
    local_groups = w_key.shape[1] // HEAD_DIM
    group_size = local_heads // local_groups
    queries = axial_rotate(query_raw.reshape(rows_local, local_heads, HEAD_DIM), positions).astype(
        jnp.bfloat16
    )
    keys_rot = axial_rotate(key_raw.reshape(rows_local, local_groups, HEAD_DIM), positions).astype(
        jnp.bfloat16
    )
    key_value = jnp.concatenate(
        [keys_rot.reshape(rows_local, local_groups * HEAD_DIM), value_raw.astype(jnp.bfloat16)],
        axis=1,
    )
    mixed_input = (pre_gate * conv_input).astype(jnp.bfloat16)
    kv_padded = padded(key_value, (("sp", 0),), WINDOW)
    conv_padded = padded(mixed_input, (("sp", 0),), 1)
    conv_float = conv_padded.astype(jnp.float32)
    convolved = (
        conv_taps[0] * conv_float[:-2]
        + conv_taps[1] * conv_float[1:-1]
        + conv_taps[2] * conv_float[2:]
    )
    conv_out = (post_gate * convolved).astype(jnp.bfloat16)
    total_tokens = rows_local * lax.axis_size("sp")
    blocks = rows_local // WINDOW
    padded_rows = rows_local + 2 * WINDOW
    block_queries = queries.reshape(blocks, WINDOW, local_groups, group_size, HEAD_DIM)
    block_keys = block_windows(
        kv_padded[:, : local_groups * HEAD_DIM].reshape(padded_rows, local_groups, HEAD_DIM),
        rows_local,
        blocks,
    )
    block_values = block_windows(
        kv_padded[:, local_groups * HEAD_DIM :].reshape(padded_rows, local_groups, HEAD_DIM),
        rows_local,
        blocks,
    )
    scores = jnp.einsum(
        "nqkgd,nskd->nkgqs", block_queries, block_keys, preferred_element_type=jnp.float32
    ) * HEAD_DIM ** (-0.5)
    query_pos = positions.reshape(blocks, WINDOW)
    key_pos = (
        offset
        - WINDOW
        + (jnp.arange(blocks, dtype=jnp.int32) * WINDOW)[:, None]
        + jnp.arange(3 * WINDOW, dtype=jnp.int32)[None, :]
    )
    distance = key_pos[:, None, :] - query_pos[:, :, None]
    allowed = (
        (jnp.abs(distance) <= WINDOW)
        & (key_pos >= 0)[:, None, :]
        & (key_pos < total_tokens)[:, None, :]
    )
    scores = jnp.where(allowed[:, None, None], scores, -jnp.inf)
    sink_values = sink_logit.reshape(local_groups, group_size)[None, :, :, None]
    row_max = jnp.maximum(jnp.max(scores, axis=-1), sink_values)
    exp_scores = jnp.exp(scores - row_max[..., None])
    denominator = jnp.sum(exp_scores, axis=-1) + jnp.exp(sink_values - row_max)
    weights = (exp_scores / denominator[..., None]).astype(jnp.bfloat16)
    attended = (
        jnp.einsum("nkgqs,nskd->nqkgd", weights, block_values, preferred_element_type=jnp.float32)
        .astype(jnp.bfloat16)
        .reshape(rows_local, local_heads * HEAD_DIM)
    )
    log_sum = row_max + jnp.log(denominator)
    log_weight_sum = jnp.transpose(log_sum, (1, 2, 0, 3)).reshape(local_heads, rows_local)
    out_attn, out_conv = (
        lax.all_gather(w_out_attn, "sp", axis=1, tiled=True),
        lax.all_gather(w_out_conv, "sp", axis=1, tiled=True),
    )
    mixed = lax.psum_scatter(
        (
            jnp.dot(attended, out_attn, preferred_element_type=jnp.float32)
            + jnp.dot(conv_out, out_conv, preferred_element_type=jnp.float32)
        ).astype(jnp.bfloat16),
        "tp",
        scatter_dimension=0,
        tiled=True,
    )
    return (mixed, log_weight_sum)


def fused_kernel(
    Z, X,
    tok_ref, gain_ref, wq_ref, wk_ref, wv_ref, wpost_ref, wpre_ref, wcin_ref, oa_ref, oc_ref, taps_ref, sink_ref,
    out_ref, lse_ref,
    cos_ref, sin_ref, tok, normed, win_a, win_b, wo, acc_a, acc_b, qbuf, kvp, cf, ac, acg, ext, lse_buf,
    keep, send1, recv1, send2, recv2, gout, gin,
    tok_send, tok_recv, wz_send, wd_send, w_recv, sw_send, sw_recv, halo_sem, r_send, r_recv, g_send, g_recv, loc_sem,
):
    S = Z * X
    rows, width = tok_ref.shape
    depth = wq_ref.shape[0]
    ow, cols = oa_ref.shape
    qw = qbuf.shape[1]
    cw = cf.shape[1]
    kw = 2 * HEAD_DIM
    TP = tok.shape[0] - 1
    chunk = rows // TP
    sp = lax.axis_index("sp")
    tp = lax.axis_index("tp")
    z, x = sp // X, sp % X
    c, y = tp % 2, tp // 2
    vs = z * X + c
    home, foreign = c == x, c != x
    role = jnp.where(home, 0, 1)
    sib = (sp, y * 2 + 1 - c)
    ynb = (sp, (1 - y) * 2 + c)
    yoth = (sp, (1 - y) * 2 + 1 - c)
    xnb = (z * X + 1 - x, tp)
    swp = (z * X + 1 - x, y * 2 + 1 - c)
    low, high = (sp - X, tp), (sp + X, tp)
    has_low, has_high = z > 0, z < Z - 1
    has_prev, has_next = vs > 0, vs < S - 1
    vn, vp = vs + 1, vs - 1 + S
    next_dev = ((vn // X) * X + x, y * 2 + vn % X)
    prev_dev = ((vp // X - Z) * X + x, y * 2 + vp % X)

    barrier = pltpu.get_barrier_semaphore()

    def greet(dev):
        pl.semaphore_signal(barrier, inc=1, device_id=dev, device_id_type=MESH)

    for dev in (sib, ynb, yoth, xnb, swp):
        greet(dev)
    peers = 5
    across_z = ((has_low, low), (has_high, high), (has_prev & (c == 0), prev_dev), (has_next & (c == 1), next_dev))
    for cond, dev in across_z:
        @pl.when(cond)
        def _(dev=dev):
            greet(dev)
        peers = peers + jnp.where(cond, 1, 0)

    pslot = jnp.where(home, sp, S)
    own_tok = jnp.where(home, tp, TP)
    load_tok = pltpu.make_async_copy(tok_ref, tok.at[own_tok], loc_sem.at[0])
    load_a = pltpu.make_async_copy(wq_ref, win_a.at[pslot, :, pl.ds(0, qw)], loc_sem.at[1])
    load_b = [
        pltpu.make_async_copy(ref, win_b.at[pslot, :, pl.ds(part * cw, cw)], loc_sem.at[2])
        for part, ref in enumerate((wpost_ref, wpre_ref, wcin_ref))
    ]
    load_c = [
        pltpu.make_async_copy(ref, wo.at[pslot, pl.ds(part * ow, ow)], loc_sem.at[3])
        for part, ref in enumerate((oa_ref, oc_ref))
    ]
    for copy in (load_a, load_tok, *load_b, *load_c):
        copy.start()
    kv_t = jnp.concatenate([wk_ref[...], wv_ref[...]], axis=0).astype(jnp.float32)
    win_a[pslot, :, qw:qw + kw] = jnp.transpose(kv_t).astype(jnp.bfloat16)
    heads = qw // HEAD_DIM
    ext[0] = jnp.zeros(ext.shape[1:], jnp.float32)
    ext[0, 0:3, :] = taps_ref[...]
    for h in range(heads):
        ext[0, 3 + h:4 + h, :] = jnp.full((1, cw), sink_ref[h], jnp.float32)

    pl.semaphore_wait(barrier, peers)

    def remote(src, dst, ssem, rsem, dev):
        return pltpu.make_async_remote_copy(
            src_ref=src, dst_ref=dst, send_sem=ssem, recv_sem=rsem,
            device_id=dev, device_id_type=MESH,
        )

    bufs = (win_a, win_b, wo)
    targets = (low, high, sib)

    def wcopy(kind, slot, direction):
        block = bufs[kind].at[slot]
        ssem = (wz_send, wz_send, wd_send)[direction].at[kind]
        return remote(block, block, ssem, w_recv.at[kind, slot], targets[direction])

    up_light = 2 * z + 1 < Z
    far = jnp.where(up_light, Z - 1, 0)
    inner = has_low & has_high
    outer = jnp.logical_not(inner)

    def sent(block, sem):
        remote(block, block, sem, sem, sib).wait_send()

    def own_far(kind):
        for direction, cond in ((0, has_low & jnp.logical_not(up_light)), (1, has_high & up_light)):
            @pl.when(cond)
            def _(direction=direction):
                wcopy(kind, vs, direction).start()
        wcopy(kind, vs, 2).start()

    def own_near(kind):
        for direction, cond in ((0, has_low & up_light), (1, has_high & jnp.logical_not(up_light))):
            @pl.when(cond)
            def _(direction=direction):
                wcopy(kind, vs, direction).start()

    def own_start(kind):
        own_near(kind)
        own_far(kind)

    def swap(i, slot):
        src, dst = (
            (win_a.at[S], win_a.at[slot]),
            (win_b.at[S], win_b.at[slot]),
            (wo.at[S], wo.at[slot]),
            (ext.at[0], ext.at[1]),
            (lse_buf.at[0], lse_buf.at[1]),
        )[i]
        return remote(src, dst, sw_send.at[i], sw_recv.at[i], swp)

    TH = 2
    part_rows = rows // TH

    def tok_copy(src, q, i, part, dev):
        r = pl.ds(part * part_rows, part_rows)
        return remote(src.at[r], tok.at[q, r], tok_send.at[i], tok_recv.at[q, part], dev)

    tok_d = [tok_copy(tok.at[own_tok], tp, 1, part, sib) for part in range(TH)]
    tok_y = [tok_copy(tok.at[own_tok], tp, 0, part, (sp, (1 - y) * 2 + x)) for part in range(TH)]
    tok_x = [tok_copy(tok.at[own_tok], tp, 0, part, (z * X + 1 - x, y * 2 + x)) for part in range(TH)]
    load_a.wait()

    @pl.when(home)
    def _():
        own_start(0)

    @pl.when(foreign)
    def _():
        swap(0, sp).start()

    load_tok.wait()
    for part in range(TH):
        tok_x[part].start()
        tok_y[part].start()

    @pl.when(foreign)
    def _():
        for copy in tok_d:
            copy.start()

    def loaded(block, sem):
        pltpu.make_async_copy(block, block, sem).wait()

    loaded(win_b.at[pslot], loc_sem.at[2])
    loaded(wo.at[pslot], loc_sem.at[3])

    @pl.when(home)
    def _():
        own_start(1)

    @pl.when(foreign)
    def _():
        for i in (1, 3, 2):
            swap(i, sp).start()

    MB = 128
    quarter = HEAD_DIM // 4

    def angles(i, carry):
        r = pl.ds(pl.multiple_of(i * MB, MB), MB)
        pos = vs * rows + i * MB + lax.broadcasted_iota(jnp.int32, (MB, kw), 0)
        lane = lax.broadcasted_iota(jnp.int32, (MB, kw), 1) % HEAD_DIM
        freq = jnp.exp((lane % quarter).astype(jnp.float32) * (-4.0 / HEAD_DIM * math.log(rope_base)))
        index = jnp.where(lane >= 2 * quarter, pos % GRID_W, pos // GRID_W)
        angle = index.astype(jnp.float32) * freq
        cos_ref[r, :] = jnp.cos(angle)
        sin_ref[r, :] = jnp.where(lane % (2 * quarter) < quarter, -1.0, 1.0) * jnp.sin(angle)
        return carry

    def comm(kind, dist, only=None, forward=True):
        for up in (0, 1):
            zz = z + dist * (2 * up - 1)
            valid = (zz >= 0) & (zz < Z)
            if only is not None:
                valid = valid & only

            @pl.when(valid)
            def _(zz=zz, up=up):
                slot = zz * X + c
                wcopy(kind, slot, 2).wait_recv()

                if forward:
                    @pl.when(has_low if up else has_high)
                    def _():
                        wcopy(kind, slot, 0 if up else 1).start()
                wcopy(kind, slot, 2).start()

    def relay(cc, part):
        q = y * 2 + cc
        return tok_copy(tok.at[q], q, 1, part, ynb)

    def tok_wait(q, part):
        tok_copy(tok.at[q], q, 0, part, ynb).wait_recv()

    RB = 64

    def norm_rows(i, carry):
        r = pl.ds(pl.multiple_of(i * RB, RB), RB)
        total = jnp.zeros((RB, 1), jnp.float32)
        for t in range(TP):
            v = tok[t, r, :].astype(jnp.float32)
            total += jnp.sum(v * v, axis=1, keepdims=True)
        scale = lax.rsqrt(total / (TP * width) + norm_eps)
        for t in range(TP):
            v = tok[t, r, :].astype(jnp.float32)
            g = gain_ref[:, t * width:(t + 1) * width]
            normed[r, t * width:(t + 1) * width] = (v * scale * g).astype(jnp.bfloat16)
        return carry

    pdepth = X * depth

    def project(kind, first, planes, fresh):
        win, acc = ((win_a, acc_a), (win_b, acc_b))[kind]
        n = acc.shape[1]
        kk = planes * pdepth
        for p in range(planes):
            wcopy(kind, (first + p) * X + 1 - c, 2).wait_recv()
        pb = acc.shape[0]

        def body(i, carry):
            r = pl.ds(0, pb)
            k = pl.ds(pl.multiple_of(first * pdepth, pdepth), kk)
            weight = win[pl.ds(first * X, planes * X)].reshape(kk, n)
            prod = jnp.dot(normed[r, k], weight, preferred_element_type=jnp.float32)
            if fresh:
                acc[r, :] = prod
            else:
                acc[r, :] += prod
            return carry
        body(0, 0)

    def each_side(dist, fn):
        def step(side, carry):
            zz = z + dist * (2 * side - 1)

            @pl.when((zz >= 0) & (zz < Z))
            def _():
                fn(zz)
            return carry
        lax.fori_loop(0, 2, step, 0)

    def halo(i, src, dst, dev):
        return remote(src, dst, halo_sem.at[2 * i], halo_sem.at[2 * i + 1], dev)

    kv_next = halo(0, kvp.at[pl.ds(rows, WINDOW)], kvp.at[pl.ds(0, WINDOW)], next_dev)
    kv_prev = halo(1, kvp.at[pl.ds(WINDOW, WINDOW)], kvp.at[pl.ds(WINDOW + rows, WINDOW)], prev_dev)
    n_next = halo(2, normed.at[pl.ds(rows - NEAR, NEAR)], normed.at[pl.ds(rows + EDGE - NEAR, NEAR)], next_dev)
    n_prev = halo(3, normed.at[pl.ds(0, NEAR)], normed.at[pl.ds(rows + EDGE, NEAR)], prev_dev)

    lax.fori_loop(0, rows // MB, angles, 0)

    @pl.when(foreign)
    def _():
        swap(0, vs).wait_recv()
        own_start(0)
        for cc in (c, 1 - c):
            tok_wait(y * 2 + cc, 0)
            relay(cc, 0).start()

    comm(0, 1)

    @pl.when(foreign)
    def _():
        for cc in (c, 1 - c):
            tok_wait(y * 2 + cc, 1)
            relay(cc, 1).start()

    @pl.when(home)
    def _():
        comm(1, 1)
    comm(0, 2)

    @pl.when(foreign)
    def _():
        swap(1, vs).wait_recv()
        own_start(1)
        swap(3, vs).wait_recv()

    @pl.when(home)
    def _():
        own_far(2)
        for part in range(TH):
            tok_wait(y * 2 + 1 - c, part)
    for part in range(TH):
        if part == TH - 1:
            for dist in range(3, Z):
                comm(0, dist)
        for cc in range(2):
            tok_wait((1 - y) * 2 + cc, part)
        lax.fori_loop(part * (part_rows // RB), (part + 1) * (part_rows // RB), norm_rows, 0)

    @pl.when(has_next)
    def _():
        n_next.start()

    @pl.when(has_prev)
    def _():
        n_prev.start()

    @pl.when(home)
    def _():
        comm(1, 2)

    project(0, jnp.int32(0), Z, True)

    @pl.when(foreign)
    def _():
        comm(1, 1, inner)
        swap(2, vs).wait_recv()
        own_far(2)
        comm(1, 1, outer)

    def turned(v, cosv, sinv):
        lane = lax.broadcasted_iota(jnp.int32, v.shape, 1)
        partner = jnp.where(
            lane % (2 * quarter) < quarter,
            pltpu.roll(v, v.shape[1] - quarter, 1),
            pltpu.roll(v, quarter, 1),
        )
        return v * cosv + partner * sinv

    def k_rows(i, carry):
        r = pl.ds(pl.multiple_of(i * MB, MB), MB)
        v = acc_a[r, qw:qw + kw]
        lane = lax.broadcasted_iota(jnp.int32, v.shape, 1)
        kv = jnp.where(lane < HEAD_DIM, turned(v, cos_ref[r, :], sin_ref[r, :]), v)
        kvp[pl.ds(pl.multiple_of(WINDOW + i * MB, MB), MB), :] = kv.astype(jnp.bfloat16)
        return carry

    lax.fori_loop(0, rows // MB, k_rows, 0)

    @pl.when(has_next)
    def _():
        kv_next.start()

    @pl.when(has_prev)
    def _():
        kv_prev.start()

    def q_rows(i, carry):
        r = pl.ds(pl.multiple_of(i * MB, MB), MB)
        for k in range(qw // kw):
            qbuf[r, k * kw:(k + 1) * kw] = turned(
                acc_a[r, k * kw:(k + 1) * kw], cos_ref[r, :], sin_ref[r, :]
            ).astype(jnp.bfloat16)
        return carry

    lax.fori_loop(0, rows // MB, q_rows, 0)

    K3 = 3 * WINDOW
    total_tokens = rows * S

    guest_dev = (sp + X * jnp.where(inner == up_light, -1, 1), tp)

    def guest_copy(half, r):
        return remote(ac.at[half, r], acg.at[half, r], g_send.at[half], g_recv.at[half], guest_dev)

    def attend(b, carry):
        r = pl.ds(pl.multiple_of(b * WINDOW, WINDOW), WINDOW)
        kv = kvp[pl.ds(pl.multiple_of(b * WINDOW, WINDOW), K3), :].astype(jnp.float32)
        lane = lax.broadcasted_iota(jnp.int32, (K3, kw), 1)
        swapped = pltpu.roll(kv, HEAD_DIM, 1)
        kk = jnp.where(lane < HEAD_DIM, kv, swapped).astype(jnp.bfloat16)
        vv = jnp.where(lane < HEAD_DIM, swapped, kv).astype(jnp.bfloat16)
        k_half = [jnp.where(lane < HEAD_DIM, kk, 0), jnp.where(lane < HEAD_DIM, 0, kk)]
        v_half = [jnp.where(lane < HEAD_DIM, vv, 0), jnp.where(lane < HEAD_DIM, 0, vv)]
        qi = lax.broadcasted_iota(jnp.int32, (WINDOW, K3), 0)
        ki = lax.broadcasted_iota(jnp.int32, (WINDOW, K3), 1)
        first = vs * rows + b * WINDOW - WINDOW
        allowed = (ki >= qi) & (ki <= qi + 2 * WINDOW) & (ki + first >= 0) & (ki + first < total_tokens)
        lse_lane = lax.broadcasted_iota(jnp.int32, (WINDOW, WINDOW), 1)
        lse_all = jnp.zeros((WINDOW, WINDOW), jnp.float32)
        for pair in range(heads // 2):
            q = qbuf[r, pair * kw:(pair + 1) * kw]
            total = jnp.zeros((WINDOW, kw), jnp.float32)
            for side in range(2):
                h = pair * 2 + side
                s = lax.dot_general(
                    q, k_half[side], (((1,), (1,)), ((), ())), preferred_element_type=jnp.float32
                ) * HEAD_DIM ** (-0.5)
                s = jnp.where(allowed, s, -jnp.inf)
                sink = ext[role, 3 + h:4 + h, 0:WINDOW]
                top = jnp.maximum(jnp.max(s, axis=1, keepdims=True), sink)
                e = jnp.exp(s - jnp.concatenate([top] * 3, axis=1))
                den = jnp.sum(e, axis=1, keepdims=True) + jnp.exp(sink - top)
                w = (e * jnp.concatenate([1.0 / den] * 3, axis=1)).astype(jnp.bfloat16)
                total += jnp.dot(w, v_half[side], preferred_element_type=jnp.float32)
                lse_all = jnp.where(lse_lane == h, top + jnp.log(den), lse_all)
            ac[0, r, pair * kw:(pair + 1) * kw] = total.astype(jnp.bfloat16)

        @pl.when(outer)
        def _():
            guest_copy(0, r).start()
        lse_buf[0, :, r] = jnp.transpose(lse_all)[0:heads, :]
        return carry

    blocks = rows // WINDOW
    zero_kv = jnp.zeros((WINDOW, kw), jnp.bfloat16)

    def prev_ready():
        @pl.when(has_prev)
        def _():
            kv_next.wait_recv()

        @pl.when(jnp.logical_not(has_prev))
        def _():
            kvp[0:WINDOW, :] = zero_kv

    def next_ready():
        @pl.when(has_next)
        def _():
            kv_prev.wait_recv()

        @pl.when(jnp.logical_not(has_next))
        def _():
            kvp[WINDOW + rows:, :] = zero_kv

    def edge_ready(at_start):
        @pl.when(at_start)
        def _():
            prev_ready()

        @pl.when(jnp.logical_not(at_start))
        def _():
            next_ready()

    def attend_from(i, carry):
        near = jnp.where(c == 0, blocks - 1, 0)
        edge_block = jnp.where(i == blocks - 2, near, blocks - 1 - near)
        return attend(jnp.where(i < blocks - 2, i + 1, edge_block), carry)

    def b_ready():
        @pl.when(has_prev)
        def _():
            n_next.wait_recv()

        @pl.when(has_next)
        def _():
            n_prev.wait_recv()

        zero_n = jnp.zeros((NEAR, TP * width), jnp.bfloat16)
        normed[rows:rows + EDGE - NEAR, :] = zero_n
        normed[rows + EDGE + NEAR:, :] = zero_n

        @pl.when(jnp.logical_not(has_prev))
        def _():
            normed[rows + EDGE - NEAR:rows + EDGE, :] = zero_n

        @pl.when(jnp.logical_not(has_next))
        def _():
            normed[rows + EDGE:rows + EDGE + NEAR, :] = zero_n

    @pl.when(home)
    def _():
        for dist in range(3, Z):
            comm(1, dist)

    lax.fori_loop(0, blocks - 2, attend_from, 0)
    edge_ready(c == 1)
    b_ready()

    @pl.when(foreign)
    def _():
        comm(1, 2)
        own_near(2)
    lax.fori_loop(blocks - 2, blocks - 1, attend_from, 0)
    edge_ready(c == 0)
    lax.fori_loop(blocks - 1, blocks, attend_from, 0)

    @pl.when(foreign)
    def _():
        swap(4, sp).start()

    project(1, jnp.where(up_light, 0, 1), Z - 1, True)

    @pl.when(foreign)
    def _():
        for dist in range(3, Z):
            comm(1, dist)
    project(1, far, 1, False)
    @pl.when(home)
    def _():
        own_near(2)

    comm(2, 1, inner)

    def gated(lo, n):
        return (acc_b[lo:lo + n, cw:2 * cw] * acc_b[lo:lo + n, 2 * cw:3 * cw]).astype(jnp.bfloat16)

    for i in range(rows // MB):
        cf[8 + i * MB:8 + (i + 1) * MB, :] = gated(i * MB, MB).astype(jnp.float32)
    edge = gated(rows, 2 * EDGE).astype(jnp.float32)
    cf[0:8, :] = edge[EDGE - 8:EDGE, :]
    cf[8 + rows:16 + rows, :] = edge[EDGE:EDGE + 8, :]

    taps = [ext[role, t:t + 1, :] for t in range(3)]
    for i in range(rows // MB):
        a = 8 + i * MB
        conv = (
            taps[0] * cf[a - 1:a - 1 + MB, :]
            + taps[1] * cf[a:a + MB, :]
            + taps[2] * cf[a + 1:a + 1 + MB, :]
        )
        ac[1, i * MB:(i + 1) * MB, :] = (acc_b[i * MB:(i + 1) * MB, 0:cw] * conv).astype(jnp.bfloat16)

        @pl.when(outer)
        def _(i=i):
            guest_copy(1, pl.ds(i * MB, MB)).start()

    mine_dev = (z * X + c, y * 2 + c)
    other_dev = (z * X + c, y * 2 + 1 - c)

    def r1(s, src, dst, dev, extra=0):
        return remote(send1.at[s, src], recv1.at[s, dst], r_send.at[extra], r_recv.at[s, dst], dev)

    def r2(s, src, dst, dev, sem, extra=0):
        return remote(send2.at[s, src], recv2.at[s, dst], r_send.at[2 + extra], r_recv.at[s, sem], dev)

    def out_dot(src, w, yo):
        r = pl.ds(pl.multiple_of(yo * 2 * chunk, chunk), 2 * chunk)
        both = jnp.concatenate([src[0, r, :], src[1, r, :]], axis=1)
        v = jnp.dot(both, wo[w], preferred_element_type=jnp.float32)
        return v[0:chunk], v[chunk:2 * chunk]

    def produce_x(s, w, src, core):
        for yo in range(2):
            v = out_dot(src, w, yo)
            keep[s, yo] = v[core]
            send1[s, 0, yo] = v[core].astype(jnp.bfloat16)
            send1[s, 1, yo] = v[1 - core].astype(jnp.bfloat16)
        r1(s, 1, role, other_dev).start()

        @pl.when(foreign)
        def _():
            r1(s, 0, 1, mine_dev, 1).start()

    def produce_y(s, w, src, core):
        v = out_dot(src, w, 1 - y)
        send1[s, 0, 0] = v[core].astype(jnp.bfloat16)
        send1[s, 0, 1] = v[1 - core].astype(jnp.bfloat16)
        r1(s, 0, 0, ynb).start()
        v = out_dot(src, w, y)
        keep[s, 0] = v[core]
        keep[s, 1] = v[1 - core]

    def stage_x(s):
        r1(s, 0, 1, mine_dev).wait_recv()

        def pass_on(base):
            send2[s, 0] = (base(1 - y) + recv1[s, 1, 1 - y].astype(jnp.float32)).astype(jnp.bfloat16)
            r2(s, 0, 0, ynb, 2).start()
            keep[s, y] = base(y) + recv1[s, 1, y].astype(jnp.float32)

        @pl.when(home)
        def _():
            pass_on(lambda yo: keep[s, yo])

        @pl.when(foreign)
        def _():
            r1(s, 1, 0, other_dev).wait_recv()
            pass_on(lambda yo: recv1[s, 0, yo].astype(jnp.float32))

    def stage_y(s):
        r1(s, 0, 0, ynb).wait_recv()
        send2[s, 1] = (keep[s, 1] + recv1[s, 0, 1].astype(jnp.float32)).astype(jnp.bfloat16)
        r2(s, 1, role, other_dev, 1 + role).start()
        mine = keep[s, 0] + recv1[s, 0, 0].astype(jnp.float32)

        @pl.when(home)
        def _():
            keep[s, 0] = mine

        @pl.when(foreign)
        def _():
            send2[s, 0] = mine.astype(jnp.bfloat16)
            r2(s, 0, 1, mine_dev, 2, 1).start()

    def place(s, v):
        out_ref[:, pl.ds(pl.multiple_of(s * cols, cols), cols)] = v.astype(jnp.bfloat16)

    def finish_x(s, place=place):
        r2(s, 0, 0, ynb, 2).wait_recv()
        place(s, keep[s, y] + recv2[s, 0].astype(jnp.float32))

    def finish_y(s, place=place):
        r2(s, 0, 1, mine_dev, 2).wait_recv()
        arrived = recv2[s, 1].astype(jnp.float32)

        @pl.when(home)
        def _():
            place(s, keep[s, 0] + arrived)

        @pl.when(foreign)
        def _():
            r2(s, 1, 0, other_dev, 1).wait_recv()
            place(s, recv2[s, 0].astype(jnp.float32) + arrived)

    def produce_from(b, zz, src, sibling_ready=lambda: None):
        @pl.when(c == 0)
        def _():
            produce_x(b, zz * X, src, 0)
            sibling_ready()
            produce_y(b + 1, zz * X + 1, src, 0)

        @pl.when(c == 1)
        def _():
            produce_y(b + 1, zz * X + 1, src, 1)
            sibling_ready()
            produce_x(b, zz * X, src, 1)

    def produce(zz):
        produce_from(zz * X, zz, ac, lambda: wcopy(2, zz * X + 1 - c, 2).wait_recv())

    def stage(zz):
        stage_x(zz * X)
        stage_y(zz * X + 1)

    def finish(zz):
        finish_x(zz * X)
        finish_y(zz * X + 1)

    def hand_back(i):
        return remote(gout.at[i], gin.at[i], g_send.at[2 + i], g_recv.at[2 + i], guest_dev)

    def back(i):
        def put(s, v):
            gout[i] = v.astype(jnp.bfloat16)
            hand_back(i).start()
        return put

    produce(z)
    comm(2, 1, outer)
    each_side(1, produce)
    comm(2, 2, inner, False)
    stage(z)
    comm(2, 2, outer, False)

    @pl.when(outer)
    def _():
        each_side(2, produce)
        each_side(1, stage)

    @pl.when(inner)
    def _():
        for half in range(2):
            remote(acg.at[half], acg.at[half], g_send.at[half], g_recv.at[half], guest_dev).wait_recv()
        wcopy(2, far * X + 1 - c, 2).wait_recv()
        produce_from(S, far, acg)
        each_side(1, stage)
        stage_y(S + 1)
        stage_x(S)
        produce_from(far * X, far, ac)
    @pl.when(inner)
    def _():
        finish_y(S + 1, back(1))
        finish_x(S, back(0))
    each_side(2, stage)
    finish(z)
    each_side(1, finish)
    each_side(2, finish)

    @pl.when(inner)
    def _():
        for i in range(2):
            hand_back(i).wait_send()

    @pl.when(outer)
    def _():
        for i in range(2):
            hand_back(i).wait_recv()
            place(far * X + i, gin[i])
        for half in range(2):
            sent(ac.at[half], g_send.at[half])

    @pl.when(home)
    def _():
        lse_ref[...] = lse_buf[0]

    @pl.when(foreign)
    def _():
        swap(4, vs).wait_recv()
        lse_ref[...] = lse_buf[1]
        for i in range(5):
            swap(i, sp).wait_send()

    @pl.when(has_next)
    def _():
        kv_next.wait_send()
        n_next.wait_send()

    @pl.when(has_prev)
    def _():
        kv_prev.wait_send()
        n_prev.wait_send()

    sent(tok.at[pl.ds(0, 2)], tok_send.at[0])
    for cond, pairs, along in ((inner, Z + 1, Z + 1), (outer, Z - 1, 1)):
        @pl.when(cond)
        def _(pairs=pairs, along=along):
            for kind in range(3):
                fewer = 1 if kind == 2 and along > 1 else 0
                sent(bufs[kind].at[pl.ds(0, along - fewer)], wz_send.at[kind])
                sent(bufs[kind].at[pl.ds(0, Z if kind < 2 else min(pairs, Z))], wd_send.at[kind])
            sent(send1.at[pl.ds(0, pairs)], r_send.at[0])
            sent(send2.at[pl.ds(0, pairs)], r_send.at[2])

            @pl.when(foreign)
            def _():
                sent(send1.at[pl.ds(0, pairs), 0], r_send.at[1])
                sent(send2.at[pl.ds(0, pairs), 0], r_send.at[3])

    @pl.when(foreign)
    def _():
        sent(tok.at[pl.ds(0, 3)], tok_send.at[1])


def fused(
    tokens, norm_gain, w_query, w_key, w_value, w_post_gate, w_pre_gate, w_conv_in,
    conv_taps, sink_logit, w_out_attn, w_out_conv,
):
    S, TP = lax.axis_size("sp"), lax.axis_size("tp")
    X = 2
    Z = S // X
    rows, width = tokens.shape
    depth, qw = w_query.shape
    cw = w_post_gate.shape[1]
    ow, cols = w_out_attn.shape
    heads = qw // HEAD_DIM
    kw = 2 * HEAD_DIM
    chunk = rows // TP
    bf, f32 = jnp.bfloat16, jnp.float32
    dma = pltpu.SemaphoreType.DMA
    mixed, log_sum = pl.pallas_call(
        functools.partial(fused_kernel, Z, X),
        out_shape=(
            pltpu.VMEM((chunk, S * cols), bf),
            pltpu.VMEM((heads, rows), f32),
        ),
        in_specs=[
            pl.BlockSpec(memory_space=space)
            for space in (pl.ANY, pltpu.VMEM, pl.ANY, *[pltpu.VMEM] * 2, *[pl.ANY] * 5, pltpu.VMEM, pltpu.SMEM)
        ],
        out_specs=(pl.BlockSpec(memory_space=pltpu.VMEM),) * 2,
        scratch_shapes=[
            pltpu.VMEM((rows, kw), f32),
            pltpu.VMEM((rows, kw), f32),
            pltpu.VMEM((TP + 1, rows, width), bf),
            pltpu.VMEM((rows + 2 * EDGE, TP * width), bf),
            pltpu.VMEM((S + 1, depth, qw + kw), bf),
            pltpu.VMEM((S + 1, depth, 3 * cw), bf),
            pltpu.VMEM((S + 1, ow + cw, cols), bf),
            pltpu.VMEM((rows, qw + kw), f32),
            pltpu.VMEM((rows + 2 * EDGE, 3 * cw), f32),
            pltpu.VMEM((rows, qw), bf),
            pltpu.VMEM((rows + 2 * WINDOW, kw), bf),
            pltpu.VMEM((rows + 16, cw), f32),
            pltpu.VMEM((2, rows, qw), bf),
            pltpu.VMEM((2, rows, qw), bf),
            pltpu.VMEM((2, -(-(3 + heads) // 8) * 8, cw), f32),
            pltpu.VMEM((2, heads, rows), f32),
            pltpu.VMEM((S + X, 2, chunk, cols), f32),
            pltpu.VMEM((S + X, 2, 2, chunk, cols), bf),
            pltpu.VMEM((S + X, 2, 2, chunk, cols), bf),
            pltpu.VMEM((S + X, 2, chunk, cols), bf),
            pltpu.VMEM((S + X, 2, chunk, cols), bf),
            pltpu.VMEM((X, chunk, cols), bf),
            pltpu.VMEM((X, chunk, cols), bf),
            dma((2,)), dma((TP, 2)),
            dma((3,)), dma((3,)), dma((3, S)),
            dma((5,)), dma((5,)),
            dma((8,)),
            dma((4,)), dma((S + X, 3)),
            dma((4,)), dma((4,)),
            dma((4,)),
        ],
        compiler_params=pltpu.CompilerParams(
            collective_id=0, has_side_effects=True, vmem_limit_bytes=60 * 1024 * 1024
        ),
    )(
        tokens, norm_gain[None, :], w_query, w_key.T, w_value.T, w_post_gate, w_pre_gate, w_conv_in,
        w_out_attn, w_out_conv, conv_taps, sink_logit,
    )
    return pl.pallas_call(
        store_kernel,
        out_shape=(jax.ShapeDtypeStruct(mixed.shape, bf), jax.ShapeDtypeStruct(log_sum.shape, f32)),
        in_specs=[pl.BlockSpec(memory_space=pltpu.VMEM)] * 2,
        out_specs=(pl.BlockSpec(memory_space=pl.ANY),) * 2,
        scratch_shapes=[dma((2,))],
    )(*(pltpu.with_memory_space_constraint(v, pltpu.VMEM) for v in (mixed, log_sum)))


def store_kernel(mixed_ref, log_sum_ref, out_ref, lse_ref, sem):
    copies = [
        pltpu.make_async_copy(src, dst, sem.at[i])
        for i, (src, dst) in enumerate(((log_sum_ref, lse_ref), (mixed_ref, out_ref)))
    ]
    for copy in copies:
        copy.start()
    for copy in copies:
        copy.wait()


def fits(
    tokens, norm_gain, w_query, w_key, w_value, w_post_gate, w_pre_gate, w_conv_in,
    conv_taps, sink_logit, w_out_attn, w_out_conv,
):
    S, TP = lax.axis_size("sp"), lax.axis_size("tp")
    return (
        TP == 4
        and S % 2 == 0
        and S == 8
        and w_key.shape[1] == HEAD_DIM
        and w_query.shape[0] % 128 == 0
        and w_query.shape[1] % 128 == 0
        and w_post_gate.shape[1] == w_query.shape[1]
        and w_out_attn.shape[1] % 128 == 0
        and tokens.shape[0] % (TP * WINDOW) == 0
        and tokens.shape[1] % 128 == 0
    )


def either(*args):
    return fused(*args) if fits(*args) else on_device(*args)


def solution(mesh):
    placed = (
        P("sp", "tp"),
        P(),
        P("sp", "tp"),
        P("sp", "tp"),
        P("sp", "tp"),
        P("sp", "tp"),
        P("sp", "tp"),
        P("sp", "tp"),
        P(None, "tp"),
        P("tp"),
        P("tp", "sp"),
        P("tp", "sp"),
    )
    return jax.shard_map(
        either,
        mesh=mesh,
        in_specs=placed,
        out_specs=(P(("sp", "tp"), None), P("tp", "sp")),
        check_vma=False,
    )
```
